256 devices in a mesh: grp: 2 (over y), ep: 32 (over z, core), tp: 4 (over x).
Axes of the slice: x: 4, y: 2, z: 16, core: 2. Of those that a mesh axis runs over, the one named last changes fastest.
The devices are a block of a 4x16x16 slice.
Arguments:
- x_in: bfloat16 [4096, 2048], P(('grp', 'ep')), parts along dimension 0, may hold values from -6 to 6
- state: float32 [4096, 96, 128], P(('grp', 'ep'), 'tp'), parts along dimension 0, may hold values from -6 to 6
- routes: int32 [4096, 2], P(('grp', 'ep')), parts along dimension 0, may hold values from 0 to 63, as said below
- w_in: bfloat16 [2048, 1536], P(None, 'tp'), may hold values from -0.125 to 0.125
- decay_rate: float32 [96, 64], P('tp'), may hold values from 0.01 to 1
- frequency: float32 [96, 64], P('tp'), may hold values from 0 to 192
- log_step: float32 [96], P('tp'), may hold values from -3 to 0
- b_in: float32 [96, 16, 128], P('tp'), may hold values from -1.5 to 1.5
- c_out: float32 [96, 16, 128], P('tp'), may hold values from -0.5 to 0.5
- skip: float32 [1536], P('tp'), may hold values from -3 to 3
- w_out: bfloat16 [1536, 2048], P('tp'), may hold values from -0.15625 to 0.15625
- gain_mix: float32 [2048], replicated, may hold values from 0.1 to 1.9
- w_group: bfloat16 [2048, 4], replicated, may hold values from -0.0625 to 0.0625
- w_expert: bfloat16 [2048, 64], replicated, may hold values from -0.0625 to 0.0625
- w_gate: bfloat16 [64, 2048, 1024], P('ep', None, 'tp'), may hold values from -0.125 to 0.125
- w_up: bfloat16 [64, 2048, 1024], P('ep', None, 'tp'), may hold values from -0.125 to 0.125
- w_down: bfloat16 [64, 1024, 2048], P('ep', 'tp'), may hold values from -3 to 3
- gain_moe: float32 [2048], replicated, may hold values from 0.1 to 1.9
Outputs:
- layer_out: bfloat16 [4096, 2048], P(('grp', 'ep')), parts along dimension 0
- new_state: float32 [4096, 96, 128], P(('grp', 'ep'), 'tp'), parts along dimension 0
The draws below stay inside these ranges and needn't reach their ends.
There are 2 independent parts, one for each index of `grp`. The reference program is written for one: setup_inputs(seed, part) draws one part's arguments, and reference() takes and returns one part's arrays. A program takes and returns all parts, laid end to end along the dimension named above; an argument that names none is the same for every part. Nothing has to cross between parts.
Inputs may be any that keep to these rules, and one draw needn't show every extreme that they name: `routes`: each row names two different experts of one group of 16 consecutive expert numbers. Within the rows of one index of ep (aligned blocks of 64 rows) no expert is named by more than 4 rows, and in every block some expert is named by exactly 4 rows.
All inputs are finite; a program needn't handle non-finite values.
Results may differ from the reference program's by a relative error of at most 0.015.
Values may be sent and summed in bfloat16 or wider, within the bound.
No kernel may reach another device: no remote copies, remote signals or barrier semaphores. Data moves between devices by JAX's collectives and lax.ppermute only.
A program may use at most 64 MiB of HBM per device.

```python
import math
import jax
import jax.numpy as jnp
from jax import lax

D = 2048
MIX = 1536
GROUP = 16
CHGROUPS = 96
STATE = 64
MIX_DEV = 384
FF = 1024
FF_DEV = 256
TOP = 2
EXPERTS = 64
EGROUPS = 4
SEQ_DEV = 64
SEQS = 2048
CAP = 4
N_EP = 32
N_TP = 4


def shuffle_rows(key_row):
    return jax.random.permutation(key_row, SEQ_DEV).astype(jnp.int32)


def shuffle_group(key_group):
    return jax.random.permutation(key_group, EXPERTS // EGROUPS).astype(jnp.int32)


def draw_routes(key, part):
    block_count = SEQS // SEQ_DEV
    pair_count = EXPERTS // 2
    group_size = EXPERTS // EGROUPS
    key_pair, key_order, key_offset, key_rows = jax.random.split(key, 4)
    within = jax.vmap(shuffle_group)(jax.random.split(key_pair, EGROUPS))
    members = within + group_size * jnp.arange(EGROUPS, dtype=jnp.int32)[:, None]
    pair_table = members.reshape(pair_count, 2)
    pair_order = jax.random.permutation(key_order, pair_count).astype(jnp.int32)
    offsets = jax.random.randint(key_offset, (block_count, 1), 0, pair_count - 1).astype(jnp.int32)
    ranks = jnp.arange(SEQ_DEV, dtype=jnp.int32)[None, :]
    slot_pick = jnp.where(ranks < CAP, 0, 1 + (ranks - CAP + offsets) % (pair_count - 1))
    slot_pick = jnp.broadcast_to(slot_pick, (block_count, SEQ_DEV))
    shuffled = jax.vmap(shuffle_rows)(jax.random.split(key_rows, block_count))
    mixed_pick = jnp.take_along_axis(slot_pick, shuffled, axis=1)
    picked = pair_table[pair_order[mixed_pick]]
    return picked.reshape(SEQS, 2).astype(jnp.int32)


def steps_of(key, shape, cuts, smallest, top_value):
    loudness, own = 1.0, jax.random.fold_in(key, 6)
    for axis_at, shards_of in cuts:
        steps = jnp.exp(jax.random.uniform(jax.random.fold_in(own, axis_at), (shards_of,), jnp.float32, smallest / len(cuts), top_value / len(cuts)))
        loudness = loudness * jnp.repeat(steps, shape[axis_at] // shards_of).reshape([-1 if axis == axis_at else 1 for axis in range(len(shape))])
    return loudness


def noise(stream_key, dims, scale, bound, shards=(), held_as=jnp.bfloat16):
    result = jax.random.normal(stream_key, dims, jnp.float32) * scale
    if len(shards) > 0:
        result = steps_of(stream_key, dims, shards, -0.22, 0.18) * result
    return jnp.clip(result, min=-bound, max=bound).astype(held_as)


def setup_inputs(seed: int = 0, part: int = 0) -> dict:
    seeds = jax.random.split(jax.random.key(seed), 19)
    part_splits = jax.random.split(jax.random.fold_in(seeds[18], part), 19)
    return {
        "x_in": noise(part_splits[0], (SEQS, D), 1.0, 6.0, ((0, 32),)),
        "state": noise(part_splits[1], (SEQS, CHGROUPS, 2 * STATE), 1.0, 6.0, ((0, 32), (1, 4)), jnp.float32),
        "routes": draw_routes(jax.random.fold_in(jax.random.fold_in(seeds[18], part), 71), part),
        "w_in": noise(seeds[3], (D, MIX), D ** -0.5, 0.125, ((1, 4),)),
        "decay_rate": jnp.clip(jnp.exp(math.log(1.0) - 4.6051702 * jax.random.uniform(seeds[4], (CHGROUPS, STATE), jnp.float32) ** steps_of(seeds[4], (CHGROUPS, STATE), ((0, 4),), -0.2, 0.2)), 0.01, 1.0),
        "frequency": jnp.clip(192.0 * jax.random.uniform(seeds[5], (CHGROUPS, STATE), jnp.float32) ** steps_of(seeds[5], (CHGROUPS, STATE), ((0, 4),), -0.2, 0.2), 0.0, 192.0),
        "log_step": jnp.clip(-3.0 + 3.0 * jax.random.uniform(seeds[6], (CHGROUPS,), jnp.float32) ** steps_of(seeds[6], (CHGROUPS,), ((0, 4),), -0.2, 0.2), -3.0, 0.0),
        "b_in": noise(seeds[7], (CHGROUPS, GROUP, 2 * STATE), GROUP ** -0.5, 1.5, ((0, 4),), jnp.float32),
        "c_out": noise(seeds[8], (CHGROUPS, GROUP, 2 * STATE), (2 * STATE) ** -0.5, 0.5, ((0, 4),), jnp.float32),
        "skip": noise(seeds[9], (MIX,), 0.5, 3.0, ((0, 4),), jnp.float32),
        "w_out": noise(seeds[10], (MIX, D), MIX ** -0.5, 0.15625, ((0, 4),)),
        "gain_mix": jnp.clip(1.0 + 0.18 * jax.random.normal(seeds[11], (D,), jnp.float32), 0.1, 1.9),
        "w_group": noise(seeds[12], (D, EGROUPS), (4 * D) ** -0.5, 0.0625),
        "w_expert": noise(seeds[13], (D, EXPERTS), (4 * D) ** -0.5, 0.0625),
        "w_gate": noise(seeds[14], (EXPERTS, D, FF), D ** -0.5, 0.125, ((0, 32), (2, 4))),
        "w_up": noise(seeds[15], (EXPERTS, D, FF), D ** -0.5, 0.125, ((0, 32), (2, 4))),
        "w_down": noise(seeds[16], (EXPERTS, FF, D), (max(1, FF // 256)) ** -0.5, 3.0, ((0, 32), (1, 4))),
        "gain_moe": jnp.clip(1.0 + 0.18 * jax.random.normal(seeds[17], (D,), jnp.float32), 0.1, 1.9),
    }


residual_scale = 8.0 ** 0.25
norm_eps = 1e-05

def normalize(values, gain):
    centre = lax.optimization_barrier(jnp.mean(values, -1, keepdims=True))
    spread = lax.optimization_barrier(jnp.mean(jnp.square(values - centre), -1, keepdims=True))
    return (values - centre) * lax.rsqrt(spread + norm_eps) * gain

def s5_advance(mix_input, state, decay_rate, frequency, log_step, b_in, c_out, skip):
    top_precision = lax.Precision.HIGHEST
    entries = decay_rate.shape[-1]
    group_count = decay_rate.shape[0]
    width = b_in.shape[1]
    seq_count = mix_input.shape[0]
    input_rows = mix_input.astype(jnp.float32).reshape(seq_count, group_count, width)
    step_size = jnp.exp(log_step)[:, None]
    lam_real = -decay_rate
    lam_imag = frequency
    magnitude = jnp.exp(lam_real * step_size)
    angle_dt = lam_imag * step_size
    bar_real = magnitude * jnp.cos(angle_dt)
    bar_imag = magnitude * jnp.sin(angle_dt)
    minus_real = bar_real - 1.0
    modulus = lam_real * lam_real + lam_imag * lam_imag
    ratio_real = (minus_real * lam_real + bar_imag * lam_imag) / modulus
    ratio_imag = (bar_imag * lam_real - minus_real * lam_imag) / modulus
    in_real = b_in[..., :entries]
    in_imag = b_in[..., entries:]
    input_matrix_real = ratio_real[:, None, :] * in_real - ratio_imag[:, None, :] * in_imag
    input_matrix_imag = ratio_real[:, None, :] * in_imag + ratio_imag[:, None, :] * in_real
    forcing_real = jnp.einsum('rxf,xfb->rxb', input_rows, input_matrix_real, precision=top_precision)
    forcing_imag = jnp.einsum('rxf,xfb->rxb', input_rows, input_matrix_imag, precision=top_precision)
    old_real = state[..., :entries]
    old_imag = state[..., entries:]
    following_real = bar_real * old_real - bar_imag * old_imag + forcing_real
    following_imag = bar_real * old_imag + bar_imag * old_real + forcing_imag
    output_real = c_out[..., :entries]
    output_imag = c_out[..., entries:]
    output_matrix = jnp.einsum('lzt,zft->lzf', following_real, output_real, precision=top_precision)
    output_matrix = output_matrix - jnp.einsum('lzt,zft->lzf', following_imag, output_imag, precision=top_precision)
    output_matrix = output_matrix + skip.reshape(group_count, width) * input_rows
    activated = jax.nn.gelu(output_matrix).reshape(seq_count, group_count * width)
    return (activated, jnp.concatenate([following_real, following_imag], axis=-1))

def route_weights(normed, routes, w_group, w_expert):
    group_total = w_group.shape[1]
    expert_total = w_expert.shape[1]
    per_group = expert_total // group_total
    group_logit = jnp.dot(normed, w_group, preferred_element_type=jnp.float32)
    group_exp = jnp.exp(group_logit)
    group_prob = group_exp / lax.optimization_barrier(jnp.sum(group_exp, -1, keepdims=True))
    chosen = routes[:, 0] // per_group
    group_pick = lax.optimization_barrier(jnp.sum(jnp.where(chosen[:, None] == jnp.arange(group_total, dtype=jnp.int32)[None, :], group_prob, 0.0), -1))
    expert_logit = jnp.dot(normed, w_expert, preferred_element_type=jnp.float32)
    picked = lax.optimization_barrier(jnp.sum(jnp.where(routes[:, :, None] == jnp.arange(expert_total, dtype=jnp.int32)[None, None, :], expert_logit[:, None, :], 0.0), -1))
    pair_exp = jnp.exp(picked)
    return pair_exp / lax.optimization_barrier(jnp.sum(pair_exp, -1, keepdims=True)) * group_pick[:, None]

def reference(x_in, state, routes, w_in, decay_rate, frequency, log_step, b_in, c_out, skip, w_out, gain_mix, w_group, w_expert, w_gate, w_up, w_down, gain_moe):
    mix_input = jnp.dot(x_in, w_in, preferred_element_type=jnp.float32).astype(jnp.bfloat16)
    activated, new_state = s5_advance(mix_input, state, decay_rate, frequency, log_step, b_in, c_out, skip)
    mix_act = activated.astype(jnp.bfloat16)
    block_parts = jnp.einsum('ntc,tcd->ntd', mix_act.astype(jnp.float32).reshape(SEQS, N_TP, MIX_DEV), w_out.astype(jnp.float32).reshape(N_TP, MIX_DEV, D))
    block_parts = lax.optimization_barrier(block_parts.astype(jnp.bfloat16))
    mixed = lax.optimization_barrier(jnp.sum(block_parts.astype(jnp.float32), axis=1))
    hidden_state = normalize(residual_scale * x_in.astype(jnp.float32) + mixed, gain_mix)
    hidden_bf = hidden_state.astype(jnp.bfloat16)
    route_weight = route_weights(hidden_bf, routes, w_group, w_expert)
    block_routes = routes.reshape(N_EP, SEQ_DEV, TOP)
    hits = (block_routes[..., None] == jnp.arange(EXPERTS, dtype=jnp.int32)).astype(jnp.int32)
    tally = lax.optimization_barrier(jnp.sum(hits, axis=2))
    prior = jnp.cumsum(tally, axis=1) - tally
    slot_in_block = lax.optimization_barrier(jnp.sum(prior[:, :, None, :] * hits, axis=-1))
    block_index = jnp.arange(N_EP, dtype=jnp.int32)[:, None, None]
    position = (block_index * CAP + slot_in_block).reshape(-1).astype(jnp.int32)
    expert_flat = routes.reshape(-1).astype(jnp.int32)
    row_copies = jnp.broadcast_to(hidden_bf[:, None, :], (SEQS, TOP, D)).reshape(SEQS * TOP, D)
    buffer = jnp.zeros((EXPERTS, N_EP * CAP, D), jnp.bfloat16).at[expert_flat, position].set(row_copies)

    def one_expert(operands):
        slot_rows, gate_weight, up_weight, down_weight = operands
        gate_val = jnp.dot(slot_rows, gate_weight, preferred_element_type=jnp.float32)
        up_val = jnp.dot(slot_rows, up_weight, preferred_element_type=jnp.float32)
        act = (jax.nn.silu(gate_val) * up_val).astype(jnp.bfloat16)
        pieces = jnp.einsum('rtf,tfd->rtd', act.astype(jnp.float32).reshape(N_EP * CAP, N_TP, FF_DEV), down_weight.astype(jnp.float32).reshape(N_TP, FF_DEV, D))
        pieces = lax.optimization_barrier(pieces.astype(jnp.bfloat16))
        return lax.optimization_barrier(jnp.sum(pieces.astype(jnp.float32), axis=1)).astype(jnp.bfloat16)
    outputs = lax.map(one_expert, (buffer, w_gate, w_up, w_down))
    expert_out = outputs[expert_flat, position].reshape(SEQS, TOP, D).astype(jnp.float32)
    moe = lax.optimization_barrier(jnp.sum(route_weight[:, :, None] * expert_out, axis=1))
    layer_out = normalize(residual_scale * hidden_state + moe, gain_moe).astype(jnp.bfloat16)
    return (layer_out, new_state)
```

```python
import jax
import jax.numpy as jnp
from jax import lax
from jax.sharding import PartitionSpec as P

residual_scale = 8.0**0.25
norm_eps = 1e-05


def exchange(x, axis):
    return lax.all_to_all(x, axis, 0, 0, tiled=True)


def to_all(x, axis):
    return exchange(jnp.broadcast_to(x[None], (lax.axis_size(axis), *x.shape)), axis)


def normalize(values, gain, axes):
    centre = jnp.mean(values, axes, keepdims=True)
    spread = jnp.mean(jnp.square(values - centre), axes, keepdims=True)
    return (values - centre) * lax.rsqrt(spread + norm_eps) * gain


def s5_advance(mix_input, state, decay_rate, frequency, log_step, b_in, c_out, skip):
    entries = decay_rate.shape[-1]
    group_count = decay_rate.shape[0]
    width = b_in.shape[1]
    seq_count = mix_input.shape[0]
    input_rows = mix_input.astype(jnp.float32).reshape(seq_count, group_count, width)
    step_size = jnp.exp(log_step)[:, None]
    lam_real = -decay_rate
    magnitude = jnp.exp(lam_real * step_size)
    angle_dt = frequency * step_size
    bar_real = magnitude * jnp.cos(angle_dt)
    bar_imag = magnitude * jnp.sin(angle_dt)
    minus_real = bar_real - 1.0
    modulus = lam_real * lam_real + frequency * frequency
    ratio_real = (minus_real * lam_real + bar_imag * frequency) / modulus
    ratio_imag = (bar_imag * lam_real - minus_real * frequency) / modulus
    in_real = b_in[..., :entries]
    in_imag = b_in[..., entries:]
    input_matrix_real = ratio_real[:, None, :] * in_real - ratio_imag[:, None, :] * in_imag
    input_matrix_imag = ratio_real[:, None, :] * in_imag + ratio_imag[:, None, :] * in_real
    forcing_real = jnp.einsum("rxf,xfb->rxb", input_rows, input_matrix_real)
    forcing_imag = jnp.einsum("rxf,xfb->rxb", input_rows, input_matrix_imag)
    old_real = state[..., :entries]
    old_imag = state[..., entries:]
    following_real = bar_real * old_real - bar_imag * old_imag + forcing_real
    following_imag = bar_real * old_imag + bar_imag * old_real + forcing_imag
    output_matrix = jnp.einsum("lzt,zft->lzf", following_real, c_out[..., :entries])
    output_matrix = output_matrix - jnp.einsum(
        "lzt,zft->lzf", following_imag, c_out[..., entries:]
    )
    output_matrix = output_matrix + skip.reshape(group_count, width) * input_rows
    activated = jax.nn.gelu(output_matrix).reshape(seq_count, group_count * width)
    return (activated, jnp.concatenate([following_real, following_imag], axis=-1))


def route_weights(normed, routes, w_group, w_expert):
    group_total = w_group.shape[1]
    expert_total = w_expert.shape[1]
    per_group = expert_total // group_total
    group_logit = jnp.dot(normed, w_group, preferred_element_type=jnp.float32)
    group_exp = jnp.exp(group_logit)
    group_prob = group_exp / jnp.sum(group_exp, -1, keepdims=True)
    chosen = routes[:, 0] // per_group
    group_pick = jnp.sum(
        jnp.where(
            chosen[:, None] == jnp.arange(group_total, dtype=jnp.int32)[None, :], group_prob, 0.0
        ),
        -1,
    )
    expert_logit = jnp.dot(normed, w_expert, preferred_element_type=jnp.float32)
    picked = jnp.sum(
        jnp.where(
            routes[:, :, None] == jnp.arange(expert_total, dtype=jnp.int32)[None, None, :],
            expert_logit[:, None, :],
            0.0,
        ),
        -1,
    )
    pair_exp = jnp.exp(picked)
    return pair_exp / jnp.sum(pair_exp, -1, keepdims=True) * group_pick[:, None]


def slots_of(routes, expert_total, capacity):
    hits = (routes[:, :, None] == jnp.arange(expert_total, dtype=jnp.int32)[None, None, :]).astype(
        jnp.int32
    )
    tally = jnp.sum(hits, axis=1)
    prior = jnp.cumsum(tally, axis=0) - tally
    return routes * capacity + jnp.sum(prior[:, None, :] * hits, axis=-1)


def layer(
    x_in,
    state,
    routes,
    w_in,
    decay_rate,
    frequency,
    log_step,
    b_in,
    c_out,
    skip,
    w_out,
    gain_mix,
    w_group,
    w_expert,
    w_gate,
    w_up,
    w_down,
    gain_moe,
):
    seq_count, model_width = x_in.shape
    shares = lax.axis_size("tp")
    share = model_width // shares
    expert_total = w_expert.shape[1]
    ep_count = lax.axis_size("ep")
    local_experts, _, hidden = w_gate.shape
    capacity = max(2, 4 * seq_count // expert_total)
    total_slots = expert_total * capacity
    local_slots = local_experts * capacity

    target = slots_of(routes, expert_total, capacity)
    slot_ids = jnp.arange(total_slots, dtype=jnp.int32)
    dispatch_map = jnp.any(slot_ids[:, None, None] == target[None, :, :], axis=-1).astype(
        jnp.bfloat16
    )

    mix_input = jnp.dot(x_in, w_in, preferred_element_type=jnp.float32).astype(jnp.bfloat16)
    activated, new_state = s5_advance(
        mix_input, state, decay_rate, frequency, log_step, b_in, c_out, skip
    )
    activated = activated.astype(jnp.bfloat16)
    partial_mix = jnp.stack(
        [
            jnp.dot(
                activated, w_out[:, k * share : (k + 1) * share], preferred_element_type=jnp.float32
            ).astype(jnp.bfloat16)
            for k in range(shares)
        ]
    )
    mixed = jnp.sum(exchange(partial_mix, "tp").astype(jnp.float32), axis=0)
    x_wide = x_in.astype(jnp.float32)
    x_own = lax.dynamic_slice_in_dim(x_in, lax.axis_index("tp") * share, share, 1)
    x_mean = jnp.mean(x_wide, -1, keepdims=True)
    own = (residual_scale * (x_own.astype(jnp.float32) - x_mean) + mixed).astype(jnp.bfloat16)

    sent = jnp.dot(dispatch_map, own, preferred_element_type=jnp.float32).astype(jnp.bfloat16)
    rows = exchange(sent.reshape(ep_count, local_slots, share), "ep")

    here = lax.axis_index("tp")
    parts = [own] + [
        lax.ppermute(own, "tp", [(i, (i + k) % shares) for i in range(shares)])
        for k in range(1, shares)
    ]
    whole = jnp.stack(parts)[(here - jnp.arange(shares)) % shares].astype(jnp.float32)
    gain_mix = gain_mix.reshape(shares, 1, share)
    hidden_state = normalize(whole, gain_mix, (0, 2))
    hidden_bf = hidden_state.astype(jnp.bfloat16)
    hidden_rows = jnp.concatenate([hidden_bf[k] for k in range(shares)], axis=-1)
    route_weight = route_weights(hidden_rows, routes, w_group, w_expert)
    matches = target[:, :, None] == slot_ids[None, None, :]
    combine_map = jnp.sum(jnp.where(matches, route_weight[:, :, None], 0.0), axis=1)

    piece = to_all(rows.reshape(total_slots, share), "tp").astype(jnp.float32)
    piece = normalize(piece, gain_mix, (0, 2)).astype(jnp.bfloat16)
    piece = jnp.concatenate([piece[k] for k in range(shares)], axis=-1)
    expert_of = (jnp.arange(total_slots, dtype=jnp.int32) % local_slots) // capacity
    acts = []
    for j in range(local_experts):
        gate_part = jnp.dot(piece, w_gate[j], preferred_element_type=jnp.float32)
        up_part = jnp.dot(piece, w_up[j], preferred_element_type=jnp.float32)
        act = jax.nn.silu(gate_part) * up_part
        acts.append(jnp.where((expert_of == j)[:, None], act, 0.0).astype(jnp.bfloat16))
    act = jnp.concatenate(acts, axis=-1)
    down = w_down.reshape(local_experts * hidden, model_width)
    partial_out = jnp.stack(
        [
            jnp.dot(
                act, down[:, k * share : (k + 1) * share], preferred_element_type=jnp.float32
            ).astype(jnp.bfloat16)
            for k in range(shares)
        ]
    )
    summed = jnp.sum(exchange(partial_out, "tp").astype(jnp.float32), axis=0)
    returned = exchange(summed.astype(jnp.bfloat16).reshape(ep_count, local_slots, share), "ep")
    moe_own = jnp.dot(
        combine_map.astype(jnp.bfloat16),
        returned.reshape(total_slots, share),
        preferred_element_type=jnp.float32,
    )
    moe = to_all(moe_own.astype(jnp.bfloat16), "tp").astype(jnp.float32)
    out = normalize(
        residual_scale * hidden_state + moe, gain_moe.reshape(shares, 1, share), (0, 2)
    ).astype(jnp.bfloat16)
    return (jnp.concatenate([out[k] for k in range(shares)], axis=-1), new_state)


def solution(mesh):
    in_specs = (
        P(("grp", "ep"), None),
        P(("grp", "ep"), "tp", None),
        P(("grp", "ep"), None),
        P(None, "tp"),
        P("tp", None),
        P("tp", None),
        P("tp"),
        P("tp", None, None),
        P("tp", None, None),
        P("tp"),
        P("tp", None),
        P(),
        P(),
        P(),
        P("ep", None, "tp"),
        P("ep", None, "tp"),
        P("ep", "tp", None),
        P(),
    )
    out_specs = (P(("grp", "ep"), None), P(("grp", "ep"), "tp", None))
    return jax.shard_map(layer, mesh=mesh, in_specs=in_specs, out_specs=out_specs, check_vma=False)
```

```python
import jax
import jax.numpy as jnp
from jax import lax
from jax.experimental import pallas as pl
from jax.experimental.pallas import tpu as pltpu
from jax.sharding import PartitionSpec as P

residual_scale = 8.0**0.25
norm_eps = 1e-05


def exchange(x, axis):
    return lax.all_to_all(x, axis, 0, 0, tiled=True)


def shifted(pieces, axis):
    size = lax.axis_size(axis)
    return [pieces[0]] + [
        lax.ppermute(pieces[k], axis, [(i, (i + k) % size) for i in range(size)])
        for k in range(1, size)
    ]


def normalize(values, gain, axes):
    centre = jnp.mean(values, axes, keepdims=True)
    spread = jnp.mean(jnp.square(values - centre), axes, keepdims=True)
    return (values - centre) * lax.rsqrt(spread + norm_eps) * gain


def s5_advance(mix_input, state, decay_rate, frequency, log_step, b_in, c_out, skip):
    entries = decay_rate.shape[-1]
    group_count = decay_rate.shape[0]
    width = b_in.shape[1]
    seq_count = mix_input.shape[0]
    input_rows = mix_input.astype(jnp.float32).reshape(seq_count, group_count, width)
    step_size = jnp.exp(log_step)[:, None]
    lam_real = -decay_rate
    magnitude = jnp.exp(lam_real * step_size)
    angle_dt = frequency * step_size
    bar_real = magnitude * jnp.cos(angle_dt)
    bar_imag = magnitude * jnp.sin(angle_dt)
    minus_real = bar_real - 1.0
    modulus = lam_real * lam_real + frequency * frequency
    ratio_real = (minus_real * lam_real + bar_imag * frequency) / modulus
    ratio_imag = (bar_imag * lam_real - minus_real * frequency) / modulus
    in_real = b_in[..., :entries]
    in_imag = b_in[..., entries:]
    input_matrix_real = ratio_real[:, None, :] * in_real - ratio_imag[:, None, :] * in_imag
    input_matrix_imag = ratio_real[:, None, :] * in_imag + ratio_imag[:, None, :] * in_real
    forcing_real = jnp.einsum("rxf,xfb->rxb", input_rows, input_matrix_real)
    forcing_imag = jnp.einsum("rxf,xfb->rxb", input_rows, input_matrix_imag)
    old_real = state[..., :entries]
    old_imag = state[..., entries:]
    following_real = bar_real * old_real - bar_imag * old_imag + forcing_real
    following_imag = bar_real * old_imag + bar_imag * old_real + forcing_imag
    output_matrix = jnp.einsum("lzt,zft->lzf", following_real, c_out[..., :entries])
    output_matrix = output_matrix - jnp.einsum(
        "lzt,zft->lzf", following_imag, c_out[..., entries:]
    )
    output_matrix = output_matrix + skip.reshape(group_count, width) * input_rows
    activated = jax.nn.gelu(output_matrix).reshape(seq_count, group_count * width)
    return (activated, jnp.concatenate([following_real, following_imag], axis=-1))


def route_weights(logits, routes, group_total):
    expert_total = logits.shape[1] - group_total
    per_group = expert_total // group_total
    group_logit = logits[:, :group_total]
    group_exp = jnp.exp(group_logit)
    group_prob = group_exp / jnp.sum(group_exp, -1, keepdims=True)
    chosen = routes[:, 0] // per_group
    group_pick = jnp.sum(
        jnp.where(
            chosen[:, None] == jnp.arange(group_total, dtype=jnp.int32)[None, :], group_prob, 0.0
        ),
        -1,
    )
    expert_logit = logits[:, group_total:]
    picked = jnp.sum(
        jnp.where(
            routes[:, :, None] == jnp.arange(expert_total, dtype=jnp.int32)[None, None, :],
            expert_logit[:, None, :],
            0.0,
        ),
        -1,
    )
    pair_exp = jnp.exp(picked)
    return pair_exp / jnp.sum(pair_exp, -1, keepdims=True) * group_pick[:, None]


def slots_of(routes, expert_total, capacity):
    hits = (routes[:, :, None] == jnp.arange(expert_total, dtype=jnp.int32)[None, None, :]).astype(
        jnp.int32
    )
    tally = jnp.sum(hits, axis=1)
    prior = jnp.cumsum(tally, axis=0) - tally
    return routes * capacity + jnp.sum(prior[:, None, :] * hits, axis=-1)


def experts(here, pieces, gain, w_gate, w_up, w_down, capacity):
    slots, share = pieces[0].shape
    shares = len(pieces)
    local_experts, width, hidden = w_gate.shape
    chunk = 32

    def kernel(here_ref, *refs):
        piece_refs = refs[:shares]
        gain_ref, gate_ref, up_ref, down_ref = refs[shares : shares + 4]
        out_refs = refs[shares + 4 : 2 * shares + 4]
        row_ref, act_ref, gate_near, up_near, down_near, sems = refs[2 * shares + 4 :]
        t = here_ref[0]
        copies = []
        for j in range(local_experts):
            copies.append(pltpu.make_async_copy(gate_ref.at[j], gate_near.at[j], sems.at[2 * j]))
            copies.append(pltpu.make_async_copy(up_ref.at[j], up_near.at[j], sems.at[2 * j + 1]))
        copies.append(pltpu.make_async_copy(down_ref, down_near, sems.at[2 * local_experts]))
        for copy in copies:
            copy.start()
        froms = [lax.rem(t + shares - k, shares) for k in range(shares)]

        def norm_rows(i, carry):
            rows = pl.ds(pl.multiple_of(i * chunk, chunk), chunk)
            values = [r[rows, :].astype(jnp.float32) for r in piece_refs]
            total = values[0]
            for v in values[1:]:
                total = total + v
            centre = jnp.sum(total, -1, keepdims=True) / width
            values = [v - centre for v in values]
            total = values[0] * values[0]
            for v in values[1:]:
                total = total + v * v
            scale = lax.rsqrt(jnp.sum(total, -1, keepdims=True) / width + norm_eps)
            for k, v in enumerate(values):
                columns = pl.ds(pl.multiple_of(froms[k] * share, share), share)
                row_ref[rows, columns] = (v * scale * gain_ref[froms[k]]).astype(jnp.bfloat16)
            return carry

        lax.fori_loop(0, slots // chunk, norm_rows, 0)
        slot = lax.broadcasted_iota(jnp.int32, (slots, hidden), 0)
        expert_of = lax.rem(slot, local_experts * capacity) // capacity
        for j in range(local_experts):
            rows = row_ref[...]
            copies[2 * j].wait()
            gate_part = jnp.dot(rows, gate_near[j], preferred_element_type=jnp.float32)
            copies[2 * j + 1].wait()
            up_part = jnp.dot(rows, up_near[j], preferred_element_type=jnp.float32)
            act = gate_part * jax.nn.sigmoid(gate_part) * up_part
            act_ref[:, j * hidden : (j + 1) * hidden] = jnp.where(
                expert_of == j, act, 0.0
            ).astype(jnp.bfloat16)
        copies[-1].wait()
        for k in (1, shares - 1, *range(2, shares - 1), 0):
            to = lax.rem(t + k, shares)
            columns = pl.ds(pl.multiple_of(to * share, share), share)
            out_refs[k][...] = jnp.dot(
                act_ref[...], down_near[:, columns], preferred_element_type=jnp.float32
            ).astype(jnp.bfloat16)

    vmem = pl.BlockSpec(memory_space=pltpu.VMEM)
    return pl.pallas_call(
        kernel,
        in_specs=[pl.BlockSpec(memory_space=pltpu.SMEM)]
        + [vmem] * (shares + 1)
        + [pl.BlockSpec(memory_space=pltpu.HBM)] * 3,
        out_specs=[vmem] * shares,
        out_shape=[jax.ShapeDtypeStruct((slots, share), jnp.bfloat16)] * shares,
        scratch_shapes=[
            pltpu.VMEM((slots, width), jnp.bfloat16),
            pltpu.VMEM((slots, local_experts * hidden), jnp.bfloat16),
            pltpu.VMEM(w_gate.shape, w_gate.dtype),
            pltpu.VMEM(w_up.shape, w_up.dtype),
            pltpu.VMEM(w_down.shape, w_down.dtype),
            pltpu.SemaphoreType.DMA((2 * local_experts + 1,)),
        ],
        compiler_params=pltpu.CompilerParams(vmem_limit_bytes=24 * 1024 * 1024),
        name="experts",
    )(here, *pieces, gain, w_gate, w_up, w_down)


def finish(here, hidden, pieces, gain):
    rows, share = pieces[0].shape
    shares = len(pieces)
    width = shares * share

    def kernel(here_ref, hidden_ref, *refs):
        piece_refs = refs[:shares]
        gain_ref, out_ref = refs[shares:]
        t = here_ref[0]
        froms = [lax.rem(t + shares - k, shares) for k in range(shares)]
        values = [
            residual_scale * hidden_ref[k] + piece_refs[k][...].astype(jnp.float32)
            for k in range(shares)
        ]
        total = values[0]
        for v in values[1:]:
            total = total + v
        centre = jnp.sum(total, -1, keepdims=True) / width
        values = [v - centre for v in values]
        total = values[0] * values[0]
        for v in values[1:]:
            total = total + v * v
        scale = lax.rsqrt(jnp.sum(total, -1, keepdims=True) / width + norm_eps)
        for k, v in enumerate(values):
            columns = pl.ds(pl.multiple_of(froms[k] * share, share), share)
            out_ref[:, columns] = (v * scale * gain_ref[froms[k]]).astype(jnp.bfloat16)

    vmem = pl.BlockSpec(memory_space=pltpu.VMEM)
    return pl.pallas_call(
        kernel,
        in_specs=[pl.BlockSpec(memory_space=pltpu.SMEM)] + [vmem] * (shares + 2),
        out_specs=vmem,
        out_shape=jax.ShapeDtypeStruct((rows, width), jnp.bfloat16),
        compiler_params=pltpu.CompilerParams(vmem_limit_bytes=8 * 1024 * 1024),
        name="finish",
    )(here, hidden, *pieces, gain)


def layer(
    x_in,
    state,
    routes,
    w_in,
    decay_rate,
    frequency,
    log_step,
    b_in,
    c_out,
    skip,
    w_out,
    gain_mix,
    w_group,
    w_expert,
    w_gate,
    w_up,
    w_down,
    gain_moe,
):
    seq_count, model_width = x_in.shape
    shares = lax.axis_size("tp")
    share = model_width // shares
    expert_total = w_expert.shape[1]
    ep_count = lax.axis_size("ep")
    local_experts, _, hidden = w_gate.shape
    capacity = max(2, 4 * seq_count // expert_total)
    total_slots = expert_total * capacity
    local_slots = local_experts * capacity
    here = lax.axis_index("tp")
    here_array = here.astype(jnp.int32).reshape(1)

    target = slots_of(routes, expert_total, capacity)
    slot_ids = jnp.arange(total_slots, dtype=jnp.int32)
    dispatch_map = jnp.any(slot_ids[:, None, None] == target[None, :, :], axis=-1).astype(
        jnp.bfloat16
    )

    mix_input = jnp.dot(x_in, w_in, preferred_element_type=jnp.float32).astype(jnp.bfloat16)
    activated, new_state = s5_advance(
        mix_input, state, decay_rate, frequency, log_step, b_in, c_out, skip
    )
    partial_mix = jnp.dot(
        activated.astype(jnp.bfloat16), w_out, preferred_element_type=jnp.float32
    ).astype(jnp.bfloat16)

    def own_columns(values, k):
        return lax.dynamic_slice_in_dim(values, ((here + k) % shares) * share, share, 1)

    arrived = shifted([own_columns(partial_mix, k) for k in range(shares)], "tp")
    mixed = sum(a.astype(jnp.float32) for a in arrived)
    x_mean = jnp.mean(x_in.astype(jnp.float32), -1, keepdims=True)
    x_own = own_columns(x_in, 0).astype(jnp.float32)
    own = (residual_scale * (x_own - x_mean) + mixed).astype(jnp.bfloat16)

    sent = jnp.dot(dispatch_map, own, preferred_element_type=jnp.float32).astype(jnp.bfloat16)
    rows = exchange(sent.reshape(ep_count, local_slots, share), "ep")

    parts = shifted([own] * shares, "tp")
    whole = jnp.stack(parts).astype(jnp.float32)
    order = (here - jnp.arange(shares)) % shares
    gain_mix = gain_mix.reshape(shares, 1, share)
    hidden_state = normalize(whole, gain_mix[order], (0, 2))
    hidden_bf = hidden_state.astype(jnp.bfloat16)
    w_router = jnp.concatenate([w_group, w_expert], axis=-1).reshape(shares, share, -1)[order]
    logits = jnp.einsum("krd,kde->re", hidden_bf, w_router, preferred_element_type=jnp.float32)
    route_weight = route_weights(logits, routes, w_group.shape[1])
    matches = target[:, :, None] == slot_ids[None, None, :]
    combine_map = jnp.sum(jnp.where(matches, route_weight[:, :, None], 0.0), axis=1)

    rows = rows.reshape(total_slots, share)
    pieces = shifted([rows] * shares, "tp")
    w_down = w_down.reshape(local_experts * hidden, model_width)
    weights = [pltpu.with_memory_space_constraint(w, pltpu.HBM) for w in (w_gate, w_up, w_down)]
    outs = experts(here_array, pieces, gain_mix, *weights, capacity)
    arrived = shifted(outs, "tp")
    summed = sum(a.astype(jnp.float32) for a in arrived).astype(jnp.bfloat16)
    returned = exchange(summed.reshape(ep_count, local_slots, share), "ep")
    moe_own = jnp.dot(
        combine_map.astype(jnp.bfloat16),
        returned.reshape(total_slots, share),
        preferred_element_type=jnp.float32,
    ).astype(jnp.bfloat16)
    moe = shifted([moe_own] * shares, "tp")
    out = finish(here_array, hidden_state, moe, gain_moe.reshape(shares, 1, share))
    return (out, new_state)


def solution(mesh):
    in_specs = (
        P(("grp", "ep"), None),
        P(("grp", "ep"), "tp", None),
        P(("grp", "ep"), None),
        P(None, "tp"),
        P("tp", None),
        P("tp", None),
        P("tp"),
        P("tp", None, None),
        P("tp", None, None),
        P("tp"),
        P("tp", None),
        P(),
        P(),
        P(),
        P("ep", None, "tp"),
        P("ep", None, "tp"),
        P("ep", "tp", None),
        P(),
    )
    out_specs = (P(("grp", "ep"), None), P(("grp", "ep"), "tp", None))
    return jax.shard_map(layer, mesh=mesh, in_specs=in_specs, out_specs=out_specs, check_vma=False)
```

```python
import jax
import jax.numpy as jnp
from jax import lax
from jax.experimental import pallas as pl
from jax.experimental.pallas import tpu as pltpu
from jax.sharding import PartitionSpec as P

residual_scale = 8.0**0.25
norm_eps = 1e-05


def exchange(x, axis):
    return lax.all_to_all(x, axis, 0, 0, tiled=True)


def shifted(pieces, axis):
    size = lax.axis_size(axis)
    return [pieces[0]] + [
        lax.ppermute(pieces[k], axis, [(i, (i + k) % size) for i in range(size)])
        for k in range(1, size)
    ]


def normalize(values, gain, axes):
    centre = jnp.mean(values, axes, keepdims=True)
    spread = jnp.mean(jnp.square(values - centre), axes, keepdims=True)
    return (values - centre) * lax.rsqrt(spread + norm_eps) * gain


def route_weights(logits, routes, group_total):
    expert_total = logits.shape[1] - group_total
    per_group = expert_total // group_total
    group_logit = logits[:, :group_total]
    group_exp = jnp.exp(group_logit)
    group_prob = group_exp / jnp.sum(group_exp, -1, keepdims=True)
    chosen = routes[:, 0] // per_group
    group_pick = jnp.sum(
        jnp.where(
            chosen[:, None] == jnp.arange(group_total, dtype=jnp.int32)[None, :], group_prob, 0.0
        ),
        -1,
    )
    expert_logit = logits[:, group_total:]
    picked = jnp.sum(
        jnp.where(
            routes[:, :, None] == jnp.arange(expert_total, dtype=jnp.int32)[None, None, :],
            expert_logit[:, None, :],
            0.0,
        ),
        -1,
    )
    pair_exp = jnp.exp(picked)
    return pair_exp / jnp.sum(pair_exp, -1, keepdims=True) * group_pick[:, None]


def slots_of(routes, expert_total, capacity):
    hits = (routes[:, :, None] == jnp.arange(expert_total, dtype=jnp.int32)[None, None, :]).astype(
        jnp.int32
    )
    tally = jnp.sum(hits, axis=1)
    prior = jnp.cumsum(tally, axis=0) - tally
    return routes * capacity + jnp.sum(prior[:, None, :] * hits, axis=-1)


def ring_places(here_ref, shares):
    t = here_ref[0]
    froms = [lax.rem(t + shares - k, shares) for k in range(shares)]
    tos = [lax.rem(t + k, shares) for k in range(shares)]
    return froms, tos


def columns_of(place, share):
    return pl.ds(pl.multiple_of(place * share, share), share)


def near(ref):
    return pltpu.VMEM(ref.shape, ref.dtype)


def mixer(here, x_in, state, w_in, decay_rate, frequency, log_step, b_in, c_out, skip, w_out):
    seq_count, width = x_in.shape
    channels = w_in.shape[1]
    groups, entries = decay_rate.shape
    per_group = b_in.shape[1]
    lanes = 2 * entries
    shares = lax.axis_size("tp")
    share = width // shares
    together = lanes // per_group
    cut = 4
    arrays = (decay_rate, frequency, log_step, x_in, w_in, b_in, state, c_out, skip, w_out)

    def kernel(here_ref, *refs):
        far = refs[: len(arrays)]
        base_ref = refs[len(arrays)]
        part_refs = refs[len(arrays) + 1 : len(arrays) + shares]
        new_far = refs[len(arrays) + shares]
        rest = refs[len(arrays) + shares + 1 :]
        close = rest[: len(arrays)]
        decay_ref, freq_ref, log_ref, x_ref, w_in_ref, b_ref, state_ref, c_ref, skip_ref, w_out_ref = close
        new_ref, in_ref, out_ref, act_ref, sems = rest[len(arrays) :]
        _, tos = ring_places(here_ref, shares)
        piece = width // cut
        copies = {}
        for i, (a, b) in enumerate(zip(far, close)):
            if i == 4:
                for q in range(cut):
                    rows = slice(q * piece, (q + 1) * piece)
                    copies[i, q] = pltpu.make_async_copy(
                        a.at[rows], b.at[rows], sems.at[len(arrays) + q]
                    )
            else:
                copies[i] = pltpu.make_async_copy(a, b, sems.at[i])
        for copy in copies.values():
            copy.start()

        lane = lax.broadcasted_iota(jnp.int32, (1, lanes), 1)
        sign = jnp.where(lane < entries, -1.0, 1.0)
        for i in (0, 1, 2):
            copies[i].wait()
        eye = lax.broadcasted_iota(jnp.int32, (groups, groups), 0) == lax.broadcasted_iota(
            jnp.int32, (groups, groups), 1
        )
        log_column = jnp.sum(jnp.where(eye, log_ref[...], 0.0), -1, keepdims=True)
        step_size = jnp.exp(log_column)
        lam_real = -decay_ref[...]
        freq = freq_ref[...]
        magnitude = jnp.exp(lam_real * step_size)
        angle = freq * step_size
        bar_real = magnitude * jnp.cos(angle)
        bar_imag = magnitude * jnp.sin(angle)
        minus_real = bar_real - 1.0
        modulus = lam_real * lam_real + freq * freq
        ratio_real = (minus_real * lam_real + bar_imag * freq) / modulus
        ratio_imag = (bar_imag * lam_real - minus_real * freq) / modulus

        def twice(v):
            return jnp.concatenate([v, v], axis=-1)

        bar_real = twice(bar_real)
        bar_imag = twice(bar_imag) * sign
        ratio_real = twice(ratio_real)
        ratio_imag = twice(ratio_imag) * sign

        copies[3].wait()
        x_wide = x_ref[...].astype(jnp.float32)
        x_mean = jnp.sum(x_wide, -1, keepdims=True) / width
        x_own = x_ref[:, columns_of(here_ref[0], share)].astype(jnp.float32)
        base_ref[...] = residual_scale * (x_own - x_mean)
        copies[5].wait()
        for g in range(groups):
            b = b_ref[g]
            in_ref[g * per_group : (g + 1) * per_group, :] = (
                ratio_real[g : g + 1] * b + ratio_imag[g : g + 1] * pltpu.roll(b, entries, 1)
            ).astype(jnp.bfloat16)
        copies[7].wait()
        for g in range(groups):
            out_ref[g * per_group : (g + 1) * per_group, :] = (c_ref[g] * -sign).astype(jnp.bfloat16)
        mix = None
        for q in range(cut):
            copies[4, q].wait()
            rows = slice(q * piece, (q + 1) * piece)
            term = jnp.dot(x_ref[:, rows], w_in_ref[rows, :], preferred_element_type=jnp.float32)
            mix = term if mix is None else mix + term
        mix = mix.astype(jnp.bfloat16).astype(jnp.float32)
        copies[6].wait()
        copies[8].wait()
        old = state_ref.reshape(seq_count * groups, lanes)
        new = new_ref.reshape(seq_count * groups, lanes)
        lane_group = lane // per_group
        for j in range(groups // together):
            span = slice(j * lanes, (j + 1) * lanes)
            inputs = mix[:, span]
            spread = jnp.concatenate(
                [jnp.where(lane_group == g, inputs, 0.0) for g in range(together)], axis=0
            ).astype(jnp.bfloat16)
            forcing = jnp.dot(spread, in_ref[span, :], preferred_element_type=jnp.float32)
            held = []
            for g in range(together):
                at = j * together + g
                rows = pl.ds(at, seq_count, stride=groups)
                h = old[rows, :]
                h = (
                    bar_real[at : at + 1] * h
                    + bar_imag[at : at + 1] * pltpu.roll(h, entries, 1)
                    + forcing[g * seq_count : (g + 1) * seq_count]
                )
                new[rows, :] = h
                held.append(h.astype(jnp.bfloat16))
            read = lax.dot_general(
                jnp.concatenate(held, axis=0),
                out_ref[span, :],
                (((1,), (1,)), ((), ())),
                preferred_element_type=jnp.float32,
            )
            value = skip_ref[:, span] * inputs
            for g in range(together):
                value = value + jnp.where(
                    lane_group == g, read[g * seq_count : (g + 1) * seq_count], 0.0
                )
            act_ref[:, span] = jax.nn.gelu(value).astype(jnp.bfloat16)
        send = pltpu.make_async_copy(new_ref, new_far, sems.at[len(arrays) + cut])
        send.start()
        copies[9].wait()
        for k in range(shares):
            part = jnp.dot(
                act_ref[...],
                w_out_ref[:, columns_of(tos[k], share)],
                preferred_element_type=jnp.float32,
            ).astype(jnp.bfloat16)
            if k == 0:
                base_ref[...] += part.astype(jnp.float32)
            else:
                part_refs[k - 1][...] = part
        send.wait()

    vmem = pl.BlockSpec(memory_space=pltpu.VMEM)
    hbm = pl.BlockSpec(memory_space=pltpu.HBM)
    return pl.pallas_call(
        kernel,
        in_specs=[pl.BlockSpec(memory_space=pltpu.SMEM)] + [hbm] * len(arrays),
        out_specs=[vmem] * shares + [hbm],
        out_shape=[jax.ShapeDtypeStruct((seq_count, share), jnp.float32)]
        + [jax.ShapeDtypeStruct((seq_count, share), jnp.bfloat16)] * (shares - 1)
        + [jax.ShapeDtypeStruct(state.shape, state.dtype)],
        scratch_shapes=[near(a) for a in arrays]
        + [
            near(state),
            pltpu.VMEM((channels, lanes), jnp.bfloat16),
            pltpu.VMEM((channels, lanes), jnp.bfloat16),
            pltpu.VMEM((seq_count, channels), jnp.bfloat16),
            pltpu.SemaphoreType.DMA((len(arrays) + cut + 1,)),
        ],
        compiler_params=pltpu.CompilerParams(vmem_limit_bytes=16 * 1024 * 1024),
        name="mixer",
    )(here, *[pltpu.with_memory_space_constraint(a, pltpu.HBM) for a in arrays])


def place_rows(base, arrived, target, total_slots):
    seq_count, share = base.shape

    def kernel(base_ref, target_ref, *refs):
        own_ref, sent_ref = refs[-2:]
        own = base_ref[...]
        for r in refs[:-2]:
            own = own + r[...].astype(jnp.float32)
        own = own.astype(jnp.bfloat16)
        own_ref[...] = own
        slot = lax.broadcasted_iota(jnp.int32, (total_slots, seq_count), 0)
        hit = slot == target_ref[0:1, :]
        for k in range(1, target_ref.shape[0]):
            hit = hit | (slot == target_ref[k : k + 1, :])
        chosen = jnp.where(hit, 1.0, 0.0).astype(jnp.bfloat16)
        sent_ref[...] = jnp.dot(chosen, own, preferred_element_type=jnp.float32).astype(jnp.bfloat16)

    vmem = pl.BlockSpec(memory_space=pltpu.VMEM)
    return pl.pallas_call(
        kernel,
        in_specs=[vmem] * (2 + len(arrived)),
        out_specs=[vmem] * 2,
        out_shape=[
            jax.ShapeDtypeStruct((seq_count, share), jnp.bfloat16),
            jax.ShapeDtypeStruct((total_slots, share), jnp.bfloat16),
        ],
        compiler_params=pltpu.CompilerParams(vmem_limit_bytes=8 * 1024 * 1024),
        name="place_rows",
    )(base, target.T, *arrived)


def fetch(*weights):
    count = len(weights)

    def kernel(*refs):
        copies = [
            pltpu.make_async_copy(refs[i], refs[count + i], refs[-1].at[i]) for i in range(count)
        ]
        for copy in copies:
            copy.start()
        for copy in copies:
            copy.wait()

    return pl.pallas_call(
        kernel,
        in_specs=[pl.BlockSpec(memory_space=pltpu.HBM)] * count,
        out_specs=[pl.BlockSpec(memory_space=pltpu.VMEM)] * count,
        out_shape=[pltpu.VMEM(w.shape, w.dtype) for w in weights],
        scratch_shapes=[pltpu.SemaphoreType.DMA((count,))],
        compiler_params=pltpu.CompilerParams(vmem_limit_bytes=1024 * 1024),
        name="fetch",
    )(*[pltpu.with_memory_space_constraint(w, pltpu.HBM) for w in weights])


def swap_halves(first, second):
    half = first.shape[1] // 2
    low = lax.broadcasted_iota(jnp.int32, first.shape, 1) < half
    return (
        jnp.where(low, first, pltpu.roll(second, half, 1)),
        jnp.where(low, pltpu.roll(first, half, 1), second),
    )


def experts(here, pieces, gain, w_gate, w_up, w_down):
    slots, share = pieces[0].shape
    shares = len(pieces)
    local_experts, width, hidden = w_gate.shape
    tile = 8
    chunk = 4 * tile
    kept = slots // local_experts

    def kernel(here_ref, *refs):
        piece_refs = refs[:shares]
        gain_ref, gate_ref, up_ref, down_ref = refs[shares : shares + 4]
        out_refs = refs[shares + 4 : 2 * shares + 4]
        row_ref, act_ref = refs[2 * shares + 4 :]
        froms, tos = ring_places(here_ref, shares)

        def norm_rows(i, carry):
            rows = pl.ds(pl.multiple_of(i * chunk, chunk), chunk)
            values = [r[rows, :].astype(jnp.float32) for r in piece_refs]
            total = values[0]
            for v in values[1:]:
                total = total + v
            centre = jnp.sum(total, -1, keepdims=True) / width
            values = [v - centre for v in values]
            total = values[0] * values[0]
            for v in values[1:]:
                total = total + v * v
            scale = lax.rsqrt(jnp.sum(total, -1, keepdims=True) / width + norm_eps)
            rows = pl.ds(pl.multiple_of(i * (chunk // 2), chunk // 2), chunk // 2)
            for k, v in enumerate(values):
                v = (v * scale * gain_ref[froms[k]]).reshape(2, 2, tile, share)
                for j, part in enumerate(swap_halves(v[:, 0], v[:, 1])):
                    row_ref[j, rows, columns_of(froms[k], share)] = part.reshape(
                        chunk // 2, share
                    ).astype(jnp.bfloat16)
            return carry

        lax.fori_loop(0, slots // chunk, norm_rows, 0)
        for j in range(local_experts):
            rows = row_ref[j]
            gate_part = jnp.dot(rows, gate_ref[j], preferred_element_type=jnp.float32)
            up_part = jnp.dot(rows, up_ref[j], preferred_element_type=jnp.float32)
            act_ref[j] = (gate_part * jax.nn.sigmoid(gate_part) * up_part).astype(jnp.bfloat16)
        for k in (1, shares - 1, *range(2, shares - 1), 0):
            outs = [
                jnp.dot(
                    act_ref[j],
                    down_ref[j, :, columns_of(tos[k], share)],
                    preferred_element_type=jnp.float32,
                ).reshape(kept // tile, tile, share)
                for j in range(local_experts)
            ]
            both = jnp.stack(swap_halves(*outs), axis=1).reshape(slots, share)
            out_refs[k][...] = both.astype(jnp.bfloat16)

    vmem = pl.BlockSpec(memory_space=pltpu.VMEM)
    return pl.pallas_call(
        kernel,
        in_specs=[pl.BlockSpec(memory_space=pltpu.SMEM)] + [vmem] * (shares + 4),
        out_specs=[vmem] * shares,
        out_shape=[jax.ShapeDtypeStruct((slots, share), jnp.bfloat16)] * shares,
        scratch_shapes=[
            pltpu.VMEM((local_experts, kept, width), jnp.bfloat16),
            pltpu.VMEM((local_experts, kept, hidden), jnp.bfloat16),
        ],
        compiler_params=pltpu.CompilerParams(vmem_limit_bytes=24 * 1024 * 1024),
        name="experts",
    )(here, *pieces, gain, w_gate, w_up, w_down)


def finish(here, hidden, pieces, gain):
    rows, share = pieces[0].shape
    shares = len(pieces)
    width = shares * share

    def kernel(here_ref, hidden_ref, *refs):
        piece_refs = refs[:shares]
        gain_ref, out_ref = refs[shares:]
        froms, _ = ring_places(here_ref, shares)
        values = [
            residual_scale * hidden_ref[k] + piece_refs[k][...].astype(jnp.float32)
            for k in range(shares)
        ]
        total = values[0]
        for v in values[1:]:
            total = total + v
        centre = jnp.sum(total, -1, keepdims=True) / width
        values = [v - centre for v in values]
        total = values[0] * values[0]
        for v in values[1:]:
            total = total + v * v
        scale = lax.rsqrt(jnp.sum(total, -1, keepdims=True) / width + norm_eps)
        for k, v in enumerate(values):
            out_ref[:, columns_of(froms[k], share)] = (v * scale * gain_ref[froms[k]]).astype(jnp.bfloat16)

    vmem = pl.BlockSpec(memory_space=pltpu.VMEM)
    return pl.pallas_call(
        kernel,
        in_specs=[pl.BlockSpec(memory_space=pltpu.SMEM)] + [vmem] * (shares + 2),
        out_specs=vmem,
        out_shape=jax.ShapeDtypeStruct((rows, width), jnp.bfloat16),
        compiler_params=pltpu.CompilerParams(vmem_limit_bytes=8 * 1024 * 1024),
        name="finish",
    )(here, hidden, *pieces, gain)


def layer(
    x_in,
    state,
    routes,
    w_in,
    decay_rate,
    frequency,
    log_step,
    b_in,
    c_out,
    skip,
    w_out,
    gain_mix,
    w_group,
    w_expert,
    w_gate,
    w_up,
    w_down,
    gain_moe,
):
    seq_count, model_width = x_in.shape
    shares = lax.axis_size("tp")
    share = model_width // shares
    expert_total = w_expert.shape[1]
    ep_count = lax.axis_size("ep")
    local_experts = w_gate.shape[0]
    capacity = max(2, 4 * seq_count // expert_total)
    total_slots = expert_total * capacity
    local_slots = local_experts * capacity
    here = lax.axis_index("tp")
    here_array = here.astype(jnp.int32).reshape(1)

    target = slots_of(routes, expert_total, capacity)
    slot_ids = jnp.arange(total_slots, dtype=jnp.int32)

    base, *parts, new_state = mixer(
        here_array,
        x_in,
        state,
        w_in,
        decay_rate,
        frequency,
        log_step.reshape(1, -1),
        b_in,
        c_out,
        skip.reshape(1, -1),
        w_out,
    )
    arrived = shifted([base, *parts], "tp")
    own, sent = place_rows(base, arrived[1:], target, total_slots)
    rows = exchange(sent.reshape(ep_count, local_slots, share), "ep")

    parts = shifted([own] * shares, "tp")
    whole = jnp.stack(parts).astype(jnp.float32)
    order = (here - jnp.arange(shares)) % shares
    gain_mix = gain_mix.reshape(shares, 1, share)
    hidden_state = normalize(whole, gain_mix[order], (0, 2))
    hidden_bf = hidden_state.astype(jnp.bfloat16)
    w_router = jnp.concatenate([w_group, w_expert], axis=-1).reshape(shares, share, -1)[order]
    logits = jnp.einsum("krd,kde->re", hidden_bf, w_router, preferred_element_type=jnp.float32)
    route_weight = route_weights(logits, routes, w_group.shape[1])
    matches = target[:, :, None] == slot_ids[None, None, :]
    combine_map = jnp.sum(jnp.where(matches, route_weight[:, :, None], 0.0), axis=1)

    rows = rows.reshape(total_slots, share)
    pieces = shifted([rows] * shares, "tp")
    weights = fetch(w_gate, w_up, w_down)
    outs = experts(here_array, pieces, gain_mix, *weights)
    arrived = shifted(outs, "tp")
    summed = sum(a.astype(jnp.float32) for a in arrived).astype(jnp.bfloat16)
    returned = exchange(summed.reshape(ep_count, local_slots, share), "ep")
    moe_own = jnp.dot(
        combine_map.astype(jnp.bfloat16),
        returned.reshape(total_slots, share),
        preferred_element_type=jnp.float32,
    ).astype(jnp.bfloat16)
    moe = shifted([moe_own] * shares, "tp")
    out = finish(here_array, hidden_state, moe, gain_moe.reshape(shares, 1, share))
    return (out, new_state)


def solution(mesh):
    in_specs = (
        P(("grp", "ep"), None),
        P(("grp", "ep"), "tp", None),
        P(("grp", "ep"), None),
        P(None, "tp"),
        P("tp", None),
        P("tp", None),
        P("tp"),
        P("tp", None, None),
        P("tp", None, None),
        P("tp"),
        P("tp", None),
        P(),
        P(),
        P(),
        P("ep", None, "tp"),
        P("ep", None, "tp"),
        P("ep", "tp", None),
        P(),
    )
    out_specs = (P(("grp", "ep"), None), P(("grp", "ep"), "tp", None))
    return jax.shard_map(layer, mesh=mesh, in_specs=in_specs, out_specs=out_specs, check_vma=False)
```

```python
import jax
import jax.numpy as jnp
from jax import lax
from jax.experimental import pallas as pl
from jax.experimental.pallas import tpu as pltpu
from jax.sharding import PartitionSpec as P

residual_scale = 8.0**0.25
norm_eps = 1e-05


def exchange(x, axis):
    return lax.all_to_all(x, axis, 0, 0, tiled=True)


def shifted(pieces, axis):
    size = lax.axis_size(axis)
    return [pieces[0]] + [
        lax.ppermute(pieces[k], axis, [(i, (i + k) % size) for i in range(size)])
        for k in range(1, size)
    ]


def normalize(values, gain, axes):
    centre = jnp.mean(values, axes, keepdims=True)
    spread = jnp.mean(jnp.square(values - centre), axes, keepdims=True)
    return (values - centre) * lax.rsqrt(spread + norm_eps) * gain


def route_weights(logits, routes, group_total):
    expert_total = logits.shape[1] - group_total
    per_group = expert_total // group_total
    group_logit = logits[:, :group_total]
    group_exp = jnp.exp(group_logit)
    group_prob = group_exp / jnp.sum(group_exp, -1, keepdims=True)
    chosen = routes[:, 0] // per_group
    group_pick = jnp.sum(
        jnp.where(
            chosen[:, None] == jnp.arange(group_total, dtype=jnp.int32)[None, :], group_prob, 0.0
        ),
        -1,
    )
    expert_logit = logits[:, group_total:]
    picked = jnp.sum(
        jnp.where(
            routes[:, :, None] == jnp.arange(expert_total, dtype=jnp.int32)[None, None, :],
            expert_logit[:, None, :],
            0.0,
        ),
        -1,
    )
    pair_exp = jnp.exp(picked)
    return pair_exp / jnp.sum(pair_exp, -1, keepdims=True) * group_pick[:, None]


def slots_of(routes, expert_total, capacity):
    hits = (routes[:, :, None] == jnp.arange(expert_total, dtype=jnp.int32)[None, None, :]).astype(
        jnp.int32
    )
    tally = jnp.sum(hits, axis=1)
    prior = jnp.cumsum(tally, axis=0) - tally
    return routes * capacity + jnp.sum(prior[:, None, :] * hits, axis=-1)


def ring_places(here_ref, shares):
    t = here_ref[0]
    froms = [lax.rem(t + shares - k, shares) for k in range(shares)]
    tos = [lax.rem(t + k, shares) for k in range(shares)]
    return froms, tos


def columns_of(place, share):
    return pl.ds(pl.multiple_of(place * share, share), share)


def near(ref):
    return pltpu.VMEM(ref.shape, ref.dtype)


def mixer(here, x_in, state, w_in, decay_rate, frequency, log_step, b_in, c_out, skip, w_out):
    seq_count, width = x_in.shape
    channels = w_in.shape[1]
    groups, entries = decay_rate.shape
    per_group = b_in.shape[1]
    lanes = 2 * entries
    shares = lax.axis_size("tp")
    share = width // shares
    together = lanes // per_group
    cut = 4
    arrays = (decay_rate, frequency, log_step, x_in, w_in, b_in, state, c_out, skip, w_out)

    def kernel(here_ref, *refs):
        far = refs[: len(arrays)]
        base_ref = refs[len(arrays)]
        part_refs = refs[len(arrays) + 1 : len(arrays) + shares]
        new_far = refs[len(arrays) + shares]
        rest = refs[len(arrays) + shares + 1 :]
        close = rest[: len(arrays)]
        decay_ref, freq_ref, log_ref, x_ref, w_in_ref, b_ref, state_ref, c_ref, skip_ref, w_out_ref = close
        new_ref, in_ref, out_ref, act_ref, sems = rest[len(arrays) :]
        _, tos = ring_places(here_ref, shares)
        piece = width // cut
        copies = {}
        for i, (a, b) in enumerate(zip(far, close)):
            if i == 4:
                for q in range(cut):
                    rows = slice(q * piece, (q + 1) * piece)
                    copies[i, q] = pltpu.make_async_copy(
                        a.at[rows], b.at[rows], sems.at[len(arrays) + q]
                    )
            else:
                copies[i] = pltpu.make_async_copy(a, b, sems.at[i])
        for copy in copies.values():
            copy.start()

        lane = lax.broadcasted_iota(jnp.int32, (1, lanes), 1)
        sign = jnp.where(lane < entries, -1.0, 1.0)
        for i in (0, 1, 2):
            copies[i].wait()
        eye = lax.broadcasted_iota(jnp.int32, (groups, groups), 0) == lax.broadcasted_iota(
            jnp.int32, (groups, groups), 1
        )
        log_column = jnp.sum(jnp.where(eye, log_ref[...], 0.0), -1, keepdims=True)
        step_size = jnp.exp(log_column)
        lam_real = -decay_ref[...]
        freq = freq_ref[...]
        magnitude = jnp.exp(lam_real * step_size)
        angle = freq * step_size
        bar_real = magnitude * jnp.cos(angle)
        bar_imag = magnitude * jnp.sin(angle)
        minus_real = bar_real - 1.0
        modulus = lam_real * lam_real + freq * freq
        ratio_real = (minus_real * lam_real + bar_imag * freq) / modulus
        ratio_imag = (bar_imag * lam_real - minus_real * freq) / modulus

        def twice(v):
            return jnp.concatenate([v, v], axis=-1)

        bar_real = twice(bar_real)
        bar_imag = twice(bar_imag) * sign
        ratio_real = twice(ratio_real)
        ratio_imag = twice(ratio_imag) * sign

        copies[3].wait()
        x_wide = x_ref[...].astype(jnp.float32)
        x_mean = jnp.sum(x_wide, -1, keepdims=True) / width
        x_own = x_ref[:, columns_of(here_ref[0], share)].astype(jnp.float32)
        base_ref[...] = residual_scale * (x_own - x_mean)
        copies[5].wait()
        for g in range(groups):
            b = b_ref[g]
            in_ref[g * per_group : (g + 1) * per_group, :] = (
                ratio_real[g : g + 1] * b + ratio_imag[g : g + 1] * pltpu.roll(b, entries, 1)
            ).astype(jnp.bfloat16)
        copies[7].wait()
        for g in range(groups):
            out_ref[g * per_group : (g + 1) * per_group, :] = (c_ref[g] * -sign).astype(jnp.bfloat16)
        mix = None
        for q in range(cut):
            copies[4, q].wait()
            rows = slice(q * piece, (q + 1) * piece)
            term = jnp.dot(x_ref[:, rows], w_in_ref[rows, :], preferred_element_type=jnp.float32)
            mix = term if mix is None else mix + term
        mix = mix.astype(jnp.bfloat16).astype(jnp.float32)
        copies[6].wait()
        copies[8].wait()
        old = state_ref.reshape(seq_count * groups, lanes)
        new = new_ref.reshape(seq_count * groups, lanes)
        lane_group = lane // per_group
        for j in range(groups // together):
            span = slice(j * lanes, (j + 1) * lanes)
            inputs = mix[:, span]
            spread = jnp.concatenate(
                [jnp.where(lane_group == g, inputs, 0.0) for g in range(together)], axis=0
            ).astype(jnp.bfloat16)
            forcing = jnp.dot(spread, in_ref[span, :], preferred_element_type=jnp.float32)
            held = []
            for g in range(together):
                at = j * together + g
                rows = pl.ds(at, seq_count, stride=groups)
                h = old[rows, :]
                h = (
                    bar_real[at : at + 1] * h
                    + bar_imag[at : at + 1] * pltpu.roll(h, entries, 1)
                    + forcing[g * seq_count : (g + 1) * seq_count]
                )
                new[rows, :] = h
                held.append(h.astype(jnp.bfloat16))
            read = lax.dot_general(
                jnp.concatenate(held, axis=0),
                out_ref[span, :],
                (((1,), (1,)), ((), ())),
                preferred_element_type=jnp.float32,
            )
            value = skip_ref[span] * inputs
            for g in range(together):
                value = value + jnp.where(
                    lane_group == g, read[g * seq_count : (g + 1) * seq_count], 0.0
                )
            act_ref[:, span] = jax.nn.gelu(value).astype(jnp.bfloat16)
        send = pltpu.make_async_copy(new_ref, new_far, sems.at[len(arrays) + cut])
        send.start()
        copies[9].wait()
        for k in range(shares):
            part = jnp.dot(
                act_ref[...],
                w_out_ref[:, columns_of(tos[k], share)],
                preferred_element_type=jnp.float32,
            ).astype(jnp.bfloat16)
            if k == 0:
                base_ref[...] += part.astype(jnp.float32)
            else:
                part_refs[k - 1][...] = part
        send.wait()

    vmem = pl.BlockSpec(memory_space=pltpu.VMEM)
    hbm = pl.BlockSpec(memory_space=pltpu.HBM)
    return pl.pallas_call(
        kernel,
        in_specs=[pl.BlockSpec(memory_space=pltpu.SMEM)] + [hbm] * len(arrays),
        out_specs=[vmem] * shares + [hbm],
        out_shape=[jax.ShapeDtypeStruct((seq_count, share), jnp.float32)]
        + [jax.ShapeDtypeStruct((seq_count, share), jnp.bfloat16)] * (shares - 1)
        + [jax.ShapeDtypeStruct(state.shape, state.dtype)],
        scratch_shapes=[near(a) for a in arrays]
        + [
            near(state),
            pltpu.VMEM((channels, lanes), jnp.bfloat16),
            pltpu.VMEM((channels, lanes), jnp.bfloat16),
            pltpu.VMEM((seq_count, channels), jnp.bfloat16),
            pltpu.SemaphoreType.DMA((len(arrays) + cut + 1,)),
        ],
        compiler_params=pltpu.CompilerParams(vmem_limit_bytes=16 * 1024 * 1024),
        name="mixer",
    )(here, *[pltpu.with_memory_space_constraint(a, pltpu.HBM) for a in arrays])


def place_rows(base, arrived, target, total_slots):
    seq_count, share = base.shape

    def kernel(base_ref, target_ref, *refs):
        own_ref, sent_ref = refs[-2:]
        own = base_ref[...]
        for r in refs[:-2]:
            own = own + r[...].astype(jnp.float32)
        own = own.astype(jnp.bfloat16)
        own_ref[...] = own
        slot = lax.broadcasted_iota(jnp.int32, (total_slots, seq_count), 0)
        hit = slot == target_ref[0:1, :]
        for k in range(1, target_ref.shape[0]):
            hit = hit | (slot == target_ref[k : k + 1, :])
        chosen = jnp.where(hit, 1.0, 0.0).astype(jnp.bfloat16)
        sent_ref[...] = jnp.dot(chosen, own, preferred_element_type=jnp.float32).astype(jnp.bfloat16)

    vmem = pl.BlockSpec(memory_space=pltpu.VMEM)
    return pl.pallas_call(
        kernel,
        in_specs=[vmem] * (2 + len(arrived)),
        out_specs=[vmem] * 2,
        out_shape=[
            jax.ShapeDtypeStruct((seq_count, share), jnp.bfloat16),
            jax.ShapeDtypeStruct((total_slots, share), jnp.bfloat16),
        ],
        compiler_params=pltpu.CompilerParams(vmem_limit_bytes=8 * 1024 * 1024),
        name="place_rows",
    )(base, target.T, *arrived)


def fetch(*weights):
    count = len(weights)

    def kernel(*refs):
        copies = [
            pltpu.make_async_copy(refs[i], refs[count + i], refs[-1].at[i]) for i in range(count)
        ]
        for copy in copies:
            copy.start()
        for copy in copies:
            copy.wait()

    return pl.pallas_call(
        kernel,
        in_specs=[pl.BlockSpec(memory_space=pltpu.HBM)] * count,
        out_specs=[pl.BlockSpec(memory_space=pltpu.VMEM)] * count,
        out_shape=[pltpu.VMEM(w.shape, w.dtype) for w in weights],
        scratch_shapes=[pltpu.SemaphoreType.DMA((count,))],
        compiler_params=pltpu.CompilerParams(vmem_limit_bytes=1024 * 1024),
        name="fetch",
    )(*[pltpu.with_memory_space_constraint(w, pltpu.HBM) for w in weights])


def swap_halves(first, second):
    half = first.shape[1] // 2
    low = lax.broadcasted_iota(jnp.int32, first.shape, 1) < half
    return (
        jnp.where(low, first, pltpu.roll(second, half, 1)),
        jnp.where(low, pltpu.roll(first, half, 1), second),
    )


def experts(here, pieces, gain, w_gate, w_up, w_down):
    slots, share = pieces[0].shape
    shares = len(pieces)
    local_experts, width, hidden = w_gate.shape
    tile = 8
    chunk = 4 * tile
    kept = slots // local_experts

    def kernel(here_ref, *refs):
        piece_refs = refs[:shares]
        gain_ref, gate_ref, up_ref, down_ref = refs[shares : shares + 4]
        out_refs = refs[shares + 4 : 2 * shares + 4]
        row_ref, act_ref = refs[2 * shares + 4 :]
        froms, tos = ring_places(here_ref, shares)

        def norm_rows(i, carry):
            rows = pl.ds(pl.multiple_of(i * chunk, chunk), chunk)
            values = [r[rows, :].astype(jnp.float32) for r in piece_refs]
            total = values[0]
            for v in values[1:]:
                total = total + v
            centre = jnp.sum(total, -1, keepdims=True) / width
            values = [v - centre for v in values]
            total = values[0] * values[0]
            for v in values[1:]:
                total = total + v * v
            scale = lax.rsqrt(jnp.sum(total, -1, keepdims=True) / width + norm_eps)
            rows = pl.ds(pl.multiple_of(i * (chunk // 2), chunk // 2), chunk // 2)
            for k, v in enumerate(values):
                v = (v * scale * gain_ref[froms[k]]).reshape(2, 2, tile, share)
                for j, part in enumerate(swap_halves(v[:, 0], v[:, 1])):
                    row_ref[j, rows, columns_of(froms[k], share)] = part.reshape(
                        chunk // 2, share
                    ).astype(jnp.bfloat16)
            return carry

        lax.fori_loop(0, slots // chunk, norm_rows, 0)
        for j in range(local_experts):
            rows = row_ref[j]
            gate_part = jnp.dot(rows, gate_ref[j], preferred_element_type=jnp.float32)
            up_part = jnp.dot(rows, up_ref[j], preferred_element_type=jnp.float32)
            act_ref[j] = (gate_part * jax.nn.sigmoid(gate_part) * up_part).astype(jnp.bfloat16)
        for k in (1, shares - 1, *range(2, shares - 1), 0):
            outs = [
                jnp.dot(
                    act_ref[j],
                    down_ref[j, :, columns_of(tos[k], share)],
                    preferred_element_type=jnp.float32,
                ).reshape(kept // tile, tile, share)
                for j in range(local_experts)
            ]
            both = jnp.stack(swap_halves(*outs), axis=1).reshape(slots, share)
            out_refs[k][...] = both.astype(jnp.bfloat16)

    vmem = pl.BlockSpec(memory_space=pltpu.VMEM)
    return pl.pallas_call(
        kernel,
        in_specs=[pl.BlockSpec(memory_space=pltpu.SMEM)] + [vmem] * (shares + 4),
        out_specs=[vmem] * shares,
        out_shape=[jax.ShapeDtypeStruct((slots, share), jnp.bfloat16)] * shares,
        scratch_shapes=[
            pltpu.VMEM((local_experts, kept, width), jnp.bfloat16),
            pltpu.VMEM((local_experts, kept, hidden), jnp.bfloat16),
        ],
        compiler_params=pltpu.CompilerParams(vmem_limit_bytes=24 * 1024 * 1024),
        name="experts",
    )(here, *pieces, gain, w_gate, w_up, w_down)


def add_up(halves):
    rows, share = halves[0][0].shape
    count = len(halves[0])

    def kernel(*refs):
        for h in range(len(halves)):
            group = refs[h * count : (h + 1) * count]
            total = group[0][...].astype(jnp.float32)
            for r in group[1:]:
                total = total + r[...].astype(jnp.float32)
            refs[-1][h * rows : (h + 1) * rows, :] = total.astype(jnp.bfloat16)

    vmem = pl.BlockSpec(memory_space=pltpu.VMEM)
    return pl.pallas_call(
        kernel,
        in_specs=[vmem] * (count * len(halves)),
        out_specs=vmem,
        out_shape=jax.ShapeDtypeStruct((rows * len(halves), share), jnp.bfloat16),
        compiler_params=pltpu.CompilerParams(vmem_limit_bytes=8 * 1024 * 1024),
        name="add_up",
    )(*[r for half in halves for r in half])


def finish(here, hidden, pieces, gain):
    rows, share = pieces[0].shape
    shares = len(pieces)
    width = shares * share

    def kernel(here_ref, hidden_ref, *refs):
        piece_refs = refs[:shares]
        gain_ref, out_ref = refs[shares:]
        froms, _ = ring_places(here_ref, shares)
        values = [
            residual_scale * hidden_ref[k] + piece_refs[k][...].astype(jnp.float32)
            for k in range(shares)
        ]
        total = values[0]
        for v in values[1:]:
            total = total + v
        centre = jnp.sum(total, -1, keepdims=True) / width
        values = [v - centre for v in values]
        total = values[0] * values[0]
        for v in values[1:]:
            total = total + v * v
        scale = lax.rsqrt(jnp.sum(total, -1, keepdims=True) / width + norm_eps)
        for k, v in enumerate(values):
            out_ref[:, columns_of(froms[k], share)] = (v * scale * gain_ref[froms[k]]).astype(jnp.bfloat16)

    vmem = pl.BlockSpec(memory_space=pltpu.VMEM)
    return pl.pallas_call(
        kernel,
        in_specs=[pl.BlockSpec(memory_space=pltpu.SMEM)] + [vmem] * (shares + 2),
        out_specs=vmem,
        out_shape=jax.ShapeDtypeStruct((rows, width), jnp.bfloat16),
        compiler_params=pltpu.CompilerParams(vmem_limit_bytes=8 * 1024 * 1024),
        name="finish",
    )(here, hidden, *pieces, gain)


def layer(
    x_in,
    state,
    routes,
    w_in,
    decay_rate,
    frequency,
    log_step,
    b_in,
    c_out,
    skip,
    w_out,
    gain_mix,
    w_group,
    w_expert,
    w_gate,
    w_up,
    w_down,
    gain_moe,
):
    seq_count, model_width = x_in.shape
    shares = lax.axis_size("tp")
    share = model_width // shares
    expert_total = w_expert.shape[1]
    ep_count = lax.axis_size("ep")
    local_experts = w_gate.shape[0]
    capacity = max(2, 4 * seq_count // expert_total)
    total_slots = expert_total * capacity
    local_slots = local_experts * capacity
    here = lax.axis_index("tp")
    here_array = here.astype(jnp.int32).reshape(1)

    target = slots_of(routes, expert_total, capacity)
    slot_ids = jnp.arange(total_slots, dtype=jnp.int32)

    base, *parts, new_state = mixer(
        here_array,
        x_in,
        state,
        w_in,
        decay_rate,
        frequency,
        log_step.reshape(1, -1),
        b_in,
        c_out,
        skip,
        w_out,
    )
    arrived = shifted([base, *parts], "tp")
    own, sent = place_rows(base, arrived[1:], target, total_slots)
    rows = exchange(sent.reshape(ep_count, local_slots, share), "ep")

    parts = shifted([own] * shares, "tp")
    whole = jnp.stack(parts).astype(jnp.float32)
    order = (here - jnp.arange(shares)) % shares
    gain_mix = gain_mix.reshape(shares, 1, share)
    hidden_state = normalize(whole, gain_mix[order], (0, 2))
    hidden_bf = hidden_state.astype(jnp.bfloat16)
    w_router = jnp.concatenate([w_group, w_expert], axis=-1).reshape(shares, share, -1)[order]
    logits = jnp.einsum("krd,kde->re", hidden_bf, w_router, preferred_element_type=jnp.float32)
    route_weight = route_weights(logits, routes, w_group.shape[1])
    matches = target[:, :, None] == slot_ids[None, None, :]
    combine_map = jnp.sum(jnp.where(matches, route_weight[:, :, None], 0.0), axis=1)

    weights = fetch(w_gate, w_up, w_down)
    half = ep_count // 2
    gathered = []
    for h in range(2):
        rows_half = rows[h * half : (h + 1) * half].reshape(half * local_slots, share)
        gathered.append(shifted([rows_half] * shares, "tp"))
    arrived = []
    for h in range(2):
        outs = experts(here_array, gathered[h], gain_mix, *weights)
        arrived.append(shifted(outs, "tp"))
    summed = add_up(arrived)
    returned = exchange(summed.reshape(ep_count, local_slots, share), "ep")
    moe_own = jnp.dot(
        combine_map.astype(jnp.bfloat16),
        returned.reshape(total_slots, share),
        preferred_element_type=jnp.float32,
    ).astype(jnp.bfloat16)
    moe = shifted([moe_own] * shares, "tp")
    out = finish(here_array, hidden_state, moe, gain_moe.reshape(shares, 1, share))
    return (out, new_state)


def solution(mesh):
    in_specs = (
        P(("grp", "ep"), None),
        P(("grp", "ep"), "tp", None),
        P(("grp", "ep"), None),
        P(None, "tp"),
        P("tp", None),
        P("tp", None),
        P("tp"),
        P("tp", None, None),
        P("tp", None, None),
        P("tp"),
        P("tp", None),
        P(),
        P(),
        P(),
        P("ep", None, "tp"),
        P("ep", None, "tp"),
        P("ep", "tp", None),
        P(),
    )
    out_specs = (P(("grp", "ep"), None), P(("grp", "ep"), "tp", None))
    return jax.shard_map(layer, mesh=mesh, in_specs=in_specs, out_specs=out_specs, check_vma=False)
```

```python
import jax
import jax.numpy as jnp
from jax import lax
from jax.experimental import pallas as pl
from jax.experimental.pallas import tpu as pltpu
from jax.sharding import PartitionSpec as P

residual_scale = 8.0**0.25
norm_eps = 1e-05


def exchange(x, axis):
    return lax.all_to_all(x, axis, 0, 0, tiled=True)


def shifted(pieces, axis):
    size = lax.axis_size(axis)
    return [pieces[0]] + [
        lax.ppermute(pieces[k], axis, [(i, (i + k) % size) for i in range(size)])
        for k in range(1, size)
    ]


def normalize(values, gain, axes):
    centre = jnp.mean(values, axes, keepdims=True)
    spread = jnp.mean(jnp.square(values - centre), axes, keepdims=True)
    return (values - centre) * lax.rsqrt(spread + norm_eps) * gain


def route_weights(logits, routes, group_total):
    expert_total = logits.shape[1] - group_total
    per_group = expert_total // group_total
    group_logit = logits[:, :group_total]
    group_exp = jnp.exp(group_logit)
    group_prob = group_exp / jnp.sum(group_exp, -1, keepdims=True)
    chosen = routes[:, 0] // per_group
    group_pick = jnp.sum(
        jnp.where(
            chosen[:, None] == jnp.arange(group_total, dtype=jnp.int32)[None, :], group_prob, 0.0
        ),
        -1,
    )
    expert_logit = logits[:, group_total:]
    picked = jnp.sum(
        jnp.where(
            routes[:, :, None] == jnp.arange(expert_total, dtype=jnp.int32)[None, None, :],
            expert_logit[:, None, :],
            0.0,
        ),
        -1,
    )
    pair_exp = jnp.exp(picked)
    return pair_exp / jnp.sum(pair_exp, -1, keepdims=True) * group_pick[:, None]


def slots_of(routes, expert_total, capacity):
    hits = (routes[:, :, None] == jnp.arange(expert_total, dtype=jnp.int32)[None, None, :]).astype(
        jnp.int32
    )
    tally = jnp.sum(hits, axis=1)
    prior = jnp.cumsum(tally, axis=0) - tally
    return routes * capacity + jnp.sum(prior[:, None, :] * hits, axis=-1)


def ring_places(here_ref, shares):
    t = here_ref[0]
    froms = [lax.rem(t + shares - k, shares) for k in range(shares)]
    tos = [lax.rem(t + k, shares) for k in range(shares)]
    return froms, tos


def columns_of(place, share):
    return pl.ds(pl.multiple_of(place * share, share), share)


def near(ref):
    return pltpu.VMEM(ref.shape, ref.dtype)


def mixer(here, x_in, state, w_in, decay_rate, frequency, log_step, b_in, c_out, skip, w_out):
    seq_count, width = x_in.shape
    channels = w_in.shape[1]
    groups, entries = decay_rate.shape
    per_group = b_in.shape[1]
    lanes = 2 * entries
    shares = lax.axis_size("tp")
    share = width // shares
    together = lanes // per_group
    cut = 4
    arrays = (decay_rate, frequency, log_step, x_in, w_in, b_in, c_out, skip, state, w_out)

    def kernel(here_ref, *refs):
        far = refs[: len(arrays)]
        base_ref = refs[len(arrays)]
        part_refs = refs[len(arrays) + 1 : len(arrays) + shares]
        new_far = refs[len(arrays) + shares]
        rest = refs[len(arrays) + shares + 1 :]
        close = rest[: len(arrays)]
        decay_ref, freq_ref, log_ref, x_ref, w_in_ref, b_ref, c_ref, skip_ref, state_ref, w_out_ref = close
        new_ref, in_ref, out_ref, act_ref, sems = rest[len(arrays) :]
        _, tos = ring_places(here_ref, shares)
        piece = width // cut
        copies = {}
        for i, (a, b) in enumerate(zip(far, close)):
            if i == 4:
                for q in range(cut):
                    rows = slice(q * piece, (q + 1) * piece)
                    copies[i, q] = pltpu.make_async_copy(
                        a.at[rows], b.at[rows], sems.at[len(arrays) + q]
                    )
            else:
                copies[i] = pltpu.make_async_copy(a, b, sems.at[i])
        for copy in copies.values():
            copy.start()

        lane = lax.broadcasted_iota(jnp.int32, (1, lanes), 1)
        sign = jnp.where(lane < entries, -1.0, 1.0)
        for i in (0, 1, 2):
            copies[i].wait()
        eye = lax.broadcasted_iota(jnp.int32, (groups, groups), 0) == lax.broadcasted_iota(
            jnp.int32, (groups, groups), 1
        )
        log_column = jnp.sum(jnp.where(eye, log_ref[...], 0.0), -1, keepdims=True)
        step_size = jnp.exp(log_column)
        lam_real = -decay_ref[...]
        freq = freq_ref[...]
        magnitude = jnp.exp(lam_real * step_size)
        angle = freq * step_size
        bar_real = magnitude * jnp.cos(angle)
        bar_imag = magnitude * jnp.sin(angle)
        minus_real = bar_real - 1.0
        modulus = lam_real * lam_real + freq * freq
        ratio_real = (minus_real * lam_real + bar_imag * freq) / modulus
        ratio_imag = (bar_imag * lam_real - minus_real * freq) / modulus

        def twice(v):
            return jnp.concatenate([v, v], axis=-1)

        bar_real = twice(bar_real)
        bar_imag = twice(bar_imag) * sign
        ratio_real = twice(ratio_real)
        ratio_imag = twice(ratio_imag) * sign

        copies[3].wait()
        mix = None
        for q in range(cut):
            copies[4, q].wait()
            rows = slice(q * piece, (q + 1) * piece)
            term = jnp.dot(x_ref[:, rows], w_in_ref[rows, :], preferred_element_type=jnp.float32)
            mix = term if mix is None else mix + term
        mix = mix.astype(jnp.bfloat16).astype(jnp.float32)
        copies[5].wait()
        for g in range(groups):
            b = b_ref[g]
            in_ref[g * per_group : (g + 1) * per_group, :] = (
                ratio_real[g : g + 1] * b + ratio_imag[g : g + 1] * pltpu.roll(b, entries, 1)
            ).astype(jnp.bfloat16)
        copies[6].wait()
        for g in range(groups):
            out_ref[g * per_group : (g + 1) * per_group, :] = (c_ref[g] * -sign).astype(jnp.bfloat16)
        x_wide = x_ref[...].astype(jnp.float32)
        x_mean = jnp.sum(x_wide, -1, keepdims=True) / width
        x_own = x_ref[:, columns_of(here_ref[0], share)].astype(jnp.float32)
        base_ref[...] = residual_scale * (x_own - x_mean)
        copies[7].wait()
        copies[8].wait()
        old = state_ref.reshape(seq_count * groups, lanes)
        new = new_ref.reshape(seq_count * groups, lanes)
        lane_group = lane // per_group
        for j in range(groups // together):
            span = slice(j * lanes, (j + 1) * lanes)
            inputs = mix[:, span]
            spread = jnp.concatenate(
                [jnp.where(lane_group == g, inputs, 0.0) for g in range(together)], axis=0
            ).astype(jnp.bfloat16)
            forcing = jnp.dot(spread, in_ref[span, :], preferred_element_type=jnp.float32)
            held = []
            for g in range(together):
                at = j * together + g
                rows = pl.ds(at, seq_count, stride=groups)
                h = old[rows, :]
                h = (
                    bar_real[at : at + 1] * h
                    + bar_imag[at : at + 1] * pltpu.roll(h, entries, 1)
                    + forcing[g * seq_count : (g + 1) * seq_count]
                )
                new[rows, :] = h
                held.append(h.astype(jnp.bfloat16))
            read = lax.dot_general(
                jnp.concatenate(held, axis=0),
                out_ref[span, :],
                (((1,), (1,)), ((), ())),
                preferred_element_type=jnp.float32,
            )
            value = skip_ref[span] * inputs
            for g in range(together):
                value = value + jnp.where(
                    lane_group == g, read[g * seq_count : (g + 1) * seq_count], 0.0
                )
            act_ref[:, span] = jax.nn.gelu(value).astype(jnp.bfloat16)
        send = pltpu.make_async_copy(new_ref, new_far, sems.at[len(arrays) + cut])
        send.start()
        copies[9].wait()
        for k in range(shares):
            part = jnp.dot(
                act_ref[...],
                w_out_ref[:, columns_of(tos[k], share)],
                preferred_element_type=jnp.float32,
            ).astype(jnp.bfloat16)
            if k == 0:
                base_ref[...] += part.astype(jnp.float32)
            else:
                part_refs[k - 1][...] = part
        send.wait()

    vmem = pl.BlockSpec(memory_space=pltpu.VMEM)
    hbm = pl.BlockSpec(memory_space=pltpu.HBM)
    return pl.pallas_call(
        kernel,
        in_specs=[pl.BlockSpec(memory_space=pltpu.SMEM)] + [hbm] * len(arrays),
        out_specs=[vmem] * shares + [hbm],
        out_shape=[jax.ShapeDtypeStruct((seq_count, share), jnp.float32)]
        + [jax.ShapeDtypeStruct((seq_count, share), jnp.bfloat16)] * (shares - 1)
        + [jax.ShapeDtypeStruct(state.shape, state.dtype)],
        scratch_shapes=[near(a) for a in arrays]
        + [
            near(state),
            pltpu.VMEM((channels, lanes), jnp.bfloat16),
            pltpu.VMEM((channels, lanes), jnp.bfloat16),
            pltpu.VMEM((seq_count, channels), jnp.bfloat16),
            pltpu.SemaphoreType.DMA((len(arrays) + cut + 1,)),
        ],
        compiler_params=pltpu.CompilerParams(vmem_limit_bytes=16 * 1024 * 1024),
        name="mixer",
    )(here, *[pltpu.with_memory_space_constraint(a, pltpu.HBM) for a in arrays])


def place_rows(base, arrived, target, total_slots):
    seq_count, share = base.shape
    cut = 4
    piece = total_slots // cut

    def kernel(base_ref, target_ref, *refs):
        own_ref, sent_far, sent_ref, sems = refs[-4:]
        own = base_ref[...]
        for r in refs[:-4]:
            own = own + r[...].astype(jnp.float32)
        own = own.astype(jnp.bfloat16)
        copies = []
        for q in range(cut):
            rows = slice(q * piece, (q + 1) * piece)
            slot = lax.broadcasted_iota(jnp.int32, (piece, seq_count), 0) + q * piece
            hit = slot == target_ref[0:1, :]
            for k in range(1, target_ref.shape[0]):
                hit = hit | (slot == target_ref[k : k + 1, :])
            chosen = jnp.where(hit, 1.0, 0.0).astype(jnp.bfloat16)
            sent_ref[rows, :] = jnp.dot(chosen, own, preferred_element_type=jnp.float32).astype(
                jnp.bfloat16
            )
            copies.append(pltpu.make_async_copy(sent_ref.at[rows], sent_far.at[rows], sems.at[q]))
            copies[-1].start()
        own_ref[...] = own
        for copy in copies:
            copy.wait()

    vmem = pl.BlockSpec(memory_space=pltpu.VMEM)
    return pl.pallas_call(
        kernel,
        in_specs=[vmem] * (2 + len(arrived)),
        out_specs=[vmem, pl.BlockSpec(memory_space=pltpu.HBM)],
        out_shape=[
            jax.ShapeDtypeStruct((seq_count, share), jnp.bfloat16),
            jax.ShapeDtypeStruct((total_slots, share), jnp.bfloat16),
        ],
        scratch_shapes=[
            pltpu.VMEM((total_slots, share), jnp.bfloat16),
            pltpu.SemaphoreType.DMA((cut,)),
        ],
        compiler_params=pltpu.CompilerParams(vmem_limit_bytes=8 * 1024 * 1024),
        name="place_rows",
    )(base, target.T, *arrived)


def fetch(*weights):
    count = len(weights)

    def kernel(*refs):
        copies = [
            pltpu.make_async_copy(refs[i], refs[count + i], refs[-1].at[i]) for i in range(count)
        ]
        for copy in copies:
            copy.start()
        for copy in copies:
            copy.wait()

    return pl.pallas_call(
        kernel,
        in_specs=[pl.BlockSpec(memory_space=pltpu.HBM)] * count,
        out_specs=[pl.BlockSpec(memory_space=pltpu.VMEM)] * count,
        out_shape=[pltpu.VMEM(w.shape, w.dtype) for w in weights],
        scratch_shapes=[pltpu.SemaphoreType.DMA((count,))],
        compiler_params=pltpu.CompilerParams(vmem_limit_bytes=1024 * 1024),
        name="fetch",
    )(*[pltpu.with_memory_space_constraint(w, pltpu.HBM) for w in weights])


def swap_halves(first, second):
    half = first.shape[1] // 2
    low = lax.broadcasted_iota(jnp.int32, first.shape, 1) < half
    return (
        jnp.where(low, first, pltpu.roll(second, half, 1)),
        jnp.where(low, pltpu.roll(first, half, 1), second),
    )


def experts(here, pieces, gain, w_gate, w_up, w_down):
    slots, share = pieces[0].shape
    shares = len(pieces)
    local_experts, width, hidden = w_gate.shape
    tile = 8
    chunk = 4 * tile
    kept = slots // local_experts

    def kernel(here_ref, *refs):
        piece_refs = refs[:shares]
        gain_ref, gate_ref, up_ref, down_ref = refs[shares : shares + 4]
        out_refs = refs[shares + 4 : 2 * shares + 4]
        row_ref, act_ref = refs[2 * shares + 4 :]
        froms, tos = ring_places(here_ref, shares)

        def norm_rows(i, carry):
            rows = pl.ds(pl.multiple_of(i * chunk, chunk), chunk)
            values = [r[rows, :].astype(jnp.float32) for r in piece_refs]
            total = values[0]
            for v in values[1:]:
                total = total + v
            centre = jnp.sum(total, -1, keepdims=True) / width
            values = [v - centre for v in values]
            total = values[0] * values[0]
            for v in values[1:]:
                total = total + v * v
            scale = lax.rsqrt(jnp.sum(total, -1, keepdims=True) / width + norm_eps)
            rows = pl.ds(pl.multiple_of(i * (chunk // 2), chunk // 2), chunk // 2)
            for k, v in enumerate(values):
                v = (v * scale * gain_ref[froms[k]]).reshape(2, 2, tile, share)
                for j, part in enumerate(swap_halves(v[:, 0], v[:, 1])):
                    row_ref[j, rows, columns_of(froms[k], share)] = part.reshape(
                        chunk // 2, share
                    ).astype(jnp.bfloat16)
            return carry

        lax.fori_loop(0, slots // chunk, norm_rows, 0)
        for j in range(local_experts):
            rows = row_ref[j]
            gate_part = jnp.dot(rows, gate_ref[j], preferred_element_type=jnp.float32)
            up_part = jnp.dot(rows, up_ref[j], preferred_element_type=jnp.float32)
            act_ref[j] = (gate_part * jax.nn.sigmoid(gate_part) * up_part).astype(jnp.bfloat16)
        for k in (1, shares - 1, *range(2, shares - 1), 0):
            outs = [
                jnp.dot(
                    act_ref[j],
                    down_ref[j, :, columns_of(tos[k], share)],
                    preferred_element_type=jnp.float32,
                ).reshape(kept // tile, tile, share)
                for j in range(local_experts)
            ]
            both = jnp.stack(swap_halves(*outs), axis=1).reshape(slots, share)
            out_refs[k][...] = both.astype(jnp.bfloat16)

    vmem = pl.BlockSpec(memory_space=pltpu.VMEM)
    return pl.pallas_call(
        kernel,
        in_specs=[pl.BlockSpec(memory_space=pltpu.SMEM)] + [vmem] * (shares + 4),
        out_specs=[vmem] * shares,
        out_shape=[jax.ShapeDtypeStruct((slots, share), jnp.bfloat16)] * shares,
        scratch_shapes=[
            pltpu.VMEM((local_experts, kept, width), jnp.bfloat16),
            pltpu.VMEM((local_experts, kept, hidden), jnp.bfloat16),
        ],
        compiler_params=pltpu.CompilerParams(vmem_limit_bytes=24 * 1024 * 1024),
        name="experts",
    )(here, *pieces, gain, w_gate, w_up, w_down)


def add_up(halves):
    rows, share = halves[0][0].shape
    count = len(halves[0])

    def kernel(*refs):
        for h in range(len(halves)):
            group = refs[h * count : (h + 1) * count]
            total = group[0][...].astype(jnp.float32)
            for r in group[1:]:
                total = total + r[...].astype(jnp.float32)
            refs[-1][h * rows : (h + 1) * rows, :] = total.astype(jnp.bfloat16)

    vmem = pl.BlockSpec(memory_space=pltpu.VMEM)
    return pl.pallas_call(
        kernel,
        in_specs=[vmem] * (count * len(halves)),
        out_specs=vmem,
        out_shape=jax.ShapeDtypeStruct((rows * len(halves), share), jnp.bfloat16),
        compiler_params=pltpu.CompilerParams(vmem_limit_bytes=8 * 1024 * 1024),
        name="add_up",
    )(*[r for half in halves for r in half])


def finish(here, hidden, pieces, gain):
    rows, share = pieces[0].shape
    shares = len(pieces)
    width = shares * share
    cut = 4
    piece = rows // cut

    def kernel(here_ref, hidden_ref, *refs):
        piece_refs = refs[:shares]
        gain_ref, out_far, out_ref, sems = refs[shares:]
        froms, _ = ring_places(here_ref, shares)
        copies = []
        for q in range(cut):
            some = slice(q * piece, (q + 1) * piece)
            values = [
                residual_scale * hidden_ref[k, some] + piece_refs[k][some].astype(jnp.float32)
                for k in range(shares)
            ]
            total = values[0]
            for v in values[1:]:
                total = total + v
            centre = jnp.sum(total, -1, keepdims=True) / width
            values = [v - centre for v in values]
            total = values[0] * values[0]
            for v in values[1:]:
                total = total + v * v
            scale = lax.rsqrt(jnp.sum(total, -1, keepdims=True) / width + norm_eps)
            for k, v in enumerate(values):
                out_ref[some, columns_of(froms[k], share)] = (v * scale * gain_ref[froms[k]]).astype(
                    jnp.bfloat16
                )
            copies.append(pltpu.make_async_copy(out_ref.at[some], out_far.at[some], sems.at[q]))
            copies[-1].start()
        for copy in copies:
            copy.wait()

    vmem = pl.BlockSpec(memory_space=pltpu.VMEM)
    return pl.pallas_call(
        kernel,
        in_specs=[pl.BlockSpec(memory_space=pltpu.SMEM)] + [vmem] * (shares + 2),
        out_specs=pl.BlockSpec(memory_space=pltpu.HBM),
        out_shape=jax.ShapeDtypeStruct((rows, width), jnp.bfloat16),
        scratch_shapes=[
            pltpu.VMEM((rows, width), jnp.bfloat16),
            pltpu.SemaphoreType.DMA((cut,)),
        ],
        compiler_params=pltpu.CompilerParams(vmem_limit_bytes=8 * 1024 * 1024),
        name="finish",
    )(here, hidden, *pieces, gain)


def layer(
    x_in,
    state,
    routes,
    w_in,
    decay_rate,
    frequency,
    log_step,
    b_in,
    c_out,
    skip,
    w_out,
    gain_mix,
    w_group,
    w_expert,
    w_gate,
    w_up,
    w_down,
    gain_moe,
):
    seq_count, model_width = x_in.shape
    shares = lax.axis_size("tp")
    share = model_width // shares
    expert_total = w_expert.shape[1]
    ep_count = lax.axis_size("ep")
    local_experts = w_gate.shape[0]
    capacity = max(2, 4 * seq_count // expert_total)
    total_slots = expert_total * capacity
    local_slots = local_experts * capacity
    here = lax.axis_index("tp")
    here_array = here.astype(jnp.int32).reshape(1)

    target = slots_of(routes, expert_total, capacity)
    slot_ids = jnp.arange(total_slots, dtype=jnp.int32)

    base, *parts, new_state = mixer(
        here_array,
        x_in,
        state,
        w_in,
        decay_rate,
        frequency,
        log_step.reshape(1, -1),
        b_in,
        c_out,
        skip,
        w_out,
    )
    arrived = shifted([base, *parts], "tp")
    own, sent = place_rows(base, arrived[1:], target, total_slots)
    rows = exchange(sent.reshape(ep_count, local_slots, share), "ep")

    parts = shifted([own] * shares, "tp")
    whole = jnp.stack(parts).astype(jnp.float32)
    order = (here - jnp.arange(shares)) % shares
    gain_mix = gain_mix.reshape(shares, 1, share)
    hidden_state = normalize(whole, gain_mix[order], (0, 2))
    hidden_bf = hidden_state.astype(jnp.bfloat16)
    w_router = jnp.concatenate([w_group, w_expert], axis=-1).reshape(shares, share, -1)[order]
    logits = jnp.einsum("krd,kde->re", hidden_bf, w_router, preferred_element_type=jnp.float32)
    route_weight = route_weights(logits, routes, w_group.shape[1])
    matches = target[:, :, None] == slot_ids[None, None, :]
    combine_map = jnp.sum(jnp.where(matches, route_weight[:, :, None], 0.0), axis=1)

    weights = fetch(w_gate, w_up, w_down)
    half = ep_count // 2
    gathered = []
    for h in range(2):
        rows_half = rows[h * half : (h + 1) * half].reshape(half * local_slots, share)
        gathered.append(shifted([rows_half] * shares, "tp"))
    arrived = []
    for h in range(2):
        outs = experts(here_array, gathered[h], gain_mix, *weights)
        arrived.append(shifted(outs, "tp"))
    summed = add_up(arrived)
    returned = exchange(summed.reshape(ep_count, local_slots, share), "ep")
    moe_own = jnp.dot(
        combine_map.astype(jnp.bfloat16),
        returned.reshape(total_slots, share),
        preferred_element_type=jnp.float32,
    ).astype(jnp.bfloat16)
    moe = shifted([moe_own] * shares, "tp")
    out = finish(here_array, hidden_state, moe, gain_moe.reshape(shares, 1, share))
    return (out, new_state)


def solution(mesh):
    in_specs = (
        P(("grp", "ep"), None),
        P(("grp", "ep"), "tp", None),
        P(("grp", "ep"), None),
        P(None, "tp"),
        P("tp", None),
        P("tp", None),
        P("tp"),
        P("tp", None, None),
        P("tp", None, None),
        P("tp"),
        P("tp", None),
        P(),
        P(),
        P(),
        P("ep", None, "tp"),
        P("ep", None, "tp"),
        P("ep", "tp", None),
        P(),
    )
    out_specs = (P(("grp", "ep"), None), P(("grp", "ep"), "tp", None))
    return jax.shard_map(layer, mesh=mesh, in_specs=in_specs, out_specs=out_specs, check_vma=False)
```

```python
import jax
import jax.numpy as jnp
from jax import lax
from jax.experimental import pallas as pl
from jax.experimental.pallas import tpu as pltpu
from jax.sharding import PartitionSpec as P

residual_scale = 8.0**0.25
norm_eps = 1e-05


def exchange(x, axis):
    return lax.all_to_all(x, axis, 0, 0, tiled=True)


def shifted(pieces, axis):
    size = lax.axis_size(axis)
    return [pieces[0]] + [
        lax.ppermute(pieces[k], axis, [(i, (i + k) % size) for i in range(size)])
        for k in range(1, size)
    ]


def normalize(values, gain, axes):
    centre = jnp.mean(values, axes, keepdims=True)
    spread = jnp.mean(jnp.square(values - centre), axes, keepdims=True)
    return (values - centre) * lax.rsqrt(spread + norm_eps) * gain


def route_weights(logits, routes, group_total):
    expert_total = logits.shape[1] - group_total
    per_group = expert_total // group_total
    group_logit = logits[:, :group_total]
    group_exp = jnp.exp(group_logit)
    group_prob = group_exp / jnp.sum(group_exp, -1, keepdims=True)
    chosen = routes[:, 0] // per_group
    group_pick = jnp.sum(
        jnp.where(
            chosen[:, None] == jnp.arange(group_total, dtype=jnp.int32)[None, :], group_prob, 0.0
        ),
        -1,
    )
    expert_logit = logits[:, group_total:]
    picked = jnp.sum(
        jnp.where(
            routes[:, :, None] == jnp.arange(expert_total, dtype=jnp.int32)[None, None, :],
            expert_logit[:, None, :],
            0.0,
        ),
        -1,
    )
    pair_exp = jnp.exp(picked)
    return pair_exp / jnp.sum(pair_exp, -1, keepdims=True) * group_pick[:, None]


def slots_of(routes, expert_total, capacity):
    hits = (routes[:, :, None] == jnp.arange(expert_total, dtype=jnp.int32)[None, None, :]).astype(
        jnp.int32
    )
    tally = jnp.sum(hits, axis=1)
    prior = jnp.cumsum(tally, axis=0) - tally
    return routes * capacity + jnp.sum(prior[:, None, :] * hits, axis=-1)


def ring_places(here_ref, shares):
    t = here_ref[0]
    froms = [lax.rem(t + shares - k, shares) for k in range(shares)]
    tos = [lax.rem(t + k, shares) for k in range(shares)]
    return froms, tos


def columns_of(place, share):
    return pl.ds(pl.multiple_of(place * share, share), share)


def near(ref):
    return pltpu.VMEM(ref.shape, ref.dtype)


def mixer(here, x_in, state, w_in, decay_rate, frequency, log_step, b_in, c_out, skip, w_out):
    seq_count, width = x_in.shape
    channels = w_in.shape[1]
    groups, entries = decay_rate.shape
    per_group = b_in.shape[1]
    lanes = 2 * entries
    shares = lax.axis_size("tp")
    share = width // shares
    together = lanes // per_group
    cut = 4
    arrays = (decay_rate, frequency, log_step, x_in, w_in, b_in, c_out, skip, state, w_out)

    def kernel(here_ref, *refs):
        far = refs[: len(arrays)]
        base_ref = refs[len(arrays)]
        part_refs = refs[len(arrays) + 1 : len(arrays) + shares]
        new_far = refs[len(arrays) + shares]
        rest = refs[len(arrays) + shares + 1 :]
        close = rest[: len(arrays)]
        decay_ref, freq_ref, log_ref, x_ref, w_in_ref, b_ref, c_ref, skip_ref, state_ref, w_out_ref = close
        new_ref, in_ref, out_ref, act_ref, sems = rest[len(arrays) :]
        _, tos = ring_places(here_ref, shares)
        piece = width // cut
        copies = {}
        for i, (a, b) in enumerate(zip(far, close)):
            if i == 4:
                for q in range(cut):
                    rows = slice(q * piece, (q + 1) * piece)
                    copies[i, q] = pltpu.make_async_copy(
                        a.at[rows], b.at[rows], sems.at[len(arrays) + q]
                    )
            else:
                copies[i] = pltpu.make_async_copy(a, b, sems.at[i])
        for copy in copies.values():
            copy.start()

        lane = lax.broadcasted_iota(jnp.int32, (1, lanes), 1)
        sign = jnp.where(lane < entries, -1.0, 1.0)
        for i in (0, 1, 2):
            copies[i].wait()
        eye = lax.broadcasted_iota(jnp.int32, (groups, groups), 0) == lax.broadcasted_iota(
            jnp.int32, (groups, groups), 1
        )
        log_column = jnp.sum(jnp.where(eye, log_ref[...], 0.0), -1, keepdims=True)
        step_size = jnp.exp(log_column)
        lam_real = -decay_ref[...]
        freq = freq_ref[...]
        magnitude = jnp.exp(lam_real * step_size)
        angle = freq * step_size
        bar_real = magnitude * jnp.cos(angle)
        bar_imag = magnitude * jnp.sin(angle)
        minus_real = bar_real - 1.0
        modulus = lam_real * lam_real + freq * freq
        ratio_real = (minus_real * lam_real + bar_imag * freq) / modulus
        ratio_imag = (bar_imag * lam_real - minus_real * freq) / modulus

        def twice(v):
            return jnp.concatenate([v, v], axis=-1)

        bar_real = twice(bar_real)
        bar_imag = twice(bar_imag) * sign
        ratio_real = twice(ratio_real)
        ratio_imag = twice(ratio_imag) * sign

        copies[3].wait()
        mix = None
        for q in range(cut):
            copies[4, q].wait()
            rows = slice(q * piece, (q + 1) * piece)
            term = jnp.dot(x_ref[:, rows], w_in_ref[rows, :], preferred_element_type=jnp.float32)
            mix = term if mix is None else mix + term
        mix = mix.astype(jnp.bfloat16).astype(jnp.float32)
        copies[5].wait()
        for g in range(groups):
            b = b_ref[g]
            in_ref[g * per_group : (g + 1) * per_group, :] = (
                ratio_real[g : g + 1] * b + ratio_imag[g : g + 1] * pltpu.roll(b, entries, 1)
            ).astype(jnp.bfloat16)
        copies[6].wait()
        for g in range(groups):
            out_ref[g * per_group : (g + 1) * per_group, :] = (c_ref[g] * -sign).astype(jnp.bfloat16)
        x_wide = x_ref[...].astype(jnp.float32)
        x_mean = jnp.sum(x_wide, -1, keepdims=True) / width
        x_own = x_ref[:, columns_of(here_ref[0], share)].astype(jnp.float32)
        base_ref[...] = residual_scale * (x_own - x_mean)
        copies[7].wait()
        copies[8].wait()
        old = state_ref.reshape(seq_count * groups, lanes)
        new = new_ref.reshape(seq_count * groups, lanes)
        lane_group = lane // per_group
        for j in range(groups // together):
            span = slice(j * lanes, (j + 1) * lanes)
            inputs = mix[:, span]
            spread = jnp.concatenate(
                [jnp.where(lane_group == g, inputs, 0.0) for g in range(together)], axis=0
            ).astype(jnp.bfloat16)
            forcing = jnp.dot(spread, in_ref[span, :], preferred_element_type=jnp.float32)
            held = []
            for g in range(together):
                at = j * together + g
                rows = pl.ds(at, seq_count, stride=groups)
                h = old[rows, :]
                h = (
                    bar_real[at : at + 1] * h
                    + bar_imag[at : at + 1] * pltpu.roll(h, entries, 1)
                    + forcing[g * seq_count : (g + 1) * seq_count]
                )
                new[rows, :] = h
                held.append(h.astype(jnp.bfloat16))
            read = lax.dot_general(
                jnp.concatenate(held, axis=0),
                out_ref[span, :],
                (((1,), (1,)), ((), ())),
                preferred_element_type=jnp.float32,
            )
            value = skip_ref[span] * inputs
            for g in range(together):
                value = value + jnp.where(
                    lane_group == g, read[g * seq_count : (g + 1) * seq_count], 0.0
                )
            act_ref[:, span] = jax.nn.gelu(value).astype(jnp.bfloat16)
        send = pltpu.make_async_copy(new_ref, new_far, sems.at[len(arrays) + cut])
        send.start()
        copies[9].wait()
        for k in range(shares):
            part = jnp.dot(
                act_ref[...],
                w_out_ref[:, columns_of(tos[k], share)],
                preferred_element_type=jnp.float32,
            ).astype(jnp.bfloat16)
            if k == 0:
                base_ref[...] += part.astype(jnp.float32)
            else:
                part_refs[k - 1][...] = part
        send.wait()

    vmem = pl.BlockSpec(memory_space=pltpu.VMEM)
    hbm = pl.BlockSpec(memory_space=pltpu.HBM)
    return pl.pallas_call(
        kernel,
        in_specs=[pl.BlockSpec(memory_space=pltpu.SMEM)] + [hbm] * len(arrays),
        out_specs=[vmem] * shares + [hbm],
        out_shape=[jax.ShapeDtypeStruct((seq_count, share), jnp.float32)]
        + [jax.ShapeDtypeStruct((seq_count, share), jnp.bfloat16)] * (shares - 1)
        + [jax.ShapeDtypeStruct(state.shape, state.dtype)],
        scratch_shapes=[near(a) for a in arrays]
        + [
            near(state),
            pltpu.VMEM((channels, lanes), jnp.bfloat16),
            pltpu.VMEM((channels, lanes), jnp.bfloat16),
            pltpu.VMEM((seq_count, channels), jnp.bfloat16),
            pltpu.SemaphoreType.DMA((len(arrays) + cut + 1,)),
        ],
        compiler_params=pltpu.CompilerParams(vmem_limit_bytes=16 * 1024 * 1024),
        name="mixer",
    )(here, *[pltpu.with_memory_space_constraint(a, pltpu.HBM) for a in arrays])


def place_rows(base, arrived, target, total_slots):
    seq_count, share = base.shape
    cut = 4
    piece = total_slots // cut

    def kernel(base_ref, target_ref, *refs):
        own_ref, sent_far, sent_ref, sems = refs[-4:]
        own = base_ref[...]
        for r in refs[:-4]:
            own = own + r[...].astype(jnp.float32)
        own = own.astype(jnp.bfloat16)
        copies = []
        for q in range(cut):
            rows = slice(q * piece, (q + 1) * piece)
            slot = lax.broadcasted_iota(jnp.int32, (piece, seq_count), 0) + q * piece
            hit = slot == target_ref[0:1, :]
            for k in range(1, target_ref.shape[0]):
                hit = hit | (slot == target_ref[k : k + 1, :])
            chosen = jnp.where(hit, 1.0, 0.0).astype(jnp.bfloat16)
            sent_ref[rows, :] = jnp.dot(chosen, own, preferred_element_type=jnp.float32).astype(
                jnp.bfloat16
            )
            copies.append(pltpu.make_async_copy(sent_ref.at[rows], sent_far.at[rows], sems.at[q]))
            copies[-1].start()
        own_ref[...] = own
        for copy in copies:
            copy.wait()

    vmem = pl.BlockSpec(memory_space=pltpu.VMEM)
    return pl.pallas_call(
        kernel,
        in_specs=[vmem] * (2 + len(arrived)),
        out_specs=[vmem, pl.BlockSpec(memory_space=pltpu.HBM)],
        out_shape=[
            jax.ShapeDtypeStruct((seq_count, share), jnp.bfloat16),
            jax.ShapeDtypeStruct((total_slots, share), jnp.bfloat16),
        ],
        scratch_shapes=[
            pltpu.VMEM((total_slots, share), jnp.bfloat16),
            pltpu.SemaphoreType.DMA((cut,)),
        ],
        compiler_params=pltpu.CompilerParams(vmem_limit_bytes=8 * 1024 * 1024),
        name="place_rows",
    )(base, target.T, *arrived)


def fetch(which, *weights):
    count = len(weights)

    def kernel(*refs):
        copies = [
            pltpu.make_async_copy(refs[i].at[which], refs[count + i], refs[-1].at[i])
            for i in range(count)
        ]
        for copy in copies:
            copy.start()
        for copy in copies:
            copy.wait()

    return pl.pallas_call(
        kernel,
        in_specs=[pl.BlockSpec(memory_space=pltpu.HBM)] * count,
        out_specs=[pl.BlockSpec(memory_space=pltpu.VMEM)] * count,
        out_shape=[pltpu.VMEM(w.shape[1:], w.dtype) for w in weights],
        scratch_shapes=[pltpu.SemaphoreType.DMA((count,))],
        compiler_params=pltpu.CompilerParams(vmem_limit_bytes=1024 * 1024),
        name="fetch",
    )(*[pltpu.with_memory_space_constraint(w, pltpu.HBM) for w in weights])


def swap_halves(first, second):
    half = first.shape[1] // 2
    low = lax.broadcasted_iota(jnp.int32, first.shape, 1) < half
    return (
        jnp.where(low, first, pltpu.roll(second, half, 1)),
        jnp.where(low, pltpu.roll(first, half, 1), second),
    )


def by_expert(rows):
    slots, share = rows.shape
    tile = 8

    def kernel(rows_ref, *out_refs):
        tiles = rows_ref[...].astype(jnp.float32).reshape(slots // (2 * tile), 2, tile, share)
        for out_ref, part in zip(out_refs, swap_halves(tiles[:, 0], tiles[:, 1])):
            out_ref[...] = part.reshape(slots // 2, share).astype(jnp.bfloat16)

    vmem = pl.BlockSpec(memory_space=pltpu.VMEM)
    return pl.pallas_call(
        kernel,
        in_specs=[vmem],
        out_specs=[vmem] * 2,
        out_shape=[jax.ShapeDtypeStruct((slots // 2, share), jnp.bfloat16)] * 2,
        compiler_params=pltpu.CompilerParams(vmem_limit_bytes=8 * 1024 * 1024),
        name="by_expert",
    )(rows)


def add_up(arrived):
    rows, share = arrived[0][0].shape
    count = len(arrived[0])
    tile = 8

    def kernel(*refs):
        totals = []
        for h in range(2):
            group = refs[h * count : (h + 1) * count]
            total = group[0][...].astype(jnp.float32)
            for r in group[1:]:
                total = total + r[...].astype(jnp.float32)
            totals.append(total.reshape(rows // tile, tile, share))
        both = jnp.stack(swap_halves(*totals), axis=1).reshape(2 * rows, share)
        refs[-1][...] = both.astype(jnp.bfloat16)

    vmem = pl.BlockSpec(memory_space=pltpu.VMEM)
    return pl.pallas_call(
        kernel,
        in_specs=[vmem] * (2 * count),
        out_specs=vmem,
        out_shape=jax.ShapeDtypeStruct((2 * rows, share), jnp.bfloat16),
        compiler_params=pltpu.CompilerParams(vmem_limit_bytes=8 * 1024 * 1024),
        name="add_up",
    )(*arrived[0], *arrived[1])


def expert(here, pieces, gain, w_gate, w_up, w_down):
    slots, share = pieces[0].shape
    shares = len(pieces)
    width = w_gate.shape[0]
    chunk = 32

    def kernel(here_ref, *refs):
        piece_refs = refs[:shares]
        gain_ref, gate_ref, up_ref, down_ref = refs[shares : shares + 4]
        out_refs = refs[shares + 4 : 2 * shares + 4]
        row_ref = refs[-1]
        froms, tos = ring_places(here_ref, shares)

        def norm_rows(i, carry):
            rows = pl.ds(pl.multiple_of(i * chunk, chunk), chunk)
            values = [r[rows, :].astype(jnp.float32) for r in piece_refs]
            total = values[0]
            for v in values[1:]:
                total = total + v
            centre = jnp.sum(total, -1, keepdims=True) / width
            values = [v - centre for v in values]
            total = values[0] * values[0]
            for v in values[1:]:
                total = total + v * v
            scale = lax.rsqrt(jnp.sum(total, -1, keepdims=True) / width + norm_eps)
            for k, v in enumerate(values):
                row_ref[rows, columns_of(froms[k], share)] = (
                    v * scale * gain_ref[froms[k]]
                ).astype(jnp.bfloat16)
            return carry

        lax.fori_loop(0, slots // chunk, norm_rows, 0)
        rows = row_ref[...]
        gate_part = jnp.dot(rows, gate_ref[...], preferred_element_type=jnp.float32)
        up_part = jnp.dot(rows, up_ref[...], preferred_element_type=jnp.float32)
        act = (gate_part * jax.nn.sigmoid(gate_part) * up_part).astype(jnp.bfloat16)
        for k in range(shares):
            out_refs[k][...] = jnp.dot(
                act, down_ref[:, columns_of(tos[k], share)], preferred_element_type=jnp.float32
            ).astype(jnp.bfloat16)

    vmem = pl.BlockSpec(memory_space=pltpu.VMEM)
    return pl.pallas_call(
        kernel,
        in_specs=[pl.BlockSpec(memory_space=pltpu.SMEM)] + [vmem] * (shares + 4),
        out_specs=[vmem] * shares,
        out_shape=[jax.ShapeDtypeStruct((slots, share), jnp.bfloat16)] * shares,
        scratch_shapes=[pltpu.VMEM((slots, width), jnp.bfloat16)],
        compiler_params=pltpu.CompilerParams(vmem_limit_bytes=16 * 1024 * 1024),
        name="expert",
    )(here, *pieces, gain, w_gate, w_up, w_down)


def finish(here, hidden, pieces, gain):
    rows, share = pieces[0].shape
    shares = len(pieces)
    width = shares * share
    cut = 4
    piece = rows // cut

    def kernel(here_ref, hidden_ref, *refs):
        piece_refs = refs[:shares]
        gain_ref, out_far, out_ref, sems = refs[shares:]
        froms, _ = ring_places(here_ref, shares)
        copies = []
        for q in range(cut):
            some = slice(q * piece, (q + 1) * piece)
            values = [
                residual_scale * hidden_ref[k, some] + piece_refs[k][some].astype(jnp.float32)
                for k in range(shares)
            ]
            total = values[0]
            for v in values[1:]:
                total = total + v
            centre = jnp.sum(total, -1, keepdims=True) / width
            values = [v - centre for v in values]
            total = values[0] * values[0]
            for v in values[1:]:
                total = total + v * v
            scale = lax.rsqrt(jnp.sum(total, -1, keepdims=True) / width + norm_eps)
            for k, v in enumerate(values):
                out_ref[some, columns_of(froms[k], share)] = (v * scale * gain_ref[froms[k]]).astype(
                    jnp.bfloat16
                )
            copies.append(pltpu.make_async_copy(out_ref.at[some], out_far.at[some], sems.at[q]))
            copies[-1].start()
        for copy in copies:
            copy.wait()

    vmem = pl.BlockSpec(memory_space=pltpu.VMEM)
    return pl.pallas_call(
        kernel,
        in_specs=[pl.BlockSpec(memory_space=pltpu.SMEM)] + [vmem] * (shares + 2),
        out_specs=pl.BlockSpec(memory_space=pltpu.HBM),
        out_shape=jax.ShapeDtypeStruct((rows, width), jnp.bfloat16),
        scratch_shapes=[
            pltpu.VMEM((rows, width), jnp.bfloat16),
            pltpu.SemaphoreType.DMA((cut,)),
        ],
        compiler_params=pltpu.CompilerParams(vmem_limit_bytes=8 * 1024 * 1024),
        name="finish",
    )(here, hidden, *pieces, gain)


def layer(
    x_in,
    state,
    routes,
    w_in,
    decay_rate,
    frequency,
    log_step,
    b_in,
    c_out,
    skip,
    w_out,
    gain_mix,
    w_group,
    w_expert,
    w_gate,
    w_up,
    w_down,
    gain_moe,
):
    seq_count, model_width = x_in.shape
    shares = lax.axis_size("tp")
    share = model_width // shares
    expert_total = w_expert.shape[1]
    ep_count = lax.axis_size("ep")
    local_experts = w_gate.shape[0]
    capacity = max(2, 4 * seq_count // expert_total)
    total_slots = expert_total * capacity
    local_slots = local_experts * capacity
    here = lax.axis_index("tp")
    here_array = here.astype(jnp.int32).reshape(1)

    target = slots_of(routes, expert_total, capacity)
    slot_ids = jnp.arange(total_slots, dtype=jnp.int32)

    base, *parts, new_state = mixer(
        here_array,
        x_in,
        state,
        w_in,
        decay_rate,
        frequency,
        log_step.reshape(1, -1),
        b_in,
        c_out,
        skip,
        w_out,
    )
    arrived = shifted([base, *parts], "tp")
    own, sent = place_rows(base, arrived[1:], target, total_slots)
    rows = exchange(sent.reshape(ep_count, local_slots, share), "ep")

    parts = shifted([own] * shares, "tp")
    whole = jnp.stack(parts).astype(jnp.float32)
    order = (here - jnp.arange(shares)) % shares
    gain_mix = gain_mix.reshape(shares, 1, share)
    hidden_state = normalize(whole, gain_mix[order], (0, 2))
    hidden_bf = hidden_state.astype(jnp.bfloat16)
    w_router = jnp.concatenate([w_group, w_expert], axis=-1).reshape(shares, share, -1)[order]
    logits = jnp.einsum("krd,kde->re", hidden_bf, w_router, preferred_element_type=jnp.float32)
    route_weight = route_weights(logits, routes, w_group.shape[1])
    matches = target[:, :, None] == slot_ids[None, None, :]
    combine_map = jnp.sum(jnp.where(matches, route_weight[:, :, None], 0.0), axis=1)

    rows = by_expert(rows.reshape(total_slots, share))
    gathered = []
    for j in range(local_experts):
        gathered.append(shifted([rows[j]] * shares, "tp"))
    arrived = []
    for j in range(local_experts):
        weights = fetch(j, w_gate, w_up, w_down)
        outs = expert(here_array, gathered[j], gain_mix, *weights)
        arrived.append(shifted(outs, "tp"))
    summed = add_up(arrived)
    returned = exchange(summed.reshape(ep_count, local_slots, share), "ep")
    moe_own = jnp.dot(
        combine_map.astype(jnp.bfloat16),
        returned.reshape(total_slots, share),
        preferred_element_type=jnp.float32,
    ).astype(jnp.bfloat16)
    moe = shifted([moe_own] * shares, "tp")
    out = finish(here_array, hidden_state, moe, gain_moe.reshape(shares, 1, share))
    return (out, new_state)


def solution(mesh):
    in_specs = (
        P(("grp", "ep"), None),
        P(("grp", "ep"), "tp", None),
        P(("grp", "ep"), None),
        P(None, "tp"),
        P("tp", None),
        P("tp", None),
        P("tp"),
        P("tp", None, None),
        P("tp", None, None),
        P("tp"),
        P("tp", None),
        P(),
        P(),
        P(),
        P("ep", None, "tp"),
        P("ep", None, "tp"),
        P("ep", "tp", None),
        P(),
    )
    out_specs = (P(("grp", "ep"), None), P(("grp", "ep"), "tp", None))
    return jax.shard_map(layer, mesh=mesh, in_specs=in_specs, out_specs=out_specs, check_vma=False)
```

```python
import jax
import jax.numpy as jnp
from jax import lax
from jax.experimental import pallas as pl
from jax.experimental.pallas import tpu as pltpu
from jax.sharding import PartitionSpec as P

residual_scale = 8.0**0.25
norm_eps = 1e-05


def exchange(x, axis):
    return lax.all_to_all(x, axis, 0, 0, tiled=True)


def shifted(pieces, axis):
    size = lax.axis_size(axis)
    return [pieces[0]] + [
        lax.ppermute(pieces[k], axis, [(i, (i + k) % size) for i in range(size)])
        for k in range(1, size)
    ]


def normalize(values, gain, axes):
    centre = jnp.mean(values, axes, keepdims=True)
    spread = jnp.mean(jnp.square(values - centre), axes, keepdims=True)
    return (values - centre) * lax.rsqrt(spread + norm_eps) * gain


def route_weights(logits, routes, group_total):
    expert_total = logits.shape[1] - group_total
    per_group = expert_total // group_total
    group_logit = logits[:, :group_total]
    group_exp = jnp.exp(group_logit)
    group_prob = group_exp / jnp.sum(group_exp, -1, keepdims=True)
    chosen = routes[:, 0] // per_group
    group_pick = jnp.sum(
        jnp.where(
            chosen[:, None] == jnp.arange(group_total, dtype=jnp.int32)[None, :], group_prob, 0.0
        ),
        -1,
    )
    expert_logit = logits[:, group_total:]
    picked = jnp.sum(
        jnp.where(
            routes[:, :, None] == jnp.arange(expert_total, dtype=jnp.int32)[None, None, :],
            expert_logit[:, None, :],
            0.0,
        ),
        -1,
    )
    pair_exp = jnp.exp(picked)
    return pair_exp / jnp.sum(pair_exp, -1, keepdims=True) * group_pick[:, None]


def ring_places(here_ref, shares):
    t = here_ref[0]
    froms = [lax.rem(t + shares - k, shares) for k in range(shares)]
    tos = [lax.rem(t + k, shares) for k in range(shares)]
    return froms, tos


def columns_of(place, share):
    return pl.ds(pl.multiple_of(place * share, share), share)


def near(ref):
    return pltpu.VMEM(ref.shape, ref.dtype)


def mixer(
    here,
    routes,
    expert_total,
    capacity,
    x_in,
    state,
    w_in,
    decay_rate,
    frequency,
    log_step,
    b_in,
    c_out,
    skip,
    w_out,
):
    seq_count, width = x_in.shape
    channels = w_in.shape[1]
    groups, entries = decay_rate.shape
    per_group = b_in.shape[1]
    lanes = 2 * entries
    shares = lax.axis_size("tp")
    share = width // shares
    together = lanes // per_group
    cut = 4
    arrays = (decay_rate, frequency, log_step, x_in, w_in, b_in, c_out, skip, state, w_out, routes)
    picks = routes.shape[0]

    def kernel(here_ref, *refs):
        far = refs[: len(arrays)]
        base_ref = refs[len(arrays)]
        part_refs = refs[len(arrays) + 1 : len(arrays) + shares]
        new_far, target_ref = refs[len(arrays) + shares : len(arrays) + shares + 2]
        rest = refs[len(arrays) + shares + 2 :]
        close = rest[: len(arrays)]
        decay_ref, freq_ref, log_ref, x_ref, w_in_ref, b_ref, c_ref, skip_ref, state_ref, w_out_ref, routes_ref = close
        new_ref, in_ref, out_ref, act_ref, sems = rest[len(arrays) :]
        _, tos = ring_places(here_ref, shares)
        piece = width // cut
        copies = {}
        for i, (a, b) in enumerate(zip(far, close)):
            if i == 4:
                for q in range(cut):
                    rows = slice(q * piece, (q + 1) * piece)
                    copies[i, q] = pltpu.make_async_copy(
                        a.at[rows], b.at[rows], sems.at[len(arrays) + q]
                    )
            else:
                copies[i] = pltpu.make_async_copy(a, b, sems.at[i])
        for copy in copies.values():
            copy.start()

        copies[10].wait()
        named = lax.broadcasted_iota(jnp.int32, (expert_total, seq_count), 0)
        hits = [jnp.where(named == routes_ref[k : k + 1, :], 1.0, 0.0) for k in range(picks)]
        earlier = lax.broadcasted_iota(jnp.int32, (seq_count, seq_count), 0) < (
            lax.broadcasted_iota(jnp.int32, (seq_count, seq_count), 1)
        )
        before = jnp.dot(
            sum(hits).astype(jnp.bfloat16),
            jnp.where(earlier, 1.0, 0.0).astype(jnp.bfloat16),
            preferred_element_type=jnp.float32,
        )
        for k in range(picks):
            place = jnp.sum(hits[k] * before, axis=0, keepdims=True)
            target_ref[k : k + 1, :] = routes_ref[k : k + 1, :] * capacity + place.astype(jnp.int32)
        lane = lax.broadcasted_iota(jnp.int32, (1, lanes), 1)
        sign = jnp.where(lane < entries, -1.0, 1.0)
        for i in (0, 1, 2):
            copies[i].wait()
        eye = lax.broadcasted_iota(jnp.int32, (groups, groups), 0) == lax.broadcasted_iota(
            jnp.int32, (groups, groups), 1
        )
        log_column = jnp.sum(jnp.where(eye, log_ref[...], 0.0), -1, keepdims=True)
        step_size = jnp.exp(log_column)
        lam_real = -decay_ref[...]
        freq = freq_ref[...]
        magnitude = jnp.exp(lam_real * step_size)
        angle = freq * step_size
        bar_real = magnitude * jnp.cos(angle)
        bar_imag = magnitude * jnp.sin(angle)
        minus_real = bar_real - 1.0
        modulus = lam_real * lam_real + freq * freq
        ratio_real = (minus_real * lam_real + bar_imag * freq) / modulus
        ratio_imag = (bar_imag * lam_real - minus_real * freq) / modulus

        def twice(v):
            return jnp.concatenate([v, v], axis=-1)

        bar_real = twice(bar_real)
        bar_imag = twice(bar_imag) * sign
        ratio_real = twice(ratio_real)
        ratio_imag = twice(ratio_imag) * sign

        copies[3].wait()
        mix = None
        for q in range(cut):
            copies[4, q].wait()
            rows = slice(q * piece, (q + 1) * piece)
            term = jnp.dot(x_ref[:, rows], w_in_ref[rows, :], preferred_element_type=jnp.float32)
            mix = term if mix is None else mix + term
        mix = mix.astype(jnp.bfloat16).astype(jnp.float32)
        copies[5].wait()
        for g in range(groups):
            b = b_ref[g]
            in_ref[g * per_group : (g + 1) * per_group, :] = (
                ratio_real[g : g + 1] * b + ratio_imag[g : g + 1] * pltpu.roll(b, entries, 1)
            ).astype(jnp.bfloat16)
        copies[6].wait()
        for g in range(groups):
            out_ref[g * per_group : (g + 1) * per_group, :] = (c_ref[g] * -sign).astype(jnp.bfloat16)
        x_wide = x_ref[...].astype(jnp.float32)
        x_mean = jnp.sum(x_wide, -1, keepdims=True) / width
        x_own = x_ref[:, columns_of(here_ref[0], share)].astype(jnp.float32)
        base_ref[...] = residual_scale * (x_own - x_mean)
        copies[7].wait()
        copies[8].wait()
        old = state_ref.reshape(seq_count * groups, lanes)
        new = new_ref.reshape(seq_count * groups, lanes)
        lane_group = lane // per_group
        for j in range(groups // together):
            span = slice(j * lanes, (j + 1) * lanes)
            inputs = mix[:, span]
            spread = jnp.concatenate(
                [jnp.where(lane_group == g, inputs, 0.0) for g in range(together)], axis=0
            ).astype(jnp.bfloat16)
            forcing = jnp.dot(spread, in_ref[span, :], preferred_element_type=jnp.float32)
            held = []
            for g in range(together):
                at = j * together + g
                rows = pl.ds(at, seq_count, stride=groups)
                h = old[rows, :]
                h = (
                    bar_real[at : at + 1] * h
                    + bar_imag[at : at + 1] * pltpu.roll(h, entries, 1)
                    + forcing[g * seq_count : (g + 1) * seq_count]
                )
                new[rows, :] = h
                held.append(h.astype(jnp.bfloat16))
            read = lax.dot_general(
                jnp.concatenate(held, axis=0),
                out_ref[span, :],
                (((1,), (1,)), ((), ())),
                preferred_element_type=jnp.float32,
            )
            value = skip_ref[span] * inputs
            for g in range(together):
                value = value + jnp.where(
                    lane_group == g, read[g * seq_count : (g + 1) * seq_count], 0.0
                )
            act_ref[:, span] = jax.nn.gelu(value).astype(jnp.bfloat16)
        send = pltpu.make_async_copy(new_ref, new_far, sems.at[len(arrays) + cut])
        send.start()
        copies[9].wait()
        for k in range(shares):
            part = jnp.dot(
                act_ref[...],
                w_out_ref[:, columns_of(tos[k], share)],
                preferred_element_type=jnp.float32,
            ).astype(jnp.bfloat16)
            if k == 0:
                base_ref[...] += part.astype(jnp.float32)
            else:
                part_refs[k - 1][...] = part
        send.wait()

    vmem = pl.BlockSpec(memory_space=pltpu.VMEM)
    hbm = pl.BlockSpec(memory_space=pltpu.HBM)
    return pl.pallas_call(
        kernel,
        in_specs=[pl.BlockSpec(memory_space=pltpu.SMEM)] + [hbm] * len(arrays),
        out_specs=[vmem] * shares + [hbm, vmem],
        out_shape=[jax.ShapeDtypeStruct((seq_count, share), jnp.float32)]
        + [jax.ShapeDtypeStruct((seq_count, share), jnp.bfloat16)] * (shares - 1)
        + [
            jax.ShapeDtypeStruct(state.shape, state.dtype),
            jax.ShapeDtypeStruct(routes.shape, jnp.int32),
        ],
        scratch_shapes=[near(a) for a in arrays]
        + [
            near(state),
            pltpu.VMEM((channels, lanes), jnp.bfloat16),
            pltpu.VMEM((channels, lanes), jnp.bfloat16),
            pltpu.VMEM((seq_count, channels), jnp.bfloat16),
            pltpu.SemaphoreType.DMA((len(arrays) + cut + 1,)),
        ],
        compiler_params=pltpu.CompilerParams(vmem_limit_bytes=16 * 1024 * 1024),
        name="mixer",
    )(here, *[pltpu.with_memory_space_constraint(a, pltpu.HBM) for a in arrays])


def place_rows(base, arrived, target, total_slots):
    seq_count, share = base.shape

    def kernel(base_ref, target_ref, *refs):
        own_ref, sent_ref = refs[-2:]
        own = base_ref[...]
        for r in refs[:-2]:
            own = own + r[...].astype(jnp.float32)
        own = own.astype(jnp.bfloat16)
        own_ref[...] = own
        slot = lax.broadcasted_iota(jnp.int32, (total_slots, seq_count), 0)
        hit = slot == target_ref[0:1, :]
        for k in range(1, target_ref.shape[0]):
            hit = hit | (slot == target_ref[k : k + 1, :])
        chosen = jnp.where(hit, 1.0, 0.0).astype(jnp.bfloat16)
        sent_ref[...] = jnp.dot(chosen, own, preferred_element_type=jnp.float32).astype(jnp.bfloat16)

    vmem = pl.BlockSpec(memory_space=pltpu.VMEM)
    return pl.pallas_call(
        kernel,
        in_specs=[vmem] * (2 + len(arrived)),
        out_specs=[vmem] * 2,
        out_shape=[
            jax.ShapeDtypeStruct((seq_count, share), jnp.bfloat16),
            jax.ShapeDtypeStruct((total_slots, share), jnp.bfloat16),
        ],
        compiler_params=pltpu.CompilerParams(vmem_limit_bytes=8 * 1024 * 1024),
        name="place_rows",
    )(base, target, *arrived)


def fetch(*weights):
    count = len(weights)
    local_experts = weights[0].shape[0]

    def kernel(*refs):
        copies = [
            pltpu.make_async_copy(
                refs[i].at[j], refs[count + j * count + i], refs[-1].at[j * count + i]
            )
            for j in range(local_experts)
            for i in range(count)
        ]
        for copy in copies:
            copy.start()
        for copy in copies:
            copy.wait()

    out = pl.pallas_call(
        kernel,
        in_specs=[pl.BlockSpec(memory_space=pltpu.HBM)] * count,
        out_specs=[pl.BlockSpec(memory_space=pltpu.VMEM)] * (count * local_experts),
        out_shape=[pltpu.VMEM(w.shape[1:], w.dtype) for w in weights] * local_experts,
        scratch_shapes=[pltpu.SemaphoreType.DMA((count * local_experts,))],
        compiler_params=pltpu.CompilerParams(vmem_limit_bytes=1024 * 1024),
        name="fetch",
    )(*[pltpu.with_memory_space_constraint(w, pltpu.HBM) for w in weights])
    return [out[j * count : (j + 1) * count] for j in range(local_experts)]


def swap_halves(first, second):
    half = first.shape[1] // 2
    low = lax.broadcasted_iota(jnp.int32, first.shape, 1) < half
    return (
        jnp.where(low, first, pltpu.roll(second, half, 1)),
        jnp.where(low, pltpu.roll(first, half, 1), second),
    )


def by_expert(rows):
    slots, share = rows.shape
    tile = 8

    def kernel(rows_ref, *out_refs):
        tiles = rows_ref[...].astype(jnp.float32).reshape(slots // (2 * tile), 2, tile, share)
        for out_ref, part in zip(out_refs, swap_halves(tiles[:, 0], tiles[:, 1])):
            out_ref[...] = part.reshape(slots // 2, share).astype(jnp.bfloat16)

    vmem = pl.BlockSpec(memory_space=pltpu.VMEM)
    return pl.pallas_call(
        kernel,
        in_specs=[vmem],
        out_specs=[vmem] * 2,
        out_shape=[jax.ShapeDtypeStruct((slots // 2, share), jnp.bfloat16)] * 2,
        compiler_params=pltpu.CompilerParams(vmem_limit_bytes=8 * 1024 * 1024),
        name="by_expert",
    )(rows)


def add_up(arrived):
    rows, share = arrived[0][0].shape
    count = len(arrived[0])
    tile = 8

    def kernel(*refs):
        totals = []
        for h in range(2):
            group = refs[h * count : (h + 1) * count]
            total = group[0][...].astype(jnp.float32)
            for r in group[1:]:
                total = total + r[...].astype(jnp.float32)
            totals.append(total.reshape(rows // tile, tile, share))
        both = jnp.stack(swap_halves(*totals), axis=1).reshape(2 * rows, share)
        refs[-1][...] = both.astype(jnp.bfloat16)

    vmem = pl.BlockSpec(memory_space=pltpu.VMEM)
    return pl.pallas_call(
        kernel,
        in_specs=[vmem] * (2 * count),
        out_specs=vmem,
        out_shape=jax.ShapeDtypeStruct((2 * rows, share), jnp.bfloat16),
        compiler_params=pltpu.CompilerParams(vmem_limit_bytes=8 * 1024 * 1024),
        name="add_up",
    )(*arrived[0], *arrived[1])


def expert(here, pieces, gain, w_gate, w_up, w_down):
    slots, share = pieces[0].shape
    shares = len(pieces)
    width = w_gate.shape[0]
    chunk = 32

    def kernel(here_ref, *refs):
        piece_refs = refs[:shares]
        gain_ref, gate_ref, up_ref, down_ref = refs[shares : shares + 4]
        out_refs = refs[shares + 4 : 2 * shares + 4]
        row_ref = refs[-1]
        froms, tos = ring_places(here_ref, shares)

        def norm_rows(i, carry):
            rows = pl.ds(pl.multiple_of(i * chunk, chunk), chunk)
            values = [r[rows, :].astype(jnp.float32) for r in piece_refs]
            total = values[0]
            for v in values[1:]:
                total = total + v
            centre = jnp.sum(total, -1, keepdims=True) / width
            values = [v - centre for v in values]
            total = values[0] * values[0]
            for v in values[1:]:
                total = total + v * v
            scale = lax.rsqrt(jnp.sum(total, -1, keepdims=True) / width + norm_eps)
            for k, v in enumerate(values):
                row_ref[rows, columns_of(froms[k], share)] = (
                    v * scale * gain_ref[froms[k]]
                ).astype(jnp.bfloat16)
            return carry

        lax.fori_loop(0, slots // chunk, norm_rows, 0)
        rows = row_ref[...]
        gate_part = jnp.dot(rows, gate_ref[...], preferred_element_type=jnp.float32)
        up_part = jnp.dot(rows, up_ref[...], preferred_element_type=jnp.float32)
        act = (gate_part * jax.nn.sigmoid(gate_part) * up_part).astype(jnp.bfloat16)
        for k in range(shares):
            out_refs[k][...] = jnp.dot(
                act, down_ref[:, columns_of(tos[k], share)], preferred_element_type=jnp.float32
            ).astype(jnp.bfloat16)

    vmem = pl.BlockSpec(memory_space=pltpu.VMEM)
    return pl.pallas_call(
        kernel,
        in_specs=[pl.BlockSpec(memory_space=pltpu.SMEM)] + [vmem] * (shares + 4),
        out_specs=[vmem] * shares,
        out_shape=[jax.ShapeDtypeStruct((slots, share), jnp.bfloat16)] * shares,
        scratch_shapes=[pltpu.VMEM((slots, width), jnp.bfloat16)],
        compiler_params=pltpu.CompilerParams(vmem_limit_bytes=16 * 1024 * 1024),
        name="expert",
    )(here, *pieces, gain, w_gate, w_up, w_down)


def finish(here, hidden, pieces, gain):
    rows, share = pieces[0].shape
    shares = len(pieces)
    width = shares * share
    cut = 4
    piece = rows // cut

    def kernel(here_ref, hidden_ref, *refs):
        piece_refs = refs[:shares]
        gain_ref, out_far, out_ref, sems = refs[shares:]
        froms, _ = ring_places(here_ref, shares)
        copies = []
        for q in range(cut):
            some = slice(q * piece, (q + 1) * piece)
            values = [
                residual_scale * hidden_ref[k, some] + piece_refs[k][some].astype(jnp.float32)
                for k in range(shares)
            ]
            total = values[0]
            for v in values[1:]:
                total = total + v
            centre = jnp.sum(total, -1, keepdims=True) / width
            values = [v - centre for v in values]
            total = values[0] * values[0]
            for v in values[1:]:
                total = total + v * v
            scale = lax.rsqrt(jnp.sum(total, -1, keepdims=True) / width + norm_eps)
            for k, v in enumerate(values):
                out_ref[some, columns_of(froms[k], share)] = (v * scale * gain_ref[froms[k]]).astype(
                    jnp.bfloat16
                )
            copies.append(pltpu.make_async_copy(out_ref.at[some], out_far.at[some], sems.at[q]))
            copies[-1].start()
        for copy in copies:
            copy.wait()

    vmem = pl.BlockSpec(memory_space=pltpu.VMEM)
    return pl.pallas_call(
        kernel,
        in_specs=[pl.BlockSpec(memory_space=pltpu.SMEM)] + [vmem] * (shares + 2),
        out_specs=pl.BlockSpec(memory_space=pltpu.HBM),
        out_shape=jax.ShapeDtypeStruct((rows, width), jnp.bfloat16),
        scratch_shapes=[
            pltpu.VMEM((rows, width), jnp.bfloat16),
            pltpu.SemaphoreType.DMA((cut,)),
        ],
        compiler_params=pltpu.CompilerParams(vmem_limit_bytes=8 * 1024 * 1024),
        name="finish",
    )(here, hidden, *pieces, gain)


def layer(
    x_in,
    state,
    routes,
    w_in,
    decay_rate,
    frequency,
    log_step,
    b_in,
    c_out,
    skip,
    w_out,
    gain_mix,
    w_group,
    w_expert,
    w_gate,
    w_up,
    w_down,
    gain_moe,
):
    seq_count, model_width = x_in.shape
    shares = lax.axis_size("tp")
    share = model_width // shares
    expert_total = w_expert.shape[1]
    ep_count = lax.axis_size("ep")
    local_experts = w_gate.shape[0]
    capacity = max(2, 4 * seq_count // expert_total)
    total_slots = expert_total * capacity
    local_slots = local_experts * capacity
    here = lax.axis_index("tp")
    here_array = here.astype(jnp.int32).reshape(1)

    base, *parts, new_state, target = mixer(
        here_array,
        routes.T,
        expert_total,
        capacity,
        x_in,
        state,
        w_in,
        decay_rate,
        frequency,
        log_step.reshape(1, -1),
        b_in,
        c_out,
        skip,
        w_out,
    )
    arrived = shifted([base, *parts], "tp")
    weights = fetch(w_gate, w_up, w_down)
    own, sent = place_rows(base, arrived[1:], target, total_slots)
    rows = exchange(sent.reshape(ep_count, local_slots, share), "ep")

    gains = gain_mix.reshape(shares, 1, share)
    rows = by_expert(rows.reshape(total_slots, share))
    gathered = []
    for j in range(local_experts):
        gathered.append(shifted([rows[j]] * shares, "tp"))
    arrived = []
    for j in range(local_experts):
        outs = expert(here_array, gathered[j], gains, *weights[j])
        arrived.append(shifted(outs, "tp"))
    summed = add_up(arrived)
    summed, own, target, routes, gain_mix, w_group, w_expert = lax.optimization_barrier(
        (summed, own, target, routes, gain_mix, w_group, w_expert)
    )
    returned = exchange(summed.reshape(ep_count, local_slots, share), "ep")

    parts = shifted([own] * shares, "tp")
    whole = jnp.stack(parts).astype(jnp.float32)
    order = (here - jnp.arange(shares)) % shares
    hidden_state = normalize(whole, gain_mix.reshape(shares, 1, share)[order], (0, 2))
    hidden_bf = hidden_state.astype(jnp.bfloat16)
    w_router = jnp.concatenate([w_group, w_expert], axis=-1).reshape(shares, share, -1)[order]
    logits = jnp.einsum("krd,kde->re", hidden_bf, w_router, preferred_element_type=jnp.float32)
    route_weight = route_weights(logits, routes, w_group.shape[1])
    slot_ids = jnp.arange(total_slots, dtype=jnp.int32)
    matches = target.T[:, :, None] == slot_ids[None, None, :]
    combine_map = jnp.sum(jnp.where(matches, route_weight[:, :, None], 0.0), axis=1)

    moe_own = jnp.dot(
        combine_map.astype(jnp.bfloat16),
        returned.reshape(total_slots, share),
        preferred_element_type=jnp.float32,
    ).astype(jnp.bfloat16)
    moe = shifted([moe_own] * shares, "tp")
    out = finish(here_array, hidden_state, moe, gain_moe.reshape(shares, 1, share))
    return (out, new_state)


def solution(mesh):
    in_specs = (
        P(("grp", "ep"), None),
        P(("grp", "ep"), "tp", None),
        P(("grp", "ep"), None),
        P(None, "tp"),
        P("tp", None),
        P("tp", None),
        P("tp"),
        P("tp", None, None),
        P("tp", None, None),
        P("tp"),
        P("tp", None),
        P(),
        P(),
        P(),
        P("ep", None, "tp"),
        P("ep", None, "tp"),
        P("ep", "tp", None),
        P(),
    )
    out_specs = (P(("grp", "ep"), None), P(("grp", "ep"), "tp", None))
    return jax.shard_map(layer, mesh=mesh, in_specs=in_specs, out_specs=out_specs, check_vma=False)
```

```python
import jax
import jax.numpy as jnp
from jax import lax
from jax.experimental import pallas as pl
from jax.experimental.pallas import tpu as pltpu
from jax.sharding import PartitionSpec as P

residual_scale = 8.0**0.25
norm_eps = 1e-05


def exchange(x, axis):
    return lax.all_to_all(x, axis, 0, 0, tiled=True)


def shifted(pieces, axis):
    size = lax.axis_size(axis)
    return [pieces[0]] + [
        lax.ppermute(pieces[k], axis, [(i, (i + k) % size) for i in range(size)])
        for k in range(1, size)
    ]


def normalize(values, gain, axes):
    centre = jnp.mean(values, axes, keepdims=True)
    spread = jnp.mean(jnp.square(values - centre), axes, keepdims=True)
    return (values - centre) * lax.rsqrt(spread + norm_eps) * gain


def route_weights(logits, routes, group_total):
    expert_total = logits.shape[1] - group_total
    per_group = expert_total // group_total
    group_logit = logits[:, :group_total]
    group_exp = jnp.exp(group_logit)
    group_prob = group_exp / jnp.sum(group_exp, -1, keepdims=True)
    chosen = routes[:, 0] // per_group
    group_pick = jnp.sum(
        jnp.where(
            chosen[:, None] == jnp.arange(group_total, dtype=jnp.int32)[None, :], group_prob, 0.0
        ),
        -1,
    )
    expert_logit = logits[:, group_total:]
    picked = jnp.sum(
        jnp.where(
            routes[:, :, None] == jnp.arange(expert_total, dtype=jnp.int32)[None, None, :],
            expert_logit[:, None, :],
            0.0,
        ),
        -1,
    )
    pair_exp = jnp.exp(picked)
    return pair_exp / jnp.sum(pair_exp, -1, keepdims=True) * group_pick[:, None]


def slots_of(routes, expert_total, capacity):
    hits = (routes[:, :, None] == jnp.arange(expert_total, dtype=jnp.int32)[None, None, :]).astype(
        jnp.int32
    )
    tally = jnp.sum(hits, axis=1)
    prior = jnp.cumsum(tally, axis=0) - tally
    return routes * capacity + jnp.sum(prior[:, None, :] * hits, axis=-1)


def ring_places(here_ref, shares):
    t = here_ref[0]
    froms = [lax.rem(t + shares - k, shares) for k in range(shares)]
    tos = [lax.rem(t + k, shares) for k in range(shares)]
    return froms, tos


def columns_of(place, share):
    return pl.ds(pl.multiple_of(place * share, share), share)


def near(ref):
    return pltpu.VMEM(ref.shape, ref.dtype)


def mixer(here, x_in, state, w_in, decay_rate, frequency, log_step, b_in, c_out, skip, w_out):
    seq_count, width = x_in.shape
    channels = w_in.shape[1]
    groups, entries = decay_rate.shape
    per_group = b_in.shape[1]
    lanes = 2 * entries
    shares = lax.axis_size("tp")
    share = width // shares
    together = lanes // per_group
    cut = 4
    arrays = (decay_rate, frequency, log_step, x_in, w_in, b_in, c_out, skip, state, w_out)

    def kernel(here_ref, *refs):
        far = refs[: len(arrays)]
        base_ref = refs[len(arrays)]
        part_refs = refs[len(arrays) + 1 : len(arrays) + shares]
        new_ref = refs[len(arrays) + shares]
        rest = refs[len(arrays) + shares + 1 :]
        close = rest[: len(arrays)]
        decay_ref, freq_ref, log_ref, x_ref, w_in_ref, b_ref, c_ref, skip_ref, state_ref, w_out_ref = close
        in_ref, out_ref, act_ref, sems = rest[len(arrays) :]
        _, tos = ring_places(here_ref, shares)
        piece = width // cut
        copies = {}
        for i, (a, b) in enumerate(zip(far, close)):
            if i == 4:
                for q in range(cut):
                    rows = slice(q * piece, (q + 1) * piece)
                    copies[i, q] = pltpu.make_async_copy(
                        a.at[rows], b.at[rows], sems.at[len(arrays) + q]
                    )
            elif i == 9:
                for k in range(shares):
                    columns = columns_of(tos[k], share)
                    copies[i, k] = pltpu.make_async_copy(
                        a.at[:, columns], b.at[:, columns], sems.at[len(arrays) + cut + k]
                    )
            else:
                copies[i] = pltpu.make_async_copy(a, b, sems.at[i])
        for copy in copies.values():
            copy.start()

        lane = lax.broadcasted_iota(jnp.int32, (1, lanes), 1)
        sign = jnp.where(lane < entries, -1.0, 1.0)
        for i in (0, 1, 2):
            copies[i].wait()
        eye = lax.broadcasted_iota(jnp.int32, (groups, groups), 0) == lax.broadcasted_iota(
            jnp.int32, (groups, groups), 1
        )
        log_column = jnp.sum(jnp.where(eye, log_ref[...], 0.0), -1, keepdims=True)
        step_size = jnp.exp(log_column)
        lam_real = -decay_ref[...]
        freq = freq_ref[...]
        magnitude = jnp.exp(lam_real * step_size)
        angle = freq * step_size
        bar_real = magnitude * jnp.cos(angle)
        bar_imag = magnitude * jnp.sin(angle)
        minus_real = bar_real - 1.0
        modulus = lam_real * lam_real + freq * freq
        ratio_real = (minus_real * lam_real + bar_imag * freq) / modulus
        ratio_imag = (bar_imag * lam_real - minus_real * freq) / modulus

        def twice(v):
            return jnp.concatenate([v, v], axis=-1)

        bar_real = twice(bar_real)
        bar_imag = twice(bar_imag) * sign
        ratio_real = twice(ratio_real)
        ratio_imag = twice(ratio_imag) * sign

        copies[3].wait()
        mix = None
        for q in range(cut):
            copies[4, q].wait()
            rows = slice(q * piece, (q + 1) * piece)
            term = jnp.dot(x_ref[:, rows], w_in_ref[rows, :], preferred_element_type=jnp.float32)
            mix = term if mix is None else mix + term
        mix = mix.astype(jnp.bfloat16).astype(jnp.float32)
        copies[5].wait()
        for g in range(groups):
            b = b_ref[g]
            in_ref[g * per_group : (g + 1) * per_group, :] = (
                ratio_real[g : g + 1] * b + ratio_imag[g : g + 1] * pltpu.roll(b, entries, 1)
            ).astype(jnp.bfloat16)
        copies[6].wait()
        for g in range(groups):
            out_ref[g * per_group : (g + 1) * per_group, :] = (c_ref[g] * -sign).astype(jnp.bfloat16)
        x_wide = x_ref[...].astype(jnp.float32)
        x_mean = jnp.sum(x_wide, -1, keepdims=True) / width
        x_own = x_ref[:, columns_of(here_ref[0], share)].astype(jnp.float32)
        base_ref[...] = residual_scale * (x_own - x_mean)
        copies[7].wait()
        copies[8].wait()
        old = state_ref.reshape(seq_count * groups, lanes)
        new = new_ref.reshape(seq_count * groups, lanes)
        lane_group = lane // per_group
        for j in range(groups // together):
            span = slice(j * lanes, (j + 1) * lanes)
            inputs = mix[:, span]
            spread = jnp.concatenate(
                [jnp.where(lane_group == g, inputs, 0.0) for g in range(together)], axis=0
            ).astype(jnp.bfloat16)
            forcing = jnp.dot(spread, in_ref[span, :], preferred_element_type=jnp.float32)
            held = []
            for g in range(together):
                at = j * together + g
                rows = pl.ds(at, seq_count, stride=groups)
                h = old[rows, :]
                h = (
                    bar_real[at : at + 1] * h
                    + bar_imag[at : at + 1] * pltpu.roll(h, entries, 1)
                    + forcing[g * seq_count : (g + 1) * seq_count]
                )
                new[rows, :] = h
                held.append(h.astype(jnp.bfloat16))
            read = lax.dot_general(
                jnp.concatenate(held, axis=0),
                out_ref[span, :],
                (((1,), (1,)), ((), ())),
                preferred_element_type=jnp.float32,
            )
            value = skip_ref[span] * inputs
            for g in range(together):
                value = value + jnp.where(
                    lane_group == g, read[g * seq_count : (g + 1) * seq_count], 0.0
                )
            act_ref[:, span] = jax.nn.gelu(value).astype(jnp.bfloat16)
        for k in range(shares):
            copies[9, k].wait()
            part = jnp.dot(
                act_ref[...],
                w_out_ref[:, columns_of(tos[k], share)],
                preferred_element_type=jnp.float32,
            ).astype(jnp.bfloat16)
            if k == 0:
                base_ref[...] += part.astype(jnp.float32)
            else:
                part_refs[k - 1][...] = part

    vmem = pl.BlockSpec(memory_space=pltpu.VMEM)
    hbm = pl.BlockSpec(memory_space=pltpu.HBM)
    return pl.pallas_call(
        kernel,
        in_specs=[pl.BlockSpec(memory_space=pltpu.SMEM)] + [hbm] * len(arrays),
        out_specs=[vmem] * (shares + 1),
        out_shape=[jax.ShapeDtypeStruct((seq_count, share), jnp.float32)]
        + [jax.ShapeDtypeStruct((seq_count, share), jnp.bfloat16)] * (shares - 1)
        + [near(state)],
        scratch_shapes=[near(a) for a in arrays]
        + [
            pltpu.VMEM((channels, lanes), jnp.bfloat16),
            pltpu.VMEM((channels, lanes), jnp.bfloat16),
            pltpu.VMEM((seq_count, channels), jnp.bfloat16),
            pltpu.SemaphoreType.DMA((len(arrays) + cut + shares,)),
        ],
        compiler_params=pltpu.CompilerParams(vmem_limit_bytes=16 * 1024 * 1024),
        name="mixer",
    )(here, *[pltpu.with_memory_space_constraint(a, pltpu.HBM) for a in arrays])


def place_rows(base, arrived, target, total_slots):
    seq_count, share = base.shape
    cut = 4
    piece = total_slots // cut

    def kernel(base_ref, target_ref, *refs):
        own_ref, sent_far, sent_ref, sems = refs[-4:]
        own = base_ref[...]
        for r in refs[:-4]:
            own = own + r[...].astype(jnp.float32)
        own = own.astype(jnp.bfloat16)
        copies = []
        for q in range(cut):
            rows = slice(q * piece, (q + 1) * piece)
            slot = lax.broadcasted_iota(jnp.int32, (piece, seq_count), 0) + q * piece
            hit = slot == target_ref[0:1, :]
            for k in range(1, target_ref.shape[0]):
                hit = hit | (slot == target_ref[k : k + 1, :])
            chosen = jnp.where(hit, 1.0, 0.0).astype(jnp.bfloat16)
            sent_ref[rows, :] = jnp.dot(chosen, own, preferred_element_type=jnp.float32).astype(
                jnp.bfloat16
            )
            copies.append(pltpu.make_async_copy(sent_ref.at[rows], sent_far.at[rows], sems.at[q]))
            copies[-1].start()
        own_ref[...] = own
        for copy in copies:
            copy.wait()

    vmem = pl.BlockSpec(memory_space=pltpu.VMEM)
    return pl.pallas_call(
        kernel,
        in_specs=[vmem] * (2 + len(arrived)),
        out_specs=[vmem, pl.BlockSpec(memory_space=pltpu.HBM)],
        out_shape=[
            jax.ShapeDtypeStruct((seq_count, share), jnp.bfloat16),
            jax.ShapeDtypeStruct((total_slots, share), jnp.bfloat16),
        ],
        scratch_shapes=[
            pltpu.VMEM((total_slots, share), jnp.bfloat16),
            pltpu.SemaphoreType.DMA((cut,)),
        ],
        compiler_params=pltpu.CompilerParams(vmem_limit_bytes=8 * 1024 * 1024),
        name="place_rows",
    )(base, target.T, *arrived)


def fetch(which, *weights):
    count = len(weights)

    def kernel(*refs):
        copies = [
            pltpu.make_async_copy(refs[i].at[which], refs[count + i], refs[-1].at[i])
            for i in range(count)
        ]
        for copy in copies:
            copy.start()
        for copy in copies:
            copy.wait()

    return pl.pallas_call(
        kernel,
        in_specs=[pl.BlockSpec(memory_space=pltpu.HBM)] * count,
        out_specs=[pl.BlockSpec(memory_space=pltpu.VMEM)] * count,
        out_shape=[pltpu.VMEM(w.shape[1:], w.dtype) for w in weights],
        scratch_shapes=[pltpu.SemaphoreType.DMA((count,))],
        compiler_params=pltpu.CompilerParams(vmem_limit_bytes=1024 * 1024),
        name="fetch",
    )(*[pltpu.with_memory_space_constraint(w, pltpu.HBM) for w in weights])


def swap_halves(first, second):
    half = first.shape[1] // 2
    low = lax.broadcasted_iota(jnp.int32, first.shape, 1) < half
    return (
        jnp.where(low, first, pltpu.roll(second, half, 1)),
        jnp.where(low, pltpu.roll(first, half, 1), second),
    )


def by_expert(rows):
    slots, share = rows.shape
    tile = 8

    def kernel(rows_ref, *out_refs):
        tiles = rows_ref[...].astype(jnp.float32).reshape(slots // (2 * tile), 2, tile, share)
        for out_ref, part in zip(out_refs, swap_halves(tiles[:, 0], tiles[:, 1])):
            out_ref[...] = part.reshape(slots // 2, share).astype(jnp.bfloat16)

    vmem = pl.BlockSpec(memory_space=pltpu.VMEM)
    return pl.pallas_call(
        kernel,
        in_specs=[vmem],
        out_specs=[vmem] * 2,
        out_shape=[jax.ShapeDtypeStruct((slots // 2, share), jnp.bfloat16)] * 2,
        compiler_params=pltpu.CompilerParams(vmem_limit_bytes=8 * 1024 * 1024),
        name="by_expert",
    )(rows)


def add_up(arrived):
    rows, share = arrived[0][0].shape
    count = len(arrived[0])
    tile = 8

    def kernel(*refs):
        totals = []
        for h in range(2):
            group = refs[h * count : (h + 1) * count]
            total = group[0][...].astype(jnp.float32)
            for r in group[1:]:
                total = total + r[...].astype(jnp.float32)
            totals.append(total.reshape(rows // tile, tile, share))
        both = jnp.stack(swap_halves(*totals), axis=1).reshape(2 * rows, share)
        refs[-1][...] = both.astype(jnp.bfloat16)

    vmem = pl.BlockSpec(memory_space=pltpu.VMEM)
    return pl.pallas_call(
        kernel,
        in_specs=[vmem] * (2 * count),
        out_specs=vmem,
        out_shape=jax.ShapeDtypeStruct((2 * rows, share), jnp.bfloat16),
        compiler_params=pltpu.CompilerParams(vmem_limit_bytes=8 * 1024 * 1024),
        name="add_up",
    )(*arrived[0], *arrived[1])


def expert(here, pieces, gain, w_gate, w_up, w_down):
    slots, share = pieces[0].shape
    shares = len(pieces)
    width = w_gate.shape[0]
    chunk = 32

    def kernel(here_ref, *refs):
        piece_refs = refs[:shares]
        gain_ref, gate_ref, up_ref, down_ref = refs[shares : shares + 4]
        out_refs = refs[shares + 4 : 2 * shares + 4]
        row_ref = refs[-1]
        froms, tos = ring_places(here_ref, shares)

        def norm_rows(i, carry):
            rows = pl.ds(pl.multiple_of(i * chunk, chunk), chunk)
            values = [r[rows, :].astype(jnp.float32) for r in piece_refs]
            total = values[0]
            for v in values[1:]:
                total = total + v
            centre = jnp.sum(total, -1, keepdims=True) / width
            values = [v - centre for v in values]
            total = values[0] * values[0]
            for v in values[1:]:
                total = total + v * v
            scale = lax.rsqrt(jnp.sum(total, -1, keepdims=True) / width + norm_eps)
            for k, v in enumerate(values):
                row_ref[rows, columns_of(froms[k], share)] = (
                    v * scale * gain_ref[froms[k]]
                ).astype(jnp.bfloat16)
            return carry

        lax.fori_loop(0, slots // chunk, norm_rows, 0)
        rows = row_ref[...]
        gate_part = jnp.dot(rows, gate_ref[...], preferred_element_type=jnp.float32)
        up_part = jnp.dot(rows, up_ref[...], preferred_element_type=jnp.float32)
        act = (gate_part * jax.nn.sigmoid(gate_part) * up_part).astype(jnp.bfloat16)
        for k in range(shares):
            out_refs[k][...] = jnp.dot(
                act, down_ref[:, columns_of(tos[k], share)], preferred_element_type=jnp.float32
            ).astype(jnp.bfloat16)

    vmem = pl.BlockSpec(memory_space=pltpu.VMEM)
    return pl.pallas_call(
        kernel,
        in_specs=[pl.BlockSpec(memory_space=pltpu.SMEM)] + [vmem] * (shares + 4),
        out_specs=[vmem] * shares,
        out_shape=[jax.ShapeDtypeStruct((slots, share), jnp.bfloat16)] * shares,
        scratch_shapes=[pltpu.VMEM((slots, width), jnp.bfloat16)],
        compiler_params=pltpu.CompilerParams(vmem_limit_bytes=16 * 1024 * 1024),
        name="expert",
    )(here, *pieces, gain, w_gate, w_up, w_down)


def finish(here, hidden, pieces, gain):
    rows, share = pieces[0].shape
    shares = len(pieces)
    width = shares * share
    cut = 4
    piece = rows // cut

    def kernel(here_ref, hidden_ref, *refs):
        piece_refs = refs[:shares]
        gain_ref, out_far, out_ref, sems = refs[shares:]
        froms, _ = ring_places(here_ref, shares)
        copies = []
        for q in range(cut):
            some = slice(q * piece, (q + 1) * piece)
            values = [
                residual_scale * hidden_ref[k, some] + piece_refs[k][some].astype(jnp.float32)
                for k in range(shares)
            ]
            total = values[0]
            for v in values[1:]:
                total = total + v
            centre = jnp.sum(total, -1, keepdims=True) / width
            values = [v - centre for v in values]
            total = values[0] * values[0]
            for v in values[1:]:
                total = total + v * v
            scale = lax.rsqrt(jnp.sum(total, -1, keepdims=True) / width + norm_eps)
            for k, v in enumerate(values):
                out_ref[some, columns_of(froms[k], share)] = (v * scale * gain_ref[froms[k]]).astype(
                    jnp.bfloat16
                )
            copies.append(pltpu.make_async_copy(out_ref.at[some], out_far.at[some], sems.at[q]))
            copies[-1].start()
        for copy in copies:
            copy.wait()

    vmem = pl.BlockSpec(memory_space=pltpu.VMEM)
    return pl.pallas_call(
        kernel,
        in_specs=[pl.BlockSpec(memory_space=pltpu.SMEM)] + [vmem] * (shares + 2),
        out_specs=pl.BlockSpec(memory_space=pltpu.HBM),
        out_shape=jax.ShapeDtypeStruct((rows, width), jnp.bfloat16),
        scratch_shapes=[
            pltpu.VMEM((rows, width), jnp.bfloat16),
            pltpu.SemaphoreType.DMA((cut,)),
        ],
        compiler_params=pltpu.CompilerParams(vmem_limit_bytes=8 * 1024 * 1024),
        name="finish",
    )(here, hidden, *pieces, gain)


def layer(
    x_in,
    state,
    routes,
    w_in,
    decay_rate,
    frequency,
    log_step,
    b_in,
    c_out,
    skip,
    w_out,
    gain_mix,
    w_group,
    w_expert,
    w_gate,
    w_up,
    w_down,
    gain_moe,
):
    seq_count, model_width = x_in.shape
    shares = lax.axis_size("tp")
    share = model_width // shares
    expert_total = w_expert.shape[1]
    ep_count = lax.axis_size("ep")
    local_experts = w_gate.shape[0]
    capacity = max(2, 4 * seq_count // expert_total)
    total_slots = expert_total * capacity
    local_slots = local_experts * capacity
    here = lax.axis_index("tp")
    here_array = here.astype(jnp.int32).reshape(1)

    target = slots_of(routes, expert_total, capacity)
    slot_ids = jnp.arange(total_slots, dtype=jnp.int32)

    base, *parts, new_state = mixer(
        here_array,
        x_in,
        state,
        w_in,
        decay_rate,
        frequency,
        log_step.reshape(1, -1),
        b_in,
        c_out,
        skip,
        w_out,
    )
    arrived = shifted([base, *parts], "tp")
    own, sent = place_rows(base, arrived[1:], target, total_slots)
    rows = exchange(sent.reshape(ep_count, local_slots, share), "ep")

    parts = shifted([own] * shares, "tp")
    whole = jnp.stack(parts).astype(jnp.float32)
    order = (here - jnp.arange(shares)) % shares
    gain_mix = gain_mix.reshape(shares, 1, share)
    hidden_state = normalize(whole, gain_mix[order], (0, 2))
    hidden_bf = hidden_state.astype(jnp.bfloat16)
    w_router = jnp.concatenate([w_group, w_expert], axis=-1).reshape(shares, share, -1)[order]
    logits = jnp.einsum("krd,kde->re", hidden_bf, w_router, preferred_element_type=jnp.float32)
    route_weight = route_weights(logits, routes, w_group.shape[1])
    matches = target[:, :, None] == slot_ids[None, None, :]
    combine_map = jnp.sum(jnp.where(matches, route_weight[:, :, None], 0.0), axis=1)

    rows = by_expert(rows.reshape(total_slots, share))
    gathered = []
    for j in range(local_experts):
        gathered.append(shifted([rows[j]] * shares, "tp"))
    arrived = []
    for j in range(local_experts):
        weights = fetch(j, w_gate, w_up, w_down)
        outs = expert(here_array, gathered[j], gain_mix, *weights)
        arrived.append(shifted(outs, "tp"))
    summed = add_up(arrived)
    returned = exchange(summed.reshape(ep_count, local_slots, share), "ep")
    moe_own = jnp.dot(
        combine_map.astype(jnp.bfloat16),
        returned.reshape(total_slots, share),
        preferred_element_type=jnp.float32,
    ).astype(jnp.bfloat16)
    moe = shifted([moe_own] * shares, "tp")
    out = finish(here_array, hidden_state, moe, gain_moe.reshape(shares, 1, share))
    return (out, new_state)


def solution(mesh):
    in_specs = (
        P(("grp", "ep"), None),
        P(("grp", "ep"), "tp", None),
        P(("grp", "ep"), None),
        P(None, "tp"),
        P("tp", None),
        P("tp", None),
        P("tp"),
        P("tp", None, None),
        P("tp", None, None),
        P("tp"),
        P("tp", None),
        P(),
        P(),
        P(),
        P("ep", None, "tp"),
        P("ep", None, "tp"),
        P("ep", "tp", None),
        P(),
    )
    out_specs = (P(("grp", "ep"), None), P(("grp", "ep"), "tp", None))
    return jax.shard_map(layer, mesh=mesh, in_specs=in_specs, out_specs=out_specs, check_vma=False)
```

```python
import jax
import jax.numpy as jnp
from jax import lax
from jax.experimental import pallas as pl
from jax.experimental.pallas import tpu as pltpu
from jax.sharding import PartitionSpec as P

residual_scale = 8.0**0.25
norm_eps = 1e-05


def exchange(x, axis):
    return lax.all_to_all(x, axis, 0, 0, tiled=True)


def shifted(pieces, axis):
    size = lax.axis_size(axis)
    return [pieces[0]] + [
        lax.ppermute(pieces[k], axis, [(i, (i + k) % size) for i in range(size)])
        for k in range(1, size)
    ]


def normalize(values, gain, axes):
    centre = jnp.mean(values, axes, keepdims=True)
    spread = jnp.mean(jnp.square(values - centre), axes, keepdims=True)
    return (values - centre) * lax.rsqrt(spread + norm_eps) * gain


def route_weights(logits, routes, group_total):
    expert_total = logits.shape[1] - group_total
    per_group = expert_total // group_total
    group_logit = logits[:, :group_total]
    group_exp = jnp.exp(group_logit)
    group_prob = group_exp / jnp.sum(group_exp, -1, keepdims=True)
    chosen = routes[:, 0] // per_group
    group_pick = jnp.sum(
        jnp.where(
            chosen[:, None] == jnp.arange(group_total, dtype=jnp.int32)[None, :], group_prob, 0.0
        ),
        -1,
    )
    expert_logit = logits[:, group_total:]
    picked = jnp.sum(
        jnp.where(
            routes[:, :, None] == jnp.arange(expert_total, dtype=jnp.int32)[None, None, :],
            expert_logit[:, None, :],
            0.0,
        ),
        -1,
    )
    pair_exp = jnp.exp(picked)
    return pair_exp / jnp.sum(pair_exp, -1, keepdims=True) * group_pick[:, None]


def slots_of(routes, expert_total, capacity):
    hits = (routes[:, :, None] == jnp.arange(expert_total, dtype=jnp.int32)[None, None, :]).astype(
        jnp.int32
    )
    tally = jnp.sum(hits, axis=1)
    prior = jnp.cumsum(tally, axis=0) - tally
    return routes * capacity + jnp.sum(prior[:, None, :] * hits, axis=-1)


def ring_places(here_ref, shares):
    t = here_ref[0]
    froms = [lax.rem(t + shares - k, shares) for k in range(shares)]
    tos = [lax.rem(t + k, shares) for k in range(shares)]
    return froms, tos


def columns_of(place, share):
    return pl.ds(pl.multiple_of(place * share, share), share)


def near(ref):
    return pltpu.VMEM(ref.shape, ref.dtype)


def mixer(here, x_in, state, w_in, decay_rate, frequency, log_step, b_in, c_out, skip, w_out):
    seq_count, width = x_in.shape
    channels = w_in.shape[1]
    groups, entries = decay_rate.shape
    per_group = b_in.shape[1]
    lanes = 2 * entries
    shares = lax.axis_size("tp")
    share = width // shares
    together = lanes // per_group
    cut = 4
    arrays = (decay_rate, frequency, log_step, x_in, w_in, b_in, c_out, skip, state, w_out)

    def kernel(here_ref, *refs):
        far = refs[: len(arrays)]
        base_ref = refs[len(arrays)]
        part_refs = refs[len(arrays) + 1 : len(arrays) + shares]
        new_ref = refs[len(arrays) + shares]
        rest = refs[len(arrays) + shares + 1 :]
        close = rest[: len(arrays)]
        decay_ref, freq_ref, log_ref, x_ref, w_in_ref, b_ref, c_ref, skip_ref, state_ref, w_out_ref = close
        in_ref, out_ref, act_ref, sems = rest[len(arrays) :]
        _, tos = ring_places(here_ref, shares)
        piece = width // cut
        copies = {}
        for i, (a, b) in enumerate(zip(far, close)):
            if i == 4:
                for q in range(cut):
                    rows = slice(q * piece, (q + 1) * piece)
                    copies[i, q] = pltpu.make_async_copy(
                        a.at[rows], b.at[rows], sems.at[len(arrays) + q]
                    )
            else:
                copies[i] = pltpu.make_async_copy(a, b, sems.at[i])
        for copy in copies.values():
            copy.start()

        lane = lax.broadcasted_iota(jnp.int32, (1, lanes), 1)
        sign = jnp.where(lane < entries, -1.0, 1.0)
        for i in (0, 1, 2):
            copies[i].wait()
        eye = lax.broadcasted_iota(jnp.int32, (groups, groups), 0) == lax.broadcasted_iota(
            jnp.int32, (groups, groups), 1
        )
        log_column = jnp.sum(jnp.where(eye, log_ref[...], 0.0), -1, keepdims=True)
        step_size = jnp.exp(log_column)
        lam_real = -decay_ref[...]
        freq = freq_ref[...]
        magnitude = jnp.exp(lam_real * step_size)
        angle = freq * step_size
        bar_real = magnitude * jnp.cos(angle)
        bar_imag = magnitude * jnp.sin(angle)
        minus_real = bar_real - 1.0
        modulus = lam_real * lam_real + freq * freq
        ratio_real = (minus_real * lam_real + bar_imag * freq) / modulus
        ratio_imag = (bar_imag * lam_real - minus_real * freq) / modulus

        def twice(v):
            return jnp.concatenate([v, v], axis=-1)

        bar_real = twice(bar_real)
        bar_imag = twice(bar_imag) * sign
        ratio_real = twice(ratio_real)
        ratio_imag = twice(ratio_imag) * sign

        copies[3].wait()
        mix = None
        for q in range(cut):
            copies[4, q].wait()
            rows = slice(q * piece, (q + 1) * piece)
            term = jnp.dot(x_ref[:, rows], w_in_ref[rows, :], preferred_element_type=jnp.float32)
            mix = term if mix is None else mix + term
        mix = mix.astype(jnp.bfloat16).astype(jnp.float32)
        copies[5].wait()
        for g in range(groups):
            b = b_ref[g]
            in_ref[g * per_group : (g + 1) * per_group, :] = (
                ratio_real[g : g + 1] * b + ratio_imag[g : g + 1] * pltpu.roll(b, entries, 1)
            ).astype(jnp.bfloat16)
        copies[6].wait()
        for g in range(groups):
            out_ref[g * per_group : (g + 1) * per_group, :] = (c_ref[g] * -sign).astype(jnp.bfloat16)
        x_wide = x_ref[...].astype(jnp.float32)
        x_mean = jnp.sum(x_wide, -1, keepdims=True) / width
        x_own = x_ref[:, columns_of(here_ref[0], share)].astype(jnp.float32)
        base_ref[...] = residual_scale * (x_own - x_mean)
        copies[7].wait()
        copies[8].wait()
        old = state_ref.reshape(seq_count * groups, lanes)
        new = new_ref.reshape(seq_count * groups, lanes)
        lane_group = lane // per_group
        for j in range(groups // together):
            span = slice(j * lanes, (j + 1) * lanes)
            inputs = mix[:, span]
            spread = jnp.concatenate(
                [jnp.where(lane_group == g, inputs, 0.0) for g in range(together)], axis=0
            ).astype(jnp.bfloat16)
            forcing = jnp.dot(spread, in_ref[span, :], preferred_element_type=jnp.float32)
            held = []
            for g in range(together):
                at = j * together + g
                rows = pl.ds(at, seq_count, stride=groups)
                h = old[rows, :]
                h = (
                    bar_real[at : at + 1] * h
                    + bar_imag[at : at + 1] * pltpu.roll(h, entries, 1)
                    + forcing[g * seq_count : (g + 1) * seq_count]
                )
                new[rows, :] = h
                held.append(h.astype(jnp.bfloat16))
            read = lax.dot_general(
                jnp.concatenate(held, axis=0),
                out_ref[span, :],
                (((1,), (1,)), ((), ())),
                preferred_element_type=jnp.float32,
            )
            value = skip_ref[span] * inputs
            for g in range(together):
                value = value + jnp.where(
                    lane_group == g, read[g * seq_count : (g + 1) * seq_count], 0.0
                )
            act_ref[:, span] = jax.nn.gelu(value).astype(jnp.bfloat16)
        copies[9].wait()
        for k in range(shares):
            part = jnp.dot(
                act_ref[...],
                w_out_ref[:, columns_of(tos[k], share)],
                preferred_element_type=jnp.float32,
            ).astype(jnp.bfloat16)
            if k == 0:
                base_ref[...] += part.astype(jnp.float32)
            else:
                part_refs[k - 1][...] = part

    vmem = pl.BlockSpec(memory_space=pltpu.VMEM)
    hbm = pl.BlockSpec(memory_space=pltpu.HBM)
    return pl.pallas_call(
        kernel,
        in_specs=[pl.BlockSpec(memory_space=pltpu.SMEM)] + [hbm] * len(arrays),
        out_specs=[vmem] * (shares + 1),
        out_shape=[jax.ShapeDtypeStruct((seq_count, share), jnp.float32)]
        + [jax.ShapeDtypeStruct((seq_count, share), jnp.bfloat16)] * (shares - 1)
        + [near(state)],
        scratch_shapes=[near(a) for a in arrays]
        + [
            pltpu.VMEM((channels, lanes), jnp.bfloat16),
            pltpu.VMEM((channels, lanes), jnp.bfloat16),
            pltpu.VMEM((seq_count, channels), jnp.bfloat16),
            pltpu.SemaphoreType.DMA((len(arrays) + cut + shares,)),
        ],
        compiler_params=pltpu.CompilerParams(vmem_limit_bytes=16 * 1024 * 1024),
        name="mixer",
    )(here, *[pltpu.with_memory_space_constraint(a, pltpu.HBM) for a in arrays])


def place_rows(base, arrived, target, total_slots):
    seq_count, share = base.shape
    cut = 4
    piece = total_slots // cut

    def kernel(base_ref, target_ref, *refs):
        own_ref, sent_far, sent_ref, sems = refs[-4:]
        own = base_ref[...]
        for r in refs[:-4]:
            own = own + r[...].astype(jnp.float32)
        own = own.astype(jnp.bfloat16)
        copies = []
        for q in range(cut):
            rows = slice(q * piece, (q + 1) * piece)
            slot = lax.broadcasted_iota(jnp.int32, (piece, seq_count), 0) + q * piece
            hit = slot == target_ref[0:1, :]
            for k in range(1, target_ref.shape[0]):
                hit = hit | (slot == target_ref[k : k + 1, :])
            chosen = jnp.where(hit, 1.0, 0.0).astype(jnp.bfloat16)
            sent_ref[rows, :] = jnp.dot(chosen, own, preferred_element_type=jnp.float32).astype(
                jnp.bfloat16
            )
            copies.append(pltpu.make_async_copy(sent_ref.at[rows], sent_far.at[rows], sems.at[q]))
            copies[-1].start()
        own_ref[...] = own
        for copy in copies:
            copy.wait()

    vmem = pl.BlockSpec(memory_space=pltpu.VMEM)
    return pl.pallas_call(
        kernel,
        in_specs=[vmem] * (2 + len(arrived)),
        out_specs=[vmem, pl.BlockSpec(memory_space=pltpu.HBM)],
        out_shape=[
            jax.ShapeDtypeStruct((seq_count, share), jnp.bfloat16),
            jax.ShapeDtypeStruct((total_slots, share), jnp.bfloat16),
        ],
        scratch_shapes=[
            pltpu.VMEM((total_slots, share), jnp.bfloat16),
            pltpu.SemaphoreType.DMA((cut,)),
        ],
        compiler_params=pltpu.CompilerParams(vmem_limit_bytes=8 * 1024 * 1024),
        name="place_rows",
    )(base, target.T, *arrived)


def fetch(*weights):
    count = len(weights)
    local_experts = weights[0].shape[0]

    def kernel(*refs):
        copies = [
            pltpu.make_async_copy(
                refs[i].at[j], refs[count + j * count + i], refs[-1].at[j * count + i]
            )
            for j in range(local_experts)
            for i in range(count)
        ]
        for copy in copies:
            copy.start()
        for copy in copies:
            copy.wait()

    out = pl.pallas_call(
        kernel,
        in_specs=[pl.BlockSpec(memory_space=pltpu.HBM)] * count,
        out_specs=[pl.BlockSpec(memory_space=pltpu.VMEM)] * (count * local_experts),
        out_shape=[pltpu.VMEM(w.shape[1:], w.dtype) for w in weights] * local_experts,
        scratch_shapes=[pltpu.SemaphoreType.DMA((count * local_experts,))],
        compiler_params=pltpu.CompilerParams(vmem_limit_bytes=1024 * 1024),
        name="fetch",
    )(*[pltpu.with_memory_space_constraint(w, pltpu.HBM) for w in weights])
    return [out[j * count : (j + 1) * count] for j in range(local_experts)]


def swap_halves(first, second):
    half = first.shape[1] // 2
    low = lax.broadcasted_iota(jnp.int32, first.shape, 1) < half
    return (
        jnp.where(low, first, pltpu.roll(second, half, 1)),
        jnp.where(low, pltpu.roll(first, half, 1), second),
    )


def by_expert(rows):
    slots, share = rows.shape
    tile = 8

    def kernel(rows_ref, *out_refs):
        tiles = rows_ref[...].astype(jnp.float32).reshape(slots // (2 * tile), 2, tile, share)
        for out_ref, part in zip(out_refs, swap_halves(tiles[:, 0], tiles[:, 1])):
            out_ref[...] = part.reshape(slots // 2, share).astype(jnp.bfloat16)

    vmem = pl.BlockSpec(memory_space=pltpu.VMEM)
    return pl.pallas_call(
        kernel,
        in_specs=[vmem],
        out_specs=[vmem] * 2,
        out_shape=[jax.ShapeDtypeStruct((slots // 2, share), jnp.bfloat16)] * 2,
        compiler_params=pltpu.CompilerParams(vmem_limit_bytes=8 * 1024 * 1024),
        name="by_expert",
    )(rows)


def add_up(arrived):
    rows, share = arrived[0][0].shape
    count = len(arrived[0])
    tile = 8

    def kernel(*refs):
        totals = []
        for h in range(2):
            group = refs[h * count : (h + 1) * count]
            total = group[0][...].astype(jnp.float32)
            for r in group[1:]:
                total = total + r[...].astype(jnp.float32)
            totals.append(total.reshape(rows // tile, tile, share))
        both = jnp.stack(swap_halves(*totals), axis=1).reshape(2 * rows, share)
        refs[-1][...] = both.astype(jnp.bfloat16)

    vmem = pl.BlockSpec(memory_space=pltpu.VMEM)
    return pl.pallas_call(
        kernel,
        in_specs=[vmem] * (2 * count),
        out_specs=vmem,
        out_shape=jax.ShapeDtypeStruct((2 * rows, share), jnp.bfloat16),
        compiler_params=pltpu.CompilerParams(vmem_limit_bytes=8 * 1024 * 1024),
        name="add_up",
    )(*arrived[0], *arrived[1])


def expert(here, pieces, gain, w_gate, w_up, w_down):
    slots, share = pieces[0].shape
    shares = len(pieces)
    width = w_gate.shape[0]
    chunk = 32

    def kernel(here_ref, *refs):
        piece_refs = refs[:shares]
        gain_ref, gate_ref, up_ref, down_ref = refs[shares : shares + 4]
        out_refs = refs[shares + 4 : 2 * shares + 4]
        row_ref = refs[-1]
        froms, tos = ring_places(here_ref, shares)

        def norm_rows(i, carry):
            rows = pl.ds(pl.multiple_of(i * chunk, chunk), chunk)
            values = [r[rows, :].astype(jnp.float32) for r in piece_refs]
            total = values[0]
            for v in values[1:]:
                total = total + v
            centre = jnp.sum(total, -1, keepdims=True) / width
            values = [v - centre for v in values]
            total = values[0] * values[0]
            for v in values[1:]:
                total = total + v * v
            scale = lax.rsqrt(jnp.sum(total, -1, keepdims=True) / width + norm_eps)
            for k, v in enumerate(values):
                row_ref[rows, columns_of(froms[k], share)] = (
                    v * scale * gain_ref[froms[k]]
                ).astype(jnp.bfloat16)
            return carry

        lax.fori_loop(0, slots // chunk, norm_rows, 0)
        rows = row_ref[...]
        gate_part = jnp.dot(rows, gate_ref[...], preferred_element_type=jnp.float32)
        up_part = jnp.dot(rows, up_ref[...], preferred_element_type=jnp.float32)
        act = (gate_part * jax.nn.sigmoid(gate_part) * up_part).astype(jnp.bfloat16)
        for k in range(shares):
            out_refs[k][...] = jnp.dot(
                act, down_ref[:, columns_of(tos[k], share)], preferred_element_type=jnp.float32
            ).astype(jnp.bfloat16)

    vmem = pl.BlockSpec(memory_space=pltpu.VMEM)
    return pl.pallas_call(
        kernel,
        in_specs=[pl.BlockSpec(memory_space=pltpu.SMEM)] + [vmem] * (shares + 4),
        out_specs=[vmem] * shares,
        out_shape=[jax.ShapeDtypeStruct((slots, share), jnp.bfloat16)] * shares,
        scratch_shapes=[pltpu.VMEM((slots, width), jnp.bfloat16)],
        compiler_params=pltpu.CompilerParams(vmem_limit_bytes=16 * 1024 * 1024),
        name="expert",
    )(here, *pieces, gain, w_gate, w_up, w_down)


def finish(here, hidden, pieces, gain):
    rows, share = pieces[0].shape
    shares = len(pieces)
    width = shares * share
    cut = 4
    piece = rows // cut

    def kernel(here_ref, hidden_ref, *refs):
        piece_refs = refs[:shares]
        gain_ref, out_far, out_ref, sems = refs[shares:]
        froms, _ = ring_places(here_ref, shares)
        copies = []
        for q in range(cut):
            some = slice(q * piece, (q + 1) * piece)
            values = [
                residual_scale * hidden_ref[k, some] + piece_refs[k][some].astype(jnp.float32)
                for k in range(shares)
            ]
            total = values[0]
            for v in values[1:]:
                total = total + v
            centre = jnp.sum(total, -1, keepdims=True) / width
            values = [v - centre for v in values]
            total = values[0] * values[0]
            for v in values[1:]:
                total = total + v * v
            scale = lax.rsqrt(jnp.sum(total, -1, keepdims=True) / width + norm_eps)
            for k, v in enumerate(values):
                out_ref[some, columns_of(froms[k], share)] = (v * scale * gain_ref[froms[k]]).astype(
                    jnp.bfloat16
                )
            copies.append(pltpu.make_async_copy(out_ref.at[some], out_far.at[some], sems.at[q]))
            copies[-1].start()
        for copy in copies:
            copy.wait()

    vmem = pl.BlockSpec(memory_space=pltpu.VMEM)
    return pl.pallas_call(
        kernel,
        in_specs=[pl.BlockSpec(memory_space=pltpu.SMEM)] + [vmem] * (shares + 2),
        out_specs=pl.BlockSpec(memory_space=pltpu.HBM),
        out_shape=jax.ShapeDtypeStruct((rows, width), jnp.bfloat16),
        scratch_shapes=[
            pltpu.VMEM((rows, width), jnp.bfloat16),
            pltpu.SemaphoreType.DMA((cut,)),
        ],
        compiler_params=pltpu.CompilerParams(vmem_limit_bytes=8 * 1024 * 1024),
        name="finish",
    )(here, hidden, *pieces, gain)


def layer(
    x_in,
    state,
    routes,
    w_in,
    decay_rate,
    frequency,
    log_step,
    b_in,
    c_out,
    skip,
    w_out,
    gain_mix,
    w_group,
    w_expert,
    w_gate,
    w_up,
    w_down,
    gain_moe,
):
    seq_count, model_width = x_in.shape
    shares = lax.axis_size("tp")
    share = model_width // shares
    expert_total = w_expert.shape[1]
    ep_count = lax.axis_size("ep")
    local_experts = w_gate.shape[0]
    capacity = max(2, 4 * seq_count // expert_total)
    total_slots = expert_total * capacity
    local_slots = local_experts * capacity
    here = lax.axis_index("tp")
    here_array = here.astype(jnp.int32).reshape(1)

    target = slots_of(routes, expert_total, capacity)
    slot_ids = jnp.arange(total_slots, dtype=jnp.int32)

    base, *parts, new_state = mixer(
        here_array,
        x_in,
        state,
        w_in,
        decay_rate,
        frequency,
        log_step.reshape(1, -1),
        b_in,
        c_out,
        skip,
        w_out,
    )
    arrived = shifted([base, *parts], "tp")
    own, sent = place_rows(base, arrived[1:], target, total_slots)
    rows = exchange(sent.reshape(ep_count, local_slots, share), "ep")

    parts = shifted([own] * shares, "tp")
    whole = jnp.stack(parts).astype(jnp.float32)
    order = (here - jnp.arange(shares)) % shares
    gain_mix = gain_mix.reshape(shares, 1, share)
    hidden_state = normalize(whole, gain_mix[order], (0, 2))
    hidden_bf = hidden_state.astype(jnp.bfloat16)
    w_router = jnp.concatenate([w_group, w_expert], axis=-1).reshape(shares, share, -1)[order]
    logits = jnp.einsum("krd,kde->re", hidden_bf, w_router, preferred_element_type=jnp.float32)
    route_weight = route_weights(logits, routes, w_group.shape[1])
    matches = target[:, :, None] == slot_ids[None, None, :]
    combine_map = jnp.sum(jnp.where(matches, route_weight[:, :, None], 0.0), axis=1)

    rows = by_expert(rows.reshape(total_slots, share))
    gathered = []
    for j in range(local_experts):
        gathered.append(shifted([rows[j]] * shares, "tp"))
    weights = fetch(w_gate, w_up, w_down)
    arrived = []
    for j in range(local_experts):
        outs = expert(here_array, gathered[j], gain_mix, *weights[j])
        arrived.append(shifted(outs, "tp"))
    summed = add_up(arrived)
    returned = exchange(summed.reshape(ep_count, local_slots, share), "ep")
    moe_own = jnp.dot(
        combine_map.astype(jnp.bfloat16),
        returned.reshape(total_slots, share),
        preferred_element_type=jnp.float32,
    ).astype(jnp.bfloat16)
    moe = shifted([moe_own] * shares, "tp")
    out = finish(here_array, hidden_state, moe, gain_moe.reshape(shares, 1, share))
    return (out, new_state)


def solution(mesh):
    in_specs = (
        P(("grp", "ep"), None),
        P(("grp", "ep"), "tp", None),
        P(("grp", "ep"), None),
        P(None, "tp"),
        P("tp", None),
        P("tp", None),
        P("tp"),
        P("tp", None, None),
        P("tp", None, None),
        P("tp"),
        P("tp", None),
        P(),
        P(),
        P(),
        P("ep", None, "tp"),
        P("ep", None, "tp"),
        P("ep", "tp", None),
        P(),
    )
    out_specs = (P(("grp", "ep"), None), P(("grp", "ep"), "tp", None))
    return jax.shard_map(layer, mesh=mesh, in_specs=in_specs, out_specs=out_specs, check_vma=False)
```

```python
import jax
import jax.numpy as jnp
from jax import lax
from jax.experimental import pallas as pl
from jax.experimental.pallas import tpu as pltpu
from jax.sharding import PartitionSpec as P

residual_scale = 8.0**0.25
norm_eps = 1e-05


def exchange(x, axis):
    return lax.all_to_all(x, axis, 0, 0, tiled=True)


def shifted(pieces, axis):
    size = lax.axis_size(axis)
    return [pieces[0]] + [
        lax.ppermute(pieces[k], axis, [(i, (i + k) % size) for i in range(size)])
        for k in range(1, size)
    ]


def normalize(values, gain, axes):
    centre = jnp.mean(values, axes, keepdims=True)
    spread = jnp.mean(jnp.square(values - centre), axes, keepdims=True)
    return (values - centre) * lax.rsqrt(spread + norm_eps) * gain


def route_weights(logits, routes, group_total):
    expert_total = logits.shape[1] - group_total
    per_group = expert_total // group_total
    group_logit = logits[:, :group_total]
    group_exp = jnp.exp(group_logit)
    group_prob = group_exp / jnp.sum(group_exp, -1, keepdims=True)
    chosen = routes[:, 0] // per_group
    group_pick = jnp.sum(
        jnp.where(
            chosen[:, None] == jnp.arange(group_total, dtype=jnp.int32)[None, :], group_prob, 0.0
        ),
        -1,
    )
    expert_logit = logits[:, group_total:]
    picked = jnp.sum(
        jnp.where(
            routes[:, :, None] == jnp.arange(expert_total, dtype=jnp.int32)[None, None, :],
            expert_logit[:, None, :],
            0.0,
        ),
        -1,
    )
    pair_exp = jnp.exp(picked)
    return pair_exp / jnp.sum(pair_exp, -1, keepdims=True) * group_pick[:, None]


def slots_of(routes, expert_total, capacity):
    hits = (routes[:, :, None] == jnp.arange(expert_total, dtype=jnp.int32)[None, None, :]).astype(
        jnp.int32
    )
    tally = jnp.sum(hits, axis=1)
    prior = jnp.cumsum(tally, axis=0) - tally
    return routes * capacity + jnp.sum(prior[:, None, :] * hits, axis=-1)


def ring_places(here_ref, shares):
    t = here_ref[0]
    froms = [lax.rem(t + shares - k, shares) for k in range(shares)]
    tos = [lax.rem(t + k, shares) for k in range(shares)]
    return froms, tos


def columns_of(place, share):
    return pl.ds(pl.multiple_of(place * share, share), share)


def near(ref):
    return pltpu.VMEM(ref.shape, ref.dtype)


def mixer(here, x_in, state, w_in, decay_rate, frequency, log_step, b_in, c_out, skip, w_out):
    seq_count, width = x_in.shape
    channels = w_in.shape[1]
    groups, entries = decay_rate.shape
    per_group = b_in.shape[1]
    lanes = 2 * entries
    shares = lax.axis_size("tp")
    share = width // shares
    together = lanes // per_group
    cut = 4
    arrays = (decay_rate, frequency, log_step, x_in, w_in, b_in, c_out, skip, state, w_out)

    def kernel(here_ref, *refs):
        far = refs[: len(arrays)]
        base_ref = refs[len(arrays)]
        part_refs = refs[len(arrays) + 1 : len(arrays) + shares]
        new_ref = refs[len(arrays) + shares]
        rest = refs[len(arrays) + shares + 1 :]
        close = rest[: len(arrays)]
        decay_ref, freq_ref, log_ref, x_ref, w_in_ref, b_ref, c_ref, skip_ref, state_ref, w_out_ref = close
        in_ref, out_ref, act_ref, sems = rest[len(arrays) :]
        _, tos = ring_places(here_ref, shares)
        piece = width // cut
        copies = {}
        for i, (a, b) in enumerate(zip(far, close)):
            if i == 4:
                for q in range(cut):
                    rows = slice(q * piece, (q + 1) * piece)
                    copies[i, q] = pltpu.make_async_copy(
                        a.at[rows], b.at[rows], sems.at[len(arrays) + q]
                    )
            else:
                copies[i] = pltpu.make_async_copy(a, b, sems.at[i])
        for copy in copies.values():
            copy.start()

        lane = lax.broadcasted_iota(jnp.int32, (1, lanes), 1)
        sign = jnp.where(lane < entries, -1.0, 1.0)
        for i in (0, 1, 2):
            copies[i].wait()
        eye = lax.broadcasted_iota(jnp.int32, (groups, groups), 0) == lax.broadcasted_iota(
            jnp.int32, (groups, groups), 1
        )
        log_column = jnp.sum(jnp.where(eye, log_ref[...], 0.0), -1, keepdims=True)
        step_size = jnp.exp(log_column)
        lam_real = -decay_ref[...]
        freq = freq_ref[...]
        magnitude = jnp.exp(lam_real * step_size)
        angle = freq * step_size
        bar_real = magnitude * jnp.cos(angle)
        bar_imag = magnitude * jnp.sin(angle)
        minus_real = bar_real - 1.0
        modulus = lam_real * lam_real + freq * freq
        ratio_real = (minus_real * lam_real + bar_imag * freq) / modulus
        ratio_imag = (bar_imag * lam_real - minus_real * freq) / modulus

        def twice(v):
            return jnp.concatenate([v, v], axis=-1)

        bar_real = twice(bar_real)
        bar_imag = twice(bar_imag) * sign
        ratio_real = twice(ratio_real)
        ratio_imag = twice(ratio_imag) * sign

        copies[3].wait()
        mix = None
        for q in range(cut):
            copies[4, q].wait()
            rows = slice(q * piece, (q + 1) * piece)
            term = jnp.dot(x_ref[:, rows], w_in_ref[rows, :], preferred_element_type=jnp.float32)
            mix = term if mix is None else mix + term
        mix = mix.astype(jnp.bfloat16).astype(jnp.float32)
        copies[5].wait()
        for g in range(groups):
            b = b_ref[g]
            in_ref[g * per_group : (g + 1) * per_group, :] = (
                ratio_real[g : g + 1] * b + ratio_imag[g : g + 1] * pltpu.roll(b, entries, 1)
            ).astype(jnp.bfloat16)
        copies[6].wait()
        for g in range(groups):
            out_ref[g * per_group : (g + 1) * per_group, :] = (c_ref[g] * -sign).astype(jnp.bfloat16)
        x_wide = x_ref[...].astype(jnp.float32)
        x_mean = jnp.sum(x_wide, -1, keepdims=True) / width
        x_own = x_ref[:, columns_of(here_ref[0], share)].astype(jnp.float32)
        base_ref[...] = residual_scale * (x_own - x_mean)
        copies[7].wait()
        copies[8].wait()
        old = state_ref.reshape(seq_count * groups, lanes)
        new = new_ref.reshape(seq_count * groups, lanes)
        lane_group = lane // per_group
        for j in range(groups // together):
            span = slice(j * lanes, (j + 1) * lanes)
            inputs = mix[:, span]
            spread = jnp.concatenate(
                [jnp.where(lane_group == g, inputs, 0.0) for g in range(together)], axis=0
            ).astype(jnp.bfloat16)
            forcing = jnp.dot(spread, in_ref[span, :], preferred_element_type=jnp.float32)
            held = []
            for g in range(together):
                at = j * together + g
                rows = pl.ds(at, seq_count, stride=groups)
                h = old[rows, :]
                h = (
                    bar_real[at : at + 1] * h
                    + bar_imag[at : at + 1] * pltpu.roll(h, entries, 1)
                    + forcing[g * seq_count : (g + 1) * seq_count]
                )
                new[rows, :] = h
                held.append(h.astype(jnp.bfloat16))
            read = lax.dot_general(
                jnp.concatenate(held, axis=0),
                out_ref[span, :],
                (((1,), (1,)), ((), ())),
                preferred_element_type=jnp.float32,
            )
            value = skip_ref[span] * inputs
            for g in range(together):
                value = value + jnp.where(
                    lane_group == g, read[g * seq_count : (g + 1) * seq_count], 0.0
                )
            act_ref[:, span] = jax.nn.gelu(value).astype(jnp.bfloat16)
        copies[9].wait()
        for k in range(shares):
            part = jnp.dot(
                act_ref[...],
                w_out_ref[:, columns_of(tos[k], share)],
                preferred_element_type=jnp.float32,
            ).astype(jnp.bfloat16)
            if k == 0:
                base_ref[...] += part.astype(jnp.float32)
            else:
                part_refs[k - 1][...] = part

    vmem = pl.BlockSpec(memory_space=pltpu.VMEM)
    hbm = pl.BlockSpec(memory_space=pltpu.HBM)
    return pl.pallas_call(
        kernel,
        in_specs=[pl.BlockSpec(memory_space=pltpu.SMEM)] + [hbm] * len(arrays),
        out_specs=[vmem] * (shares + 1),
        out_shape=[jax.ShapeDtypeStruct((seq_count, share), jnp.float32)]
        + [jax.ShapeDtypeStruct((seq_count, share), jnp.bfloat16)] * (shares - 1)
        + [near(state)],
        scratch_shapes=[near(a) for a in arrays]
        + [
            pltpu.VMEM((channels, lanes), jnp.bfloat16),
            pltpu.VMEM((channels, lanes), jnp.bfloat16),
            pltpu.VMEM((seq_count, channels), jnp.bfloat16),
            pltpu.SemaphoreType.DMA((len(arrays) + cut + shares,)),
        ],
        compiler_params=pltpu.CompilerParams(vmem_limit_bytes=16 * 1024 * 1024),
        name="mixer",
    )(here, *[pltpu.with_memory_space_constraint(a, pltpu.HBM) for a in arrays])


def place_rows(base, arrived, target, total_slots):
    seq_count, share = base.shape
    cut = 4
    piece = total_slots // cut

    def kernel(base_ref, target_ref, *refs):
        own_ref, sent_far, sent_ref, sems = refs[-4:]
        own = base_ref[...]
        for r in refs[:-4]:
            own = own + r[...].astype(jnp.float32)
        own = own.astype(jnp.bfloat16)
        copies = []
        for q in range(cut):
            rows = slice(q * piece, (q + 1) * piece)
            slot = lax.broadcasted_iota(jnp.int32, (piece, seq_count), 0) + q * piece
            hit = slot == target_ref[0:1, :]
            for k in range(1, target_ref.shape[0]):
                hit = hit | (slot == target_ref[k : k + 1, :])
            chosen = jnp.where(hit, 1.0, 0.0).astype(jnp.bfloat16)
            sent_ref[rows, :] = jnp.dot(chosen, own, preferred_element_type=jnp.float32).astype(
                jnp.bfloat16
            )
            copies.append(pltpu.make_async_copy(sent_ref.at[rows], sent_far.at[rows], sems.at[q]))
            copies[-1].start()
        own_ref[...] = own
        for copy in copies:
            copy.wait()

    vmem = pl.BlockSpec(memory_space=pltpu.VMEM)
    return pl.pallas_call(
        kernel,
        in_specs=[vmem] * (2 + len(arrived)),
        out_specs=[vmem, pl.BlockSpec(memory_space=pltpu.HBM)],
        out_shape=[
            jax.ShapeDtypeStruct((seq_count, share), jnp.bfloat16),
            jax.ShapeDtypeStruct((total_slots, share), jnp.bfloat16),
        ],
        scratch_shapes=[
            pltpu.VMEM((total_slots, share), jnp.bfloat16),
            pltpu.SemaphoreType.DMA((cut,)),
        ],
        compiler_params=pltpu.CompilerParams(vmem_limit_bytes=8 * 1024 * 1024),
        name="place_rows",
    )(base, target.T, *arrived)


def fetch(new_state, *weights):
    count = len(weights)
    local_experts = weights[0].shape[0]

    def kernel(new_ref, *refs):
        new_far, refs = refs[count], refs[:count] + refs[count + 1 :]
        copies = [
            pltpu.make_async_copy(
                refs[i].at[j], refs[count + j * count + i], refs[-1].at[j * count + i]
            )
            for j in range(local_experts)
            for i in range(count)
        ]
        copies.append(
            pltpu.make_async_copy(new_ref, new_far, refs[-1].at[count * local_experts])
        )
        for copy in copies:
            copy.start()
        for copy in copies:
            copy.wait()

    out = pl.pallas_call(
        kernel,
        in_specs=[pl.BlockSpec(memory_space=pltpu.VMEM)]
        + [pl.BlockSpec(memory_space=pltpu.HBM)] * count,
        out_specs=[pl.BlockSpec(memory_space=pltpu.HBM)]
        + [pl.BlockSpec(memory_space=pltpu.VMEM)] * (count * local_experts),
        out_shape=[jax.ShapeDtypeStruct(new_state.shape, new_state.dtype)]
        + [pltpu.VMEM(w.shape[1:], w.dtype) for w in weights] * local_experts,
        scratch_shapes=[pltpu.SemaphoreType.DMA((count * local_experts + 1,))],
        compiler_params=pltpu.CompilerParams(vmem_limit_bytes=2 * 1024 * 1024),
        name="fetch",
    )(new_state, *[pltpu.with_memory_space_constraint(w, pltpu.HBM) for w in weights])
    new_state, *out = out
    return new_state, [out[j * count : (j + 1) * count] for j in range(local_experts)]


def swap_halves(first, second):
    half = first.shape[1] // 2
    low = lax.broadcasted_iota(jnp.int32, first.shape, 1) < half
    return (
        jnp.where(low, first, pltpu.roll(second, half, 1)),
        jnp.where(low, pltpu.roll(first, half, 1), second),
    )


def by_expert(rows):
    slots, share = rows.shape
    tile = 8

    def kernel(rows_ref, *out_refs):
        tiles = rows_ref[...].astype(jnp.float32).reshape(slots // (2 * tile), 2, tile, share)
        for out_ref, part in zip(out_refs, swap_halves(tiles[:, 0], tiles[:, 1])):
            out_ref[...] = part.reshape(slots // 2, share).astype(jnp.bfloat16)

    vmem = pl.BlockSpec(memory_space=pltpu.VMEM)
    return pl.pallas_call(
        kernel,
        in_specs=[vmem],
        out_specs=[vmem] * 2,
        out_shape=[jax.ShapeDtypeStruct((slots // 2, share), jnp.bfloat16)] * 2,
        compiler_params=pltpu.CompilerParams(vmem_limit_bytes=8 * 1024 * 1024),
        name="by_expert",
    )(rows)


def add_up(arrived):
    rows, share = arrived[0][0].shape
    count = len(arrived[0])
    tile = 8

    def kernel(*refs):
        totals = []
        for h in range(2):
            group = refs[h * count : (h + 1) * count]
            total = group[0][...].astype(jnp.float32)
            for r in group[1:]:
                total = total + r[...].astype(jnp.float32)
            totals.append(total.reshape(rows // tile, tile, share))
        both = jnp.stack(swap_halves(*totals), axis=1).reshape(2 * rows, share)
        refs[-1][...] = both.astype(jnp.bfloat16)

    vmem = pl.BlockSpec(memory_space=pltpu.VMEM)
    return pl.pallas_call(
        kernel,
        in_specs=[vmem] * (2 * count),
        out_specs=vmem,
        out_shape=jax.ShapeDtypeStruct((2 * rows, share), jnp.bfloat16),
        compiler_params=pltpu.CompilerParams(vmem_limit_bytes=8 * 1024 * 1024),
        name="add_up",
    )(*arrived[0], *arrived[1])


def expert(here, pieces, gain, w_gate, w_up, w_down):
    slots, share = pieces[0].shape
    shares = len(pieces)
    width = w_gate.shape[0]
    chunk = 32

    def kernel(here_ref, *refs):
        piece_refs = refs[:shares]
        gain_ref, gate_ref, up_ref, down_ref = refs[shares : shares + 4]
        out_refs = refs[shares + 4 : 2 * shares + 4]
        row_ref = refs[-1]
        froms, tos = ring_places(here_ref, shares)

        def norm_rows(i, carry):
            rows = pl.ds(pl.multiple_of(i * chunk, chunk), chunk)
            values = [r[rows, :].astype(jnp.float32) for r in piece_refs]
            total = values[0]
            for v in values[1:]:
                total = total + v
            centre = jnp.sum(total, -1, keepdims=True) / width
            values = [v - centre for v in values]
            total = values[0] * values[0]
            for v in values[1:]:
                total = total + v * v
            scale = lax.rsqrt(jnp.sum(total, -1, keepdims=True) / width + norm_eps)
            for k, v in enumerate(values):
                row_ref[rows, columns_of(froms[k], share)] = (
                    v * scale * gain_ref[froms[k]]
                ).astype(jnp.bfloat16)
            return carry

        lax.fori_loop(0, slots // chunk, norm_rows, 0)
        rows = row_ref[...]
        gate_part = jnp.dot(rows, gate_ref[...], preferred_element_type=jnp.float32)
        up_part = jnp.dot(rows, up_ref[...], preferred_element_type=jnp.float32)
        act = (gate_part * jax.nn.sigmoid(gate_part) * up_part).astype(jnp.bfloat16)
        for k in range(shares):
            out_refs[k][...] = jnp.dot(
                act, down_ref[:, columns_of(tos[k], share)], preferred_element_type=jnp.float32
            ).astype(jnp.bfloat16)

    vmem = pl.BlockSpec(memory_space=pltpu.VMEM)
    return pl.pallas_call(
        kernel,
        in_specs=[pl.BlockSpec(memory_space=pltpu.SMEM)] + [vmem] * (shares + 4),
        out_specs=[vmem] * shares,
        out_shape=[jax.ShapeDtypeStruct((slots, share), jnp.bfloat16)] * shares,
        scratch_shapes=[pltpu.VMEM((slots, width), jnp.bfloat16)],
        compiler_params=pltpu.CompilerParams(vmem_limit_bytes=16 * 1024 * 1024),
        name="expert",
    )(here, *pieces, gain, w_gate, w_up, w_down)


def finish(here, hidden, pieces, gain):
    rows, share = pieces[0].shape
    shares = len(pieces)
    width = shares * share
    cut = 4
    piece = rows // cut

    def kernel(here_ref, hidden_ref, *refs):
        piece_refs = refs[:shares]
        gain_ref, out_far, out_ref, sems = refs[shares:]
        froms, _ = ring_places(here_ref, shares)
        copies = []
        for q in range(cut):
            some = slice(q * piece, (q + 1) * piece)
            values = [
                residual_scale * hidden_ref[k, some] + piece_refs[k][some].astype(jnp.float32)
                for k in range(shares)
            ]
            total = values[0]
            for v in values[1:]:
                total = total + v
            centre = jnp.sum(total, -1, keepdims=True) / width
            values = [v - centre for v in values]
            total = values[0] * values[0]
            for v in values[1:]:
                total = total + v * v
            scale = lax.rsqrt(jnp.sum(total, -1, keepdims=True) / width + norm_eps)
            for k, v in enumerate(values):
                out_ref[some, columns_of(froms[k], share)] = (v * scale * gain_ref[froms[k]]).astype(
                    jnp.bfloat16
                )
            copies.append(pltpu.make_async_copy(out_ref.at[some], out_far.at[some], sems.at[q]))
            copies[-1].start()
        for copy in copies:
            copy.wait()

    vmem = pl.BlockSpec(memory_space=pltpu.VMEM)
    return pl.pallas_call(
        kernel,
        in_specs=[pl.BlockSpec(memory_space=pltpu.SMEM)] + [vmem] * (shares + 2),
        out_specs=pl.BlockSpec(memory_space=pltpu.HBM),
        out_shape=jax.ShapeDtypeStruct((rows, width), jnp.bfloat16),
        scratch_shapes=[
            pltpu.VMEM((rows, width), jnp.bfloat16),
            pltpu.SemaphoreType.DMA((cut,)),
        ],
        compiler_params=pltpu.CompilerParams(vmem_limit_bytes=8 * 1024 * 1024),
        name="finish",
    )(here, hidden, *pieces, gain)


def layer(
    x_in,
    state,
    routes,
    w_in,
    decay_rate,
    frequency,
    log_step,
    b_in,
    c_out,
    skip,
    w_out,
    gain_mix,
    w_group,
    w_expert,
    w_gate,
    w_up,
    w_down,
    gain_moe,
):
    seq_count, model_width = x_in.shape
    shares = lax.axis_size("tp")
    share = model_width // shares
    expert_total = w_expert.shape[1]
    ep_count = lax.axis_size("ep")
    local_experts = w_gate.shape[0]
    capacity = max(2, 4 * seq_count // expert_total)
    total_slots = expert_total * capacity
    local_slots = local_experts * capacity
    here = lax.axis_index("tp")
    here_array = here.astype(jnp.int32).reshape(1)

    target = slots_of(routes, expert_total, capacity)
    slot_ids = jnp.arange(total_slots, dtype=jnp.int32)

    base, *parts, new_state = mixer(
        here_array,
        x_in,
        state,
        w_in,
        decay_rate,
        frequency,
        log_step.reshape(1, -1),
        b_in,
        c_out,
        skip,
        w_out,
    )
    arrived = shifted([base, *parts], "tp")
    own, sent = place_rows(base, arrived[1:], target, total_slots)
    rows = exchange(sent.reshape(ep_count, local_slots, share), "ep")

    parts = shifted([own] * shares, "tp")
    whole = jnp.stack(parts).astype(jnp.float32)
    order = (here - jnp.arange(shares)) % shares
    gain_mix = gain_mix.reshape(shares, 1, share)
    hidden_state = normalize(whole, gain_mix[order], (0, 2))
    hidden_bf = hidden_state.astype(jnp.bfloat16)
    w_router = jnp.concatenate([w_group, w_expert], axis=-1).reshape(shares, share, -1)[order]
    logits = jnp.einsum("krd,kde->re", hidden_bf, w_router, preferred_element_type=jnp.float32)
    route_weight = route_weights(logits, routes, w_group.shape[1])
    matches = target[:, :, None] == slot_ids[None, None, :]
    combine_map = jnp.sum(jnp.where(matches, route_weight[:, :, None], 0.0), axis=1)

    rows = by_expert(rows.reshape(total_slots, share))
    gathered = []
    for j in range(local_experts):
        gathered.append(shifted([rows[j]] * shares, "tp"))
    new_state, weights = fetch(new_state, w_gate, w_up, w_down)
    arrived = []
    for j in range(local_experts):
        outs = expert(here_array, gathered[j], gain_mix, *weights[j])
        arrived.append(shifted(outs, "tp"))
    summed = add_up(arrived)
    returned = exchange(summed.reshape(ep_count, local_slots, share), "ep")
    moe_own = jnp.dot(
        combine_map.astype(jnp.bfloat16),
        returned.reshape(total_slots, share),
        preferred_element_type=jnp.float32,
    ).astype(jnp.bfloat16)
    moe = shifted([moe_own] * shares, "tp")
    out = finish(here_array, hidden_state, moe, gain_moe.reshape(shares, 1, share))
    return (out, new_state)


def solution(mesh):
    in_specs = (
        P(("grp", "ep"), None),
        P(("grp", "ep"), "tp", None),
        P(("grp", "ep"), None),
        P(None, "tp"),
        P("tp", None),
        P("tp", None),
        P("tp"),
        P("tp", None, None),
        P("tp", None, None),
        P("tp"),
        P("tp", None),
        P(),
        P(),
        P(),
        P("ep", None, "tp"),
        P("ep", None, "tp"),
        P("ep", "tp", None),
        P(),
    )
    out_specs = (P(("grp", "ep"), None), P(("grp", "ep"), "tp", None))
    return jax.shard_map(layer, mesh=mesh, in_specs=in_specs, out_specs=out_specs, check_vma=False)
```
